32 devices in a mesh: sp: 8 (over z, x), tp: 4 (over y, core).
Axes of the slice: x: 2, y: 2, z: 4, core: 2. Of those that a mesh axis runs over, the one named last changes fastest.
Arguments:
- queries: bfloat16 [8192, 2048], P('sp', 'tp'), may hold values from -16 to 16
- key_rows: bfloat16 [8192, 512], P('sp', 'tp'), may hold values from -16 to 16
- value_rows: bfloat16 [8192, 512], P('sp', 'tp'), may hold values from -6 to 6
- doc_ids: int32 [8192], P('sp'), may hold values from 0 to 3, never falling along the last dimension, each value on 1 to 4096 neighbouring positions
- sink_logit: float32 [32], P('tp'), may hold values from 3 to 7
- residual: bfloat16 [8192, 2048], P(('sp', 'tp')), may hold values from -6 to 6
- out_weight: bfloat16 [2048, 2048], P('tp'), may hold values from -3.5 to 3.5
- norm_gain: float32 [2048], replicated, may hold values from 0.1 to 1.9
- gate_weight: bfloat16 [8, 2048, 512], P('sp'), may hold values from -0.125 to 0.125
- up_weight: bfloat16 [8, 2048, 512], P('sp'), may hold values from -0.125 to 0.125
- down_weight: bfloat16 [8, 512, 2048], P('sp'), may hold values from -0.25 to 0.25
- routes: int32 [8192, 2], P(('sp', 'tp')), may hold values from 0 to 7, as said below
- route_weights: float32 [8192, 2], P(('sp', 'tp')), may hold values from 0.2 to 0.8
Outputs:
- mixed: bfloat16 [8192, 2048], P(('sp', 'tp'))
The draws below stay inside these ranges and needn't reach their ends.
Inputs may be any that keep to these rules, and one draw needn't show every extreme that they name: `doc_ids`: never falls along the positions. `routes`: each aligned block of 256 rows names every expert exactly 64 times; the experts of one row differ and lie in one group of 2 consecutive numbers.
All inputs are finite; a program needn't handle non-finite values.
Results may differ from the reference program's by a relative error of at most 0.012.
Values may be sent and summed in bfloat16 or wider, within the bound.
A program may use at most 128 MiB of HBM per device.

```python
import math
import jax
import jax.numpy as jnp
import numpy as np
from jax import lax

D = 2048
HEADS = 32
KV_HEADS = 8
HD = 64
FF = 512
WINDOW = 128
GROUPS = 4
TOPK = 2
TOKENS = 8192
EXPERTS = 8
GROUP_SIZE = 2
ROWS_HOME = 256
CAP = 64
DOCS = 4
DOC_MOST = 4096
N_TP = 4


def draw_queries(key, part):
    noise = jax.random.truncated_normal(jax.random.fold_in(key, 11), -4.0, 4.0, (TOKENS, HEADS * HD), jnp.float32)
    return noise.astype(jnp.bfloat16)


def draw_key_rows(key, part):
    noise = jax.random.truncated_normal(jax.random.fold_in(key, 12), -4.0, 4.0, (TOKENS, KV_HEADS * HD), jnp.float32)
    return noise.astype(jnp.bfloat16)


def draw_routes(key, part):
    block_total = TOKENS // ROWS_HOME
    half_slots = GROUP_SIZE * CAP // 2

    def one_block(block_key):
        order_key, shuffle_key = jax.random.split(block_key)
        group_keys = jax.random.split(order_key, GROUPS)
        ordering = jax.vmap(lambda group_key: jax.random.permutation(group_key, GROUP_SIZE))(group_keys)
        ordering = ordering.astype(jnp.int32) + (jnp.arange(GROUPS, dtype=jnp.int32) * GROUP_SIZE)[:, None]
        slot_ids = jnp.arange(half_slots, dtype=jnp.int32)
        leading = ordering[:, slot_ids // CAP]
        trailing = ordering[:, (slot_ids + half_slots) // CAP]
        paired = jnp.stack([leading.reshape(-1), trailing.reshape(-1)], axis=1)
        shuffle = jax.random.permutation(shuffle_key, ROWS_HOME)
        return paired[shuffle].astype(jnp.int32)
    blocks = jax.vmap(one_block)(jax.random.split(jax.random.fold_in(key, 77), block_total))
    return blocks.reshape(TOKENS, TOPK)


def levels(key, shape, cuts, low, high):
    gain, own = 1.0, jax.random.fold_in(key, 6)
    for dim, blocks in cuts:
        draws = jnp.exp(jax.random.uniform(jax.random.fold_in(own, dim), (blocks,), jnp.float32, low / len(cuts), high / len(cuts)))
        gain = gain * jnp.repeat(draws, shape[dim] // blocks).reshape([-1 if axis == dim else 1 for axis in range(len(shape))])
    return gain


def split_up(number_of, total, limit, lean):
    portions = [(1 << 20) // math.isqrt(standing ** lean) + 1 for standing in range(2, number_of + 1)]
    rest, counts = total - limit - (number_of - 1), [1] * (number_of - 1)
    while rest > 0:
        candidates = [i for i in range(number_of - 1) if counts[i] < limit]
        whole, remaining = sum([portions[i] for i in candidates]), rest
        for i in candidates:
            extra = min(limit - counts[i], max(1, remaining * portions[i] // whole), rest)
            counts[i] = counts[i] + extra
            rest = rest - extra
    return np.array([limit] + counts)


def uneven(own_key, number_of, total, bound, skew):
    if number_of == 2:
        one = jax.random.randint(own_key, (), max(1, total - bound), min(bound, total - 1) + 1)
        return jnp.stack([one, total - one])
    lengths = jnp.asarray(split_up(number_of, total, bound, skew), jnp.int32)
    pairs = (number_of - 1) // 2
    giver, taker = lengths[1:1 + 2 * pairs:2], lengths[2:2 + 2 * pairs:2]
    margin = jnp.minimum(giver - 1, bound - taker)
    moved = jax.random.randint(jax.random.fold_in(own_key, 1), (pairs,), 0, 1 << 20) % (margin + 1)
    lengths = lengths.at[1:1 + 2 * pairs:2].set(giver - moved).at[2:2 + 2 * pairs:2].set(taker + moved)
    return lengths[jax.random.permutation(jax.random.fold_in(own_key, 2), number_of)]


def normal_values(key, extent, width, most, pieces=(), kind=jnp.bfloat16):
    factor_of = levels(key, extent, pieces, -0.22, 0.18) if pieces else 1.0
    values = jax.random.normal(key, extent, jnp.float32) * width * factor_of
    return jnp.minimum(jnp.maximum(values, -most), most).astype(kind)


def setup_inputs(seed: int = 0) -> dict:
    keys = jax.random.split(jax.random.key(seed), 14)
    queries = draw_queries(jax.random.fold_in(keys[13], 71), 0)
    key_rows = draw_key_rows(jax.random.fold_in(keys[13], 71), 0)
    value_rows = normal_values(keys[2], (TOKENS, KV_HEADS * HD), 1.0, 6.0, ((0, 8), (1, 4)))
    doc_ids = jnp.searchsorted(jnp.cumsum(uneven(keys[3], DOCS, TOKENS, DOC_MOST, 1)), jnp.arange(TOKENS), side="right").astype(jnp.int32)
    sink_logit = jnp.clip(3.0 + 4.0 * jax.random.uniform(keys[4], (HEADS,), jnp.float32) ** levels(keys[4], (HEADS,), ((0, 4),), -0.2, 0.2), 3.0, 7.0)
    residual = normal_values(keys[5], (TOKENS, D), 1.0, 6.0, ((0, 32),))
    out_weight = normal_values(keys[6], (HEADS * HD, D), ((HEADS * HD) ** -0.5 * 10), 3.5, ((0, 4),))
    norm_gain = jnp.clip(1.0 + 0.18 * jax.random.normal(keys[7], (D,), jnp.float32), 0.1, 1.9)
    gate_weight = normal_values(keys[8], (EXPERTS, D, FF), D ** -0.5, 0.125, ((0, 8),))
    up_weight = normal_values(keys[9], (EXPERTS, D, FF), D ** -0.5, 0.125, ((0, 8),))
    down_weight = normal_values(keys[10], (EXPERTS, FF, D), FF ** -0.5, 0.25, ((0, 8),))
    routes = draw_routes(jax.random.fold_in(keys[13], 71), 0)
    route_weights = jnp.clip(0.2 + 0.6 * jax.random.uniform(keys[12], (TOKENS, TOPK), jnp.float32) ** levels(keys[12], (TOKENS, TOPK), ((0, 32),), -0.2, 0.2), 0.2, 0.8)
    return dict(queries=queries, key_rows=key_rows, value_rows=value_rows, doc_ids=doc_ids, sink_logit=sink_logit, residual=residual, out_weight=out_weight, norm_gain=norm_gain, gate_weight=gate_weight, up_weight=up_weight, down_weight=down_weight, routes=routes, route_weights=route_weights)


neg_fill = -1e+30
eps_norm = 1e-06

def reference(queries, key_rows, value_rows, doc_ids, sink_logit, residual, out_weight, norm_gain, gate_weight, up_weight, down_weight, routes, route_weights):
    head_ratio = HEADS // KV_HEADS
    block_rows = 512
    block_total = TOKENS // block_rows
    key_pad = jnp.pad(key_rows, ((WINDOW, WINDOW), (0, 0)))
    value_pad = jnp.pad(value_rows, ((WINDOW, WINDOW), (0, 0)))
    doc_pad = jnp.pad(doc_ids, (WINDOW, WINDOW), constant_values=-1)
    sink_col = sink_logit.astype(jnp.float32).reshape(KV_HEADS, head_ratio)[:, :, None, None]

    def one_block(block_index):
        row_start = (block_index * block_rows).astype(jnp.int32)
        key_count = block_rows + 2 * WINDOW
        query_part = lax.dynamic_slice_in_dim(queries, row_start, block_rows, 0).astype(jnp.float32)
        query_part = query_part.reshape(block_rows, KV_HEADS, head_ratio, HD)
        key_part = lax.dynamic_slice_in_dim(key_pad, row_start, key_count, 0).astype(jnp.float32).reshape(key_count, KV_HEADS, HD)
        value_part = lax.dynamic_slice_in_dim(value_pad, row_start, key_count, 0).astype(jnp.float32).reshape(key_count, KV_HEADS, HD)
        query_docs = lax.dynamic_slice_in_dim(doc_ids, row_start, block_rows, 0)
        key_docs = lax.dynamic_slice_in_dim(doc_pad, row_start, key_count, 0)
        query_pos = row_start + jnp.arange(block_rows, dtype=jnp.int32)
        key_pos = row_start - WINDOW + jnp.arange(key_count, dtype=jnp.int32)
        allowed = (jnp.abs(query_pos[:, None] - key_pos[None, :]) <= WINDOW) & (query_docs[:, None] == key_docs[None, :])
        scores = jnp.einsum('qgrd,kgd->grqk', query_part, key_part) * HD ** (-0.5)
        masked = jnp.where(allowed[None, None], scores, neg_fill)
        row_top = jnp.maximum(lax.optimization_barrier(jnp.max(masked, axis=3, keepdims=True)), sink_col)
        exponent = jnp.where(allowed[None, None], jnp.exp(masked - row_top), 0.0)
        denominator = lax.optimization_barrier(jnp.sum(exponent, axis=3, keepdims=True)) + jnp.exp(sink_col - row_top)
        attn_weight = (exponent / denominator).astype(jnp.bfloat16)
        attended = jnp.einsum('grqk,kgd->qgrd', attn_weight.astype(jnp.float32), value_part)
        return attended.astype(jnp.bfloat16).reshape(block_rows, HEADS * HD)
    attended = lax.map(one_block, jnp.arange(block_total, dtype=jnp.int32)).reshape(TOKENS, HEADS * HD)
    group_cols = HEADS * HD // N_TP
    summed = jnp.zeros((TOKENS, D), jnp.float32)
    for group_index in range(N_TP):
        cols = attended[:, group_index * group_cols:(group_index + 1) * group_cols]
        rows_w = out_weight[group_index * group_cols:(group_index + 1) * group_cols]
        partial_value = jnp.dot(cols, rows_w, preferred_element_type=jnp.float32).astype(jnp.bfloat16)
        partial_value = lax.optimization_barrier(partial_value)
        summed = summed + partial_value.astype(jnp.float32)
    stream = (residual.astype(jnp.float32) + summed).astype(jnp.bfloat16)
    stream_f = stream.astype(jnp.float32)
    scale = lax.rsqrt(lax.optimization_barrier(jnp.mean(stream_f * stream_f, axis=1, keepdims=True)) + eps_norm)
    normed = (stream_f * scale * norm_gain.astype(jnp.float32)[None, :]).astype(jnp.bfloat16)
    flat_routes = routes.reshape(-1)
    flat_weights = route_weights.reshape(-1).astype(jnp.float32)
    per_expert = TOKENS * TOPK // EXPERTS

    def expert_step(accum, inputs):
        expert_id, gate_one, up_one, down_one = inputs
        found = jnp.nonzero(flat_routes == expert_id, size=per_expert)[0].astype(jnp.int32)
        token_index = found // TOPK
        rows = normed[token_index]
        gate_act = jnp.dot(rows, gate_one, preferred_element_type=jnp.float32)
        up_act = jnp.dot(rows, up_one, preferred_element_type=jnp.float32)
        hidden = (jax.nn.silu(gate_act) * up_act).astype(jnp.bfloat16)
        expert_out = jnp.dot(hidden, down_one, preferred_element_type=jnp.float32).astype(jnp.bfloat16)
        accum = accum.at[token_index].add(flat_weights[found][:, None] * expert_out.astype(jnp.float32))
        return (accum, None)
    accum0 = jnp.zeros((TOKENS, D), jnp.float32)
    accum, _ = lax.scan(expert_step, accum0, (jnp.arange(EXPERTS, dtype=jnp.int32), gate_weight, up_weight, down_weight))
    return (stream_f + accum).astype(jnp.bfloat16)
```

```python
import functools

import jax
import jax.numpy as jnp
from jax import lax
from jax.experimental import pallas as pl
from jax.experimental.pallas import tpu as pltpu
from jax.sharding import PartitionSpec as P

HD = 64
WINDOW = 128
GROUPS = 4
CHUNKS = 4
HALVES = 2


neg_fill = -1e30
eps_norm = 1e-06


def extended(block, sides, width):
    for axis, dim in sides:
        count = lax.axis_size(axis)
        forward = [(i, i + 1) for i in range(count - 1)]
        backward = [(target, source) for source, target in forward]
        low = lax.ppermute(
            lax.slice_in_dim(block, block.shape[dim] - width, None, axis=dim), axis, forward
        )
        high = lax.ppermute(lax.slice_in_dim(block, 0, width, axis=dim), axis, backward)
        block = jnp.concatenate([low, block, high], axis=dim)
    return block


def attend(
    query_part,
    key_part,
    value_part,
    query_docs,
    key_docs,
    query_start,
    key_start,
    sink_logit,
    extent,
):
    query_count = query_part.shape[0]
    key_count = key_part.shape[0]
    groups = key_part.shape[1] // HD
    head_ratio = sink_logit.shape[0] // groups
    query_heads = query_part.reshape(query_count, groups, head_ratio, HD)
    key_heads = key_part.reshape(key_count, groups, HD)
    value_heads = value_part.reshape(key_count, groups, HD)
    scores = jnp.einsum(
        "qgrd,kgd->grqk", query_heads, key_heads, preferred_element_type=jnp.float32
    ) * HD ** (-0.5)
    query_pos = query_start + jnp.arange(query_count, dtype=jnp.int32)
    key_pos = key_start + jnp.arange(key_count, dtype=jnp.int32)
    inside = (key_pos >= 0) & (key_pos < extent)
    allowed = (
        (jnp.abs(query_pos[:, None] - key_pos[None, :]) <= WINDOW)
        & (query_docs[:, None] == key_docs[None, :])
        & inside[None, :]
    )
    masked = jnp.where(allowed[None, None], scores, neg_fill)
    sink_col = sink_logit.reshape(groups, head_ratio)[:, :, None, None]
    row_top = jnp.maximum(jnp.max(masked, axis=3, keepdims=True), sink_col)
    exponent = jnp.where(allowed[None, None], jnp.exp(masked - row_top), 0.0)
    denominator = jnp.sum(exponent, axis=3, keepdims=True) + jnp.exp(sink_col - row_top)
    attn_weight = (exponent / denominator).astype(jnp.bfloat16)
    attended = jnp.einsum(
        "grqk,kgd->qgrd", attn_weight, value_heads, preferred_element_type=jnp.float32
    )
    return attended.astype(jnp.bfloat16).reshape(query_count, -1)


def fetch_margins(key_rows, value_rows, doc_float):
    return (
        extended(key_rows, (("sp", 0),), WINDOW),
        extended(value_rows, (("sp", 0),), WINDOW),
        extended(doc_float, (("sp", 0),), WINDOW),
    )


def plane_order(gz):
    return [(gz + 2) % 4, gz, 3 - gz, gz + 1 - 2 * (gz % 2)]


def slots_of(routes, order, cap):
    rows = routes.shape[1]
    f32, bf = jnp.float32, jnp.bfloat16
    group_of = routes[0:1, :] // 2
    sub = lax.broadcasted_iota(jnp.int32, (8, rows), 0)
    wanted = jnp.full((8, rows), -1, jnp.int32)
    for k, plane in enumerate(order):
        wanted = jnp.where(sub == k, plane, wanted)
    one_hot = jnp.where(group_of == wanted, 1.0, 0.0)
    ri = lax.broadcasted_iota(jnp.int32, (rows, rows), 0)
    ci = lax.broadcasted_iota(jnp.int32, (rows, rows), 1)
    above = jnp.where(ri < ci, 1.0, 0.0).astype(bf)
    ranks = jnp.dot(one_hot.astype(bf), above, preferred_element_type=f32)
    base = sub.astype(f32) * cap
    return jnp.sum((ranks + base) * one_hot, axis=0, keepdims=True)


def moe_kernel(
    groups, halves,
    sink_ref, doc_ref, routes_ref, rw_ref, gain_ref,
    q_hbm, k_hbm, v_hbm, res_hbm, w_hbm, gate_hbm, up_hbm, down_hbm,
    out_ref,
    qv, resv, wv, w_mate, kx, vx, dl, dr, dx, att, am_far, am_near, routes_far,
    mixed_att, acc, ysend, yrecv, send, own, peer, comb, ret, hid_own, hid_send, hid_recv,
    wsend, wrecv, fin, gv, uv, dv, dv_mate,
    ls, hs, hr, ms, mr, ys, yr, zs, zr, xs, xr, gs, gr, bs, br, ws, wr, ds, dr_sem,
):
    sp = lax.axis_index("sp")
    tp = lax.axis_index("tp")
    sp_count = lax.axis_size("sp")
    gz, side = sp // 2, sp % 2
    x_mate = {"sp": gz * 2 + 1 - side}
    mate = tp + 1 - 2 * (tp % 2)
    core = tp % 2
    across = (tp + 2) % 4
    mate_across = (mate + 2) % 4
    after = (sp + 1) % sp_count
    before = (sp + sp_count - 1) % sp_count
    order = plane_order(gz)
    here = 1
    away = [k for k in range(groups) if k != here]
    rows, width = out_ref.shape
    cap = rows // groups
    hw = width // halves
    cw = width // 4
    blocks = k_hbm.shape[0]
    home_blocks = blocks // 4
    half = blocks // 2
    kv_heads = k_hbm.shape[2] // HD
    ratio = q_hbm.shape[1] // k_hbm.shape[2]
    heads = q_hbm.shape[1]
    f32, bf = jnp.float32, jnp.bfloat16
    mesh_id = pl.DeviceIdType.MESH

    def remote(src, dst, s_sem, r_sem, where):
        return pltpu.make_async_remote_copy(
            src_ref=src, dst_ref=dst, send_sem=s_sem, recv_sem=r_sem,
            device_id=where, device_id_type=mesh_id,
        )

    def to_plane(k):
        return {"sp": order[k] * 2 + side}

    barrier = pltpu.get_barrier_semaphore()
    partners = [{"sp": after}, {"sp": before}, {"tp": mate}, {"tp": across}, x_mate]
    partners += [to_plane(k) for k in away]
    for where in partners:
        pl.semaphore_signal(barrier, inc=1, device_id=where, device_id_type=mesh_id)
    loads = [
        pltpu.make_async_copy(src, dst, ls.at[i])
        for i, (src, dst) in enumerate((
            (k_hbm, kx.at[pl.ds(1, blocks)]), (v_hbm, vx.at[pl.ds(1, blocks)]), (q_hbm, qv),
            (w_hbm, wv), (res_hbm, resv), (gate_hbm.at[0], gv), (up_hbm.at[0], uv),
            (down_hbm.at[0], dv),
        ))
    ]
    for load in loads:
        load.start()
    for b in range(blocks):
        dx[b + 1] = jnp.broadcast_to(doc_ref[b:b + 1, :].astype(f32), (8, WINDOW))

    slot = slots_of(routes_ref[...], order, cap)
    ri = lax.broadcasted_iota(jnp.int32, (rows, rows), 0)
    ci = lax.broadcasted_iota(jnp.int32, (rows, rows), 1)
    slot_col = jnp.sum(jnp.where(ri == ci, slot, 0.0), axis=1, keepdims=True)
    spread = jnp.where(slot_col == ci.astype(f32), 1.0, 0.0)
    weight_rows = []
    for parity in (side, 1 - side):
        w_row = jnp.where(routes_ref[0:1, :] % 2 == parity, rw_ref[0:1, :], rw_ref[1:2, :])
        w_col = jnp.sum(jnp.where(ri == ci, w_row, 0.0), axis=1, keepdims=True)
        weight_rows.append(jnp.sum(spread * w_col, axis=0, keepdims=True))
    sub8 = lax.broadcasted_iota(jnp.int32, (8, rows), 0)
    wsend[...] = jnp.where(
        sub8 == 0, weight_rows[0], jnp.where(sub8 == 1, weight_rows[1], 0.0)
    )

    loads[0].wait()
    loads[1].wait()
    pl.semaphore_wait(barrier, len(partners))
    pending = []

    def go(copy):
        copy.start()
        pending.append(copy)
        return copy

    halo = [
        go(remote(src, dst, hs.at[i], hr.at[i], {"sp": where}))
        for i, (src, dst, where) in enumerate((
            (kx.at[blocks], kx.at[0], after), (vx.at[blocks], vx.at[0], after),
            (doc_ref, dl, after),
            (kx.at[1], kx.at[blocks + 1], before), (vx.at[1], vx.at[blocks + 1], before),
            (doc_ref, dr, before),
        ))
    ]
    w_copy = go(remote(w_hbm, w_mate, ms.at[0], mr.at[0], {"tp": mate}))
    r_copy = go(remote(routes_ref, routes_far, ms.at[3], mr.at[3], {"tp": across}))
    for k in away:
        go(remote(wsend, wrecv.at[k], ws.at[k], wr.at[k], to_plane(k)))
    ff = dv.shape[0]
    own_half = pl.ds(core * (ff // 2), ff // 2)
    d_copy = go(remote(down_hbm.at[0, own_half], dv_mate.at[own_half], ds.at[0], dr_sem.at[0], x_mate))

    qi = lax.broadcasted_iota(jnp.int32, (WINDOW, 3 * WINDOW), 0)
    ki = lax.broadcasted_iota(jnp.int32, (WINDOW, 3 * WINDOW), 1)
    band = (ki >= qi) & (ki <= qi + 2 * WINDOW)
    eye = lax.broadcasted_iota(jnp.int32, (WINDOW, WINDOW), 0) == lax.broadcasted_iota(
        jnp.int32, (WINDOW, WINDOW), 1
    )

    def attend_block(b):
        own_docs = dx[b + 1][0:1]
        key_docs = jnp.concatenate([dx[b][0:1], own_docs, dx[b + 2][0:1]], axis=1)
        query_docs = jnp.sum(jnp.where(eye, own_docs, 0.0), axis=1, keepdims=True)
        bias = jnp.where(band & (key_docs == query_docs), 0.0, neg_fill)
        keys = kx[pl.ds(b, 3)].reshape(3 * WINDOW, kv_heads * HD)
        values = vx[pl.ds(b, 3)].reshape(3 * WINDOW, kv_heads * HD)
        home = b // home_blocks
        to_rows = pl.ds(pl.multiple_of((b % home_blocks) * WINDOW, WINDOW), WINDOW)
        from_rows = pl.ds(pl.multiple_of(b * WINDOW, WINDOW), WINDOW)
        for g in range(kv_heads):
            span = slice(g * ratio * HD, (g + 1) * ratio * HD)
            q = qv[from_rows, span] * jnp.asarray(HD ** (-0.5), bf)
            stacked = jnp.concatenate([q[:, r * HD:(r + 1) * HD] for r in range(ratio)], axis=0)
            scores = lax.dot_general(
                stacked, keys[:, g * HD:(g + 1) * HD], (((1,), (1,)), ((), ())),
                preferred_element_type=f32,
            )
            vg = values[:, g * HD:(g + 1) * HD]
            parts = []
            for r in range(ratio):
                sink = sink_ref[g * ratio + r]
                s = scores[r * WINDOW:(r + 1) * WINDOW] + bias
                top = jnp.maximum(jnp.max(s, axis=1, keepdims=True), sink)
                e = jnp.exp(s - top)
                den = jnp.sum(e, axis=1, keepdims=True) + jnp.exp(sink - top)
                o = jnp.dot(e.astype(bf), vg, preferred_element_type=f32)
                parts.append((o / den).astype(bf))
            att[home, to_rows, span] = jnp.concatenate(parts, axis=1)

    def far_step(i, carry):
        @pl.when(i == half - 1)
        def _():
            for copy in halo:
                copy.wait_recv()
            left = dl[blocks - 1:blocks, :].astype(f32)
            right = dr[0:1, :].astype(f32)
            left = jnp.where(sp == 0, -1.0, left)
            right = jnp.where(sp == sp_count - 1, -1.0, right)
            dx[0] = jnp.broadcast_to(left, (8, WINDOW))
            dx[blocks + 1] = jnp.broadcast_to(right, (8, WINDOW))

        attend_block(jnp.where(tp < 2, half + i, half - 1 - i))
        return carry

    def pick_of(slot_row):
        return jnp.where(ri.astype(f32) == slot_row, 1.0, 0.0).astype(bf)

    def gather_rows(pick, mine, mates):
        mixed_att[:, :heads] = jnp.dot(pick, mine, preferred_element_type=f32).astype(bf)
        mixed_att[:, heads:] = jnp.dot(pick, mates, preferred_element_type=f32).astype(bf)

    def project(cols):
        part = jnp.dot(mixed_att[:, :heads], wv[:, cols], preferred_element_type=f32)
        return part + jnp.dot(mixed_att[:, heads:], w_mate[:, cols], preferred_element_type=f32)

    loads[2].wait()
    with jax.named_scope("attn_far"):
        lax.fori_loop(0, half, far_step, 0)
    far_copy = go(remote(att.at[mate_across], am_far, ms.at[1], mr.at[1], {"tp": mate}))
    with jax.named_scope("wait_far"):
        r_copy.wait_recv()
        pick_far = pick_of(slots_of(routes_far[...], order, cap))
        loads[3].wait()
        w_copy.wait_recv()
        far_copy.wait_recv()
    with jax.named_scope("far_proj"):
        gather_rows(pick_far, att[across], am_far[...])
        y_copies = {}

        def send_y(k, h):
            y_copies[k, h] = go(remote(
                ysend.at[h, k], yrecv.at[h, k], ys.at[h, k], yr.at[h, k], {"tp": across}
            ))

        per = 4 // halves
        for h in range(halves):
            for c in range(per):
                cols = slice(h * hw + c * cw, h * hw + (c + 1) * cw)
                part = project(cols).astype(bf).reshape(groups, cap, cw)
                ysend[h, :, :, c * cw:(c + 1) * cw] = part
            if h < halves - 1:
                send_y(0, h)
        send_y(0, halves - 1)
        for k in range(1, groups):
            for h in range(halves):
                send_y(k, h)

    def near_step(i, carry):
        attend_block(jnp.where(tp < 2, half - 1 - i, half + i))
        return carry

    with jax.named_scope("attn_near"):
        lax.fori_loop(0, half, near_step, 0)
    near_copy = go(remote(att.at[mate], am_near, ms.at[2], mr.at[2], {"tp": mate}))
    for i in range(4, 8):
        loads[i].wait()
    with jax.named_scope("wait_near"):
        pick = pick_of(slot)
        near_copy.wait_recv()
    with jax.named_scope("near_proj"):
        gather_rows(pick, att[tp], am_near[...])
        for c in range(4):
            cols = slice(c * cw, (c + 1) * cw)
            part = project(cols)
            part += jnp.dot(pick, resv[:, cols], preferred_element_type=f32)
            acc[:, :, cols] = part.reshape(groups, cap, cw)

    def emit(k, h):
        with jax.named_scope("y%d_%d" % (k, h)):
            y_copies[k, h].wait_recv()
        cols = slice(h * hw, (h + 1) * hw)
        piece = (acc[k, :, cols] + yrecv[h, k].astype(f32)).astype(bf)
        send[h, k] = piece
        if k == here:
            own[h, k] = piece
            go(remote(send.at[h, k], peer.at[h, k], xs.at[h, k], xr.at[h, k], x_mate))
        else:
            go(remote(send.at[h, k], own.at[h, k], zs.at[h, k], zr.at[h, k], to_plane(k)))

    def relay(k, h):
        with jax.named_scope("z%d_%d" % (k, h)):
            remote(send.at[h, k], own.at[h, k], zs.at[h, k], zr.at[h, k], x_mate).wait_recv()
        go(remote(own.at[h, k], peer.at[h, k], xs.at[h, k], xr.at[h, k], x_mate))

    def hidden_of(buf, k):
        squares = gate_act = up_act = 0.0
        for h in range(halves):
            span = slice(h * hw, (h + 1) * hw)
            wide = buf[h, k].astype(f32)
            squares = squares + jnp.sum(wide * wide, axis=1, keepdims=True)
            block = (wide * gain_ref[:, span]).astype(bf)
            gate_act = gate_act + jnp.dot(block, gv[span, :], preferred_element_type=f32)
            up_act = up_act + jnp.dot(block, uv[span, :], preferred_element_type=f32)
        scale = lax.rsqrt(squares / width + eps_norm)
        g = gate_act * scale
        return (g / (1.0 + jnp.exp(-g)) * (up_act * scale)).astype(bf)

    def expert_own(k):
        with jax.named_scope("own%d" % k):
            hid_own[k] = hidden_of(own, k)

    def expert_peer(k):
        with jax.named_scope("x%d" % k):
            for h in range(halves):
                remote(own.at[h, k], peer.at[h, k], xs.at[h, k], xr.at[h, k], x_mate).wait_recv()
        with jax.named_scope("peer%d" % k):
            hid_send[k] = hidden_of(peer, k)
            go(remote(hid_send.at[k], hid_recv.at[k], gs.at[k], gr.at[k], x_mate))

    sub_c = lax.broadcasted_iota(jnp.int32, (cap, rows), 0)
    lane_c = lax.broadcasted_iota(jnp.int32, (cap, rows), 1)

    def combine(k):
        with jax.named_scope("hid%d" % k):
            remote(hid_send.at[k], hid_recv.at[k], gs.at[k], gr.at[k], x_mate).wait_recv()
            if k == here:
                table = wsend[...]
            else:
                remote(wsend, wrecv.at[k], ws.at[k], wr.at[k], x_mate).wait_recv()
                table = wrecv[k]
        with jax.named_scope("down%d" % k):
            chosen = lane_c == sub_c + k * cap
            w_own = jnp.sum(jnp.where(chosen, table[0:1, :], 0.0), axis=1, keepdims=True)
            w_peer = jnp.sum(jnp.where(chosen, table[1:2, :], 0.0), axis=1, keepdims=True)
            mine, theirs = hid_own[k], hid_recv[k]
            for h in range(halves):
                for c in range(per):
                    cols = slice(h * hw + c * cw, h * hw + (c + 1) * cw)
                    total = jnp.dot(mine, dv[:, cols], preferred_element_type=f32) * w_own
                    total += jnp.dot(theirs, dv_mate[:, cols], preferred_element_type=f32) * w_peer
                    comb[h, k, :, c * cw:(c + 1) * cw] = total.astype(bf)
                if k != here:
                    go(remote(comb.at[h, k], ret.at[h, k], bs.at[h, k], br.at[h, k], to_plane(k)))

    def finish(k, h):
        if k == here:
            back = comb[h, k]
        else:
            with jax.named_scope("r%d_%d" % (k, h)):
                remote(comb.at[h, k], ret.at[h, k], bs.at[h, k], br.at[h, k], x_mate).wait_recv()
            back = ret[h, k]
        total = send[h, k].astype(f32) + back.astype(f32)
        fin[k * cap:(k + 1) * cap, h * hw:(h + 1) * hw] = total.astype(bf)

    hs_all = range(halves)
    for k in (0, here):
        for h in hs_all:
            emit(k, h)
    with jax.named_scope("dmate"):
        d_copy.wait_recv()
    d_fwd = go(remote(
        dv_mate.at[own_half], dv_mate.at[own_half], ds.at[1], dr_sem.at[1], {"tp": mate}
    ))
    expert_own(here)
    for h in hs_all[:-1]:
        relay(0, h)
    for h in hs_all:
        emit(2, h)
    relay(0, halves - 1)
    expert_own(0)
    expert_peer(here)
    for h in hs_all:
        emit(3, h)
    d_fwd.wait_recv()
    combine(here)
    expert_peer(0)
    combine(0)
    for k in (3, 2):
        for h in hs_all:
            relay(k, h)
        expert_own(k)
    for k in (3, 2):
        expert_peer(k)
    for k in (3, 2):
        combine(k)
    for k in (here, 0, 3, 2):
        for h in hs_all:
            finish(k, h)
    with jax.named_scope("out"):
        spread_b = spread.astype(bf)
        for c in range(4):
            cols = slice(c * cw, (c + 1) * cw)
            out_ref[:, cols] = jnp.dot(
                spread_b, fin[:, cols], preferred_element_type=f32
            ).astype(bf)
    with jax.named_scope("sends"):
        for copy in pending:
            copy.wait_send()


def front_kernel(
    chunks, extra, entered, emit,
    sink_ref, q_ref, k_ref, v_ref, doc_ref, res_ref, w_ref,
    out_ref,
    kx, vx, dl, dr, dx, att, am_far, am_near, w_mate, acc, ysend, yrecv,
    hs, hr, ms, mr, ys, yr,
):
    sp = lax.axis_index("sp")
    tp = lax.axis_index("tp")
    sp_count = lax.axis_size("sp")
    mate = tp + 1 - 2 * (tp % 2)
    across = (tp + 2) % 4
    mate_across = (mate + 2) % 4
    after = (sp + 1) % sp_count
    before = (sp + sp_count - 1) % sp_count
    blocks = q_ref.shape[0] // WINDOW
    home_blocks = blocks // 4
    half = blocks // 2
    kv_heads = k_ref.shape[1] // HD
    ratio = q_ref.shape[1] // k_ref.shape[1]
    width = out_ref.shape[1]
    cw = width // chunks
    f32, bf = jnp.float32, jnp.bfloat16
    mesh_id = pl.DeviceIdType.MESH

    def remote(src, dst, ss, rs, where):
        return pltpu.make_async_remote_copy(
            src_ref=src, dst_ref=dst, send_sem=ss, recv_sem=rs,
            device_id=where, device_id_type=mesh_id,
        )

    barrier = pltpu.get_barrier_semaphore()
    for where in ({"sp": after}, {"sp": before}, {"tp": mate}, {"tp": across}):
        pl.semaphore_signal(barrier, inc=1, device_id=where, device_id_type=mesh_id)
    for b in range(blocks):
        kx[b + 1] = k_ref[b * WINDOW:(b + 1) * WINDOW, :]
        vx[b + 1] = v_ref[b * WINDOW:(b + 1) * WINDOW, :]
        dx[b + 1] = jnp.broadcast_to(doc_ref[b:b + 1, :].astype(f32), (8, WINDOW))
    pl.semaphore_wait(barrier, 4 + extra)

    tail = pl.ds((blocks - 1) * WINDOW, WINDOW)
    lead = pl.ds(0, WINDOW)
    halo = [
        remote(k_ref.at[tail], kx.at[0], hs.at[0], hr.at[0], {"sp": after}),
        remote(v_ref.at[tail], vx.at[0], hs.at[1], hr.at[1], {"sp": after}),
        remote(doc_ref, dl, hs.at[2], hr.at[2], {"sp": after}),
        remote(k_ref.at[lead], kx.at[blocks + 1], hs.at[3], hr.at[3], {"sp": before}),
        remote(v_ref.at[lead], vx.at[blocks + 1], hs.at[4], hr.at[4], {"sp": before}),
        remote(doc_ref, dr, hs.at[5], hr.at[5], {"sp": before}),
    ]
    for copy in halo:
        copy.start()
    w_copy = remote(w_ref, w_mate, ms.at[0], mr.at[0], {"tp": mate})
    w_copy.start()
    if entered is not None:
        entered()

    qi = lax.broadcasted_iota(jnp.int32, (WINDOW, 3 * WINDOW), 0)
    ki = lax.broadcasted_iota(jnp.int32, (WINDOW, 3 * WINDOW), 1)
    band = (ki >= qi) & (ki <= qi + 2 * WINDOW)
    eye = lax.broadcasted_iota(jnp.int32, (WINDOW, WINDOW), 0) == lax.broadcasted_iota(
        jnp.int32, (WINDOW, WINDOW), 1
    )

    def attend_block(b):
        own_docs = dx[b + 1][0:1]
        key_docs = jnp.concatenate([dx[b][0:1], own_docs, dx[b + 2][0:1]], axis=1)
        query_docs = jnp.sum(jnp.where(eye, own_docs, 0.0), axis=1, keepdims=True)
        bias = jnp.where(band & (key_docs == query_docs), 0.0, neg_fill)
        keys = kx[pl.ds(b, 3)].reshape(3 * WINDOW, kv_heads * HD)
        values = vx[pl.ds(b, 3)].reshape(3 * WINDOW, kv_heads * HD)
        home = b // home_blocks
        to_rows = pl.ds(pl.multiple_of((b % home_blocks) * WINDOW, WINDOW), WINDOW)
        from_rows = pl.ds(pl.multiple_of(b * WINDOW, WINDOW), WINDOW)
        for g in range(kv_heads):
            span = slice(g * ratio * HD, (g + 1) * ratio * HD)
            q = q_ref[from_rows, span] * jnp.asarray(HD ** (-0.5), bf)
            stacked = jnp.concatenate([q[:, r * HD:(r + 1) * HD] for r in range(ratio)], axis=0)
            scores = lax.dot_general(
                stacked, keys[:, g * HD:(g + 1) * HD], (((1,), (1,)), ((), ())),
                preferred_element_type=f32,
            )
            vg = values[:, g * HD:(g + 1) * HD]
            parts = []
            for r in range(ratio):
                sink = sink_ref[g * ratio + r]
                s = scores[r * WINDOW:(r + 1) * WINDOW] + bias
                top = jnp.maximum(jnp.max(s, axis=1, keepdims=True), sink)
                e = jnp.exp(s - top)
                den = jnp.sum(e, axis=1, keepdims=True) + jnp.exp(sink - top)
                o = jnp.dot(e.astype(bf), vg, preferred_element_type=f32)
                parts.append((o / den).astype(bf))
            att[home, to_rows, span] = jnp.concatenate(parts, axis=1)

    def far_step(i, carry):
        @pl.when(i == half - 1)
        def _():
            for copy in halo:
                copy.wait_recv()
            left = dl[blocks - 1:blocks, :].astype(f32)
            right = dr[0:1, :].astype(f32)
            left = jnp.where(sp == 0, -1.0, left)
            right = jnp.where(sp == sp_count - 1, -1.0, right)
            dx[0] = jnp.broadcast_to(left, (8, WINDOW))
            dx[blocks + 1] = jnp.broadcast_to(right, (8, WINDOW))

        attend_block(jnp.where(tp < 2, half + i, half - 1 - i))
        return carry

    lax.fori_loop(0, half, far_step, 0)
    far_copy = remote(att.at[mate_across], am_far, ms.at[1], mr.at[1], {"tp": mate})
    far_copy.start()
    w_copy.wait_recv()
    far_copy.wait_recv()
    sent = []
    for c in range(chunks):
        cols = slice(c * cw, (c + 1) * cw)
        part = jnp.dot(att[across], w_ref[:, cols], preferred_element_type=f32)
        part += jnp.dot(am_far[...], w_mate[:, cols], preferred_element_type=f32)
        ysend[c] = part.astype(bf)
        copy = remote(ysend.at[c], yrecv.at[c], ys.at[c], yr.at[c], {"tp": across})
        copy.start()
        sent.append(copy)

    def near_step(i, carry):
        attend_block(jnp.where(tp < 2, half - 1 - i, half + i))
        return carry

    lax.fori_loop(0, half, near_step, 0)
    near_copy = remote(att.at[mate], am_near, ms.at[2], mr.at[2], {"tp": mate})
    near_copy.start()
    near_copy.wait_recv()
    for c in range(chunks):
        cols = slice(c * cw, (c + 1) * cw)
        part = jnp.dot(att[tp], w_ref[:, cols], preferred_element_type=f32)
        part += jnp.dot(am_near[...], w_mate[:, cols], preferred_element_type=f32)
        acc[:, cols] = part + res_ref[:, cols].astype(f32)
    for c in range(chunks):
        cols = slice(c * cw, (c + 1) * cw)
        sent[c].wait_recv()
        out_ref[:, cols] = (acc[:, cols] + yrecv[c].astype(f32)).astype(bf)
        if emit is not None:
            emit(c)
    for copy in halo + [w_copy, far_copy, near_copy] + sent:
        copy.wait_send()


def front_scratch(queries, key_rows, residual, out_weight):
    rows, width = residual.shape
    local, heads_width = queries.shape
    kv_width = key_rows.shape[1]
    blocks = local // WINDOW
    bf, f32 = jnp.bfloat16, jnp.float32
    dma = pltpu.SemaphoreType.DMA
    return [
            pltpu.VMEM((blocks + 2, WINDOW, kv_width), bf),
            pltpu.VMEM((blocks + 2, WINDOW, kv_width), bf),
            pltpu.VMEM((blocks, WINDOW), jnp.int32),
            pltpu.VMEM((blocks, WINDOW), jnp.int32),
            pltpu.VMEM((blocks + 2, 8, WINDOW), f32),
            pltpu.VMEM((4, rows, heads_width), bf),
            pltpu.VMEM((rows, heads_width), bf),
            pltpu.VMEM((rows, heads_width), bf),
            pltpu.VMEM(out_weight.shape, bf),
            pltpu.VMEM((rows, width), f32),
            pltpu.VMEM((CHUNKS, rows, width // CHUNKS), bf),
            pltpu.VMEM((CHUNKS, rows, width // CHUNKS), bf),
            dma((6,)), dma((6,)), dma((3,)), dma((3,)), dma((CHUNKS,)), dma((CHUNKS,)),
    ]


def front(queries, key_rows, value_rows, doc_ids, sink_logit, residual, out_weight):
    rows, width = residual.shape
    local, heads_width = queries.shape
    kv_width = key_rows.shape[1]
    blocks = local // WINDOW
    bf, f32 = jnp.bfloat16, jnp.float32
    dma = pltpu.SemaphoreType.DMA
    vm = pl.BlockSpec(memory_space=pltpu.VMEM)
    docs = doc_ids.reshape(blocks, WINDOW)
    return pl.pallas_call(
        functools.partial(front_kernel, CHUNKS, 0, None, None),
        out_shape=jax.ShapeDtypeStruct((rows, width), bf),
        in_specs=[pl.BlockSpec(memory_space=pltpu.SMEM)] + [vm] * 6,
        out_specs=vm,
        scratch_shapes=front_scratch(queries, key_rows, residual, out_weight),
        compiler_params=pltpu.CompilerParams(
            collective_id=4, has_side_effects=True, vmem_limit_bytes=48 * 1024 * 1024
        ),
        name="front",
    )(sink_logit, queries, key_rows, value_rows, docs, residual, out_weight)


def pair_routed(routes, gate_weight):
    count = lax.axis_size("sp")
    experts = count * gate_weight.shape[0]
    return (
        gate_weight.shape[0] == 1
        and routes.shape[1] == 2
        and experts == 2 * GROUPS
    )


def mixture(
    queries, key_rows, value_rows, doc_ids, sink_logit, residual, out_weight,
    norm_gain, routes, route_weights, gate_weight, up_weight, down_weight,
):
    rows, width = residual.shape
    blocks = queries.shape[0] // WINDOW
    heads = queries.shape[1]
    kv_width = key_rows.shape[1]
    docs = doc_ids.reshape(blocks, WINDOW)
    ff = gate_weight.shape[2]
    groups = lax.axis_size("sp") // 2
    cap, hw = rows // groups, width // HALVES
    bf, f32, i32 = jnp.bfloat16, jnp.float32, jnp.int32
    pieces = pltpu.VMEM((HALVES, groups, cap, hw), bf)
    hidden = pltpu.VMEM((groups, cap, ff), bf)
    dma = pltpu.SemaphoreType.DMA
    vm = pl.BlockSpec(memory_space=pltpu.VMEM)
    hbm = pl.BlockSpec(memory_space=pl.ANY)
    edge = pltpu.VMEM((blocks + 2, WINDOW, kv_width), bf)
    per_piece = dma((HALVES, groups))
    return pl.pallas_call(
        functools.partial(moe_kernel, groups, HALVES),
        out_shape=jax.ShapeDtypeStruct((rows, width), bf),
        in_specs=[pl.BlockSpec(memory_space=pltpu.SMEM)] + [vm] * 4 + [hbm] * 8,
        out_specs=vm,
        scratch_shapes=[
            pltpu.VMEM(queries.shape, bf), pltpu.VMEM((rows, width), bf),
            pltpu.VMEM(out_weight.shape, bf), pltpu.VMEM(out_weight.shape, bf),
            edge, edge,
            pltpu.VMEM((blocks, WINDOW), i32), pltpu.VMEM((blocks, WINDOW), i32),
            pltpu.VMEM((blocks + 2, 8, WINDOW), f32),
            pltpu.VMEM((4, rows, heads), bf),
            pltpu.VMEM((rows, heads), bf), pltpu.VMEM((rows, heads), bf),
            pltpu.VMEM(routes.shape[::-1], i32),
            pltpu.VMEM((rows, 2 * heads), bf),
            pltpu.VMEM((groups, cap, width), f32),
            pieces, pieces, pieces, pieces, pieces, pieces, pieces,
            hidden, hidden, hidden,
            pltpu.VMEM((8, rows), f32), pltpu.VMEM((groups, 8, rows), f32),
            pltpu.VMEM((rows, width), bf),
            pltpu.VMEM((width, ff), bf), pltpu.VMEM((width, ff), bf),
            pltpu.VMEM((ff, width), bf), pltpu.VMEM((ff, width), bf),
            dma((8,)), dma((6,)), dma((6,)), dma((4,)), dma((4,)),
            per_piece, per_piece, per_piece, per_piece, per_piece, per_piece,
            dma((groups,)), dma((groups,)), per_piece, per_piece,
            dma((groups,)), dma((groups,)), dma((2,)), dma((2,)),
        ],
        compiler_params=pltpu.CompilerParams(
            collective_id=3, has_side_effects=True, vmem_limit_bytes=56 * 1024 * 1024
        ),
        name="mixture",
    )(
        sink_logit, docs, routes.T, route_weights.T, norm_gain[None, :],
        queries, key_rows.reshape(blocks, WINDOW, kv_width),
        value_rows.reshape(blocks, WINDOW, kv_width), residual, out_weight,
        gate_weight, up_weight, down_weight,
    )


def fits_front(queries):
    return lax.axis_size("tp") == 4 and queries.shape[0] % (8 * WINDOW) == 0


def stream_of(
    queries, key_rows, value_rows, doc_ids, sink_logit, residual, out_weight
):
    local_rows = queries.shape[0]
    if fits_front(queries):
        return front(queries, key_rows, value_rows, doc_ids, sink_logit, residual, out_weight)
    anchor = lax.axis_index("sp") * local_rows
    extent = local_rows * lax.axis_size("sp")
    doc_float = doc_ids.astype(jnp.bfloat16)
    block_rows = min(512, local_rows)
    padded_keys, padded_values, padded_docs = fetch_margins(key_rows, value_rows, doc_float)
    block_parts = []
    for row_start in range(0, local_rows, block_rows):
        key_end = row_start + block_rows + 2 * WINDOW
        block_parts.append(
            attend(
                queries[row_start : row_start + block_rows],
                padded_keys[row_start:key_end],
                padded_values[row_start:key_end],
                doc_float[row_start : row_start + block_rows],
                padded_docs[row_start:key_end],
                anchor + row_start,
                anchor + row_start - WINDOW,
                sink_logit,
                extent,
            )
        )
    attended = jnp.concatenate(block_parts, axis=0)
    regrouped = lax.all_to_all(attended, "tp", split_axis=0, concat_axis=1, tiled=True)
    shard_rows = out_weight.shape[0]
    initial = jnp.zeros((regrouped.shape[0], out_weight.shape[1]), jnp.float32)
    running = initial
    weight_piece = lax.all_gather(out_weight, "tp", axis=0, tiled=True)
    for shard_index in range(weight_piece.shape[0] // shard_rows):
        columns = lax.dynamic_slice_in_dim(regrouped, shard_index * shard_rows, shard_rows, 1)
        partial_value = jnp.dot(
            columns,
            weight_piece[shard_index * shard_rows : (shard_index + 1) * shard_rows],
            preferred_element_type=jnp.float32,
        )
        running = running + partial_value.astype(jnp.bfloat16).astype(jnp.float32)
    stream = (residual.astype(jnp.float32) + running).astype(jnp.bfloat16)
    return stream


def per_device(
    queries,
    key_rows,
    value_rows,
    doc_ids,
    sink_logit,
    residual,
    out_weight,
    norm_gain,
    gate_weight,
    up_weight,
    down_weight,
    routes,
    route_weights,
):
    front_args = (
        queries, key_rows, value_rows, doc_ids, sink_logit, residual, out_weight
    )
    if pair_routed(routes, gate_weight) and fits_front(queries):
        return mixture(
            *front_args, norm_gain, routes, route_weights, gate_weight, up_weight, down_weight
        )
    stream = stream_of(*front_args)
    stream_f = stream.astype(jnp.float32)
    scale = lax.rsqrt(jnp.mean(stream_f * stream_f, axis=1, keepdims=True) + eps_norm)
    normed = (stream_f * scale * norm_gain[None, :]).astype(jnp.bfloat16)
    home_rows = normed.shape[0]
    width = normed.shape[1]
    route_count = routes.shape[1]
    expert_count = lax.axis_size("sp") * gate_weight.shape[0]
    capacity = route_count * home_rows // expert_count
    flat_routes = routes.reshape(-1)
    one_hot = (flat_routes[:, None] == jnp.arange(expert_count, dtype=jnp.int32)[None, :]).astype(
        jnp.int32
    )
    earlier = jnp.cumsum(one_hot, axis=0) - one_hot
    slot_rank = jnp.sum(earlier * one_hot, axis=1)
    slot_index = flat_routes * capacity + slot_rank
    source_row = (
        jnp.zeros((expert_count * capacity,), jnp.int32)
        .at[slot_index]
        .set(jnp.arange(home_rows * route_count, dtype=jnp.int32) // route_count)
    )
    outgoing = normed[source_row].reshape(expert_count, capacity, width)
    incoming = lax.all_to_all(outgoing, "sp", split_axis=0, concat_axis=0, tiled=True)
    flat_rows = incoming.reshape(-1, width)
    gate_act = jnp.dot(flat_rows, gate_weight[0], preferred_element_type=jnp.float32)
    up_act = jnp.dot(flat_rows, up_weight[0], preferred_element_type=jnp.float32)
    hidden = (jax.nn.silu(gate_act) * up_act).astype(jnp.bfloat16)
    produced = jnp.dot(hidden, down_weight[0], preferred_element_type=jnp.float32).astype(
        jnp.bfloat16
    )
    returned = lax.all_to_all(
        produced.reshape(incoming.shape), "sp", split_axis=0, concat_axis=0, tiled=True
    )
    route_out = returned.reshape(-1, width)[slot_index].reshape(home_rows, route_count, width)
    weighted = jnp.sum(route_weights[:, :, None] * route_out.astype(jnp.float32), axis=1)
    return (stream_f + weighted).astype(jnp.bfloat16)


def solution(mesh):
    return jax.shard_map(
        per_device,
        mesh=mesh,
        in_specs=(
            P("sp", "tp"),
            P("sp", "tp"),
            P("sp", "tp"),
            P("sp"),
            P("tp"),
            P(("sp", "tp"), None),
            P("tp", None),
            P(),
            P("sp", None, None),
            P("sp", None, None),
            P("sp", None, None),
            P(("sp", "tp"), None),
            P(("sp", "tp"), None),
        ),
        out_specs=P(("sp", "tp"), None),
        check_vma=False,
    )
```

```python
import functools

import jax
import jax.numpy as jnp
from jax import lax
from jax.experimental import pallas as pl
from jax.experimental.pallas import tpu as pltpu
from jax.sharding import PartitionSpec as P

HD = 64
WINDOW = 128
GROUPS = 4
CHUNKS = 4
HALVES = 2


neg_fill = -1e30
eps_norm = 1e-06


def extended(block, sides, width):
    for axis, dim in sides:
        count = lax.axis_size(axis)
        forward = [(i, i + 1) for i in range(count - 1)]
        backward = [(target, source) for source, target in forward]
        low = lax.ppermute(
            lax.slice_in_dim(block, block.shape[dim] - width, None, axis=dim), axis, forward
        )
        high = lax.ppermute(lax.slice_in_dim(block, 0, width, axis=dim), axis, backward)
        block = jnp.concatenate([low, block, high], axis=dim)
    return block


def attend(
    query_part,
    key_part,
    value_part,
    query_docs,
    key_docs,
    query_start,
    key_start,
    sink_logit,
    extent,
):
    query_count = query_part.shape[0]
    key_count = key_part.shape[0]
    groups = key_part.shape[1] // HD
    head_ratio = sink_logit.shape[0] // groups
    query_heads = query_part.reshape(query_count, groups, head_ratio, HD)
    key_heads = key_part.reshape(key_count, groups, HD)
    value_heads = value_part.reshape(key_count, groups, HD)
    scores = jnp.einsum(
        "qgrd,kgd->grqk", query_heads, key_heads, preferred_element_type=jnp.float32
    ) * HD ** (-0.5)
    query_pos = query_start + jnp.arange(query_count, dtype=jnp.int32)
    key_pos = key_start + jnp.arange(key_count, dtype=jnp.int32)
    inside = (key_pos >= 0) & (key_pos < extent)
    allowed = (
        (jnp.abs(query_pos[:, None] - key_pos[None, :]) <= WINDOW)
        & (query_docs[:, None] == key_docs[None, :])
        & inside[None, :]
    )
    masked = jnp.where(allowed[None, None], scores, neg_fill)
    sink_col = sink_logit.reshape(groups, head_ratio)[:, :, None, None]
    row_top = jnp.maximum(jnp.max(masked, axis=3, keepdims=True), sink_col)
    exponent = jnp.where(allowed[None, None], jnp.exp(masked - row_top), 0.0)
    denominator = jnp.sum(exponent, axis=3, keepdims=True) + jnp.exp(sink_col - row_top)
    attn_weight = (exponent / denominator).astype(jnp.bfloat16)
    attended = jnp.einsum(
        "grqk,kgd->qgrd", attn_weight, value_heads, preferred_element_type=jnp.float32
    )
    return attended.astype(jnp.bfloat16).reshape(query_count, -1)


def fetch_margins(key_rows, value_rows, doc_float):
    return (
        extended(key_rows, (("sp", 0),), WINDOW),
        extended(value_rows, (("sp", 0),), WINDOW),
        extended(doc_float, (("sp", 0),), WINDOW),
    )


def plane_order(gz):
    return [(gz + 2) % 4, 3 - gz, gz + 1 - 2 * (gz % 2), gz]


def slots_of(routes, order, cap):
    rows = routes.shape[1]
    f32, bf = jnp.float32, jnp.bfloat16
    group_of = routes[0:1, :] // 2
    sub = lax.broadcasted_iota(jnp.int32, (8, rows), 0)
    wanted = jnp.full((8, rows), -1, jnp.int32)
    for k, plane in enumerate(order):
        wanted = jnp.where(sub == k, plane, wanted)
    one_hot = jnp.where(group_of == wanted, 1.0, 0.0)
    ri = lax.broadcasted_iota(jnp.int32, (rows, rows), 0)
    ci = lax.broadcasted_iota(jnp.int32, (rows, rows), 1)
    above = jnp.where(ri < ci, 1.0, 0.0).astype(bf)
    ranks = jnp.dot(one_hot.astype(bf), above, preferred_element_type=f32)
    base = sub.astype(f32) * cap
    return jnp.sum((ranks + base) * one_hot, axis=0, keepdims=True)


def moe_kernel(
    groups, halves,
    sink_ref, doc_ref, routes_ref, rw_ref, gain_ref,
    q_hbm, k_hbm, v_hbm, res_hbm, w_hbm, gate_hbm, up_hbm, down_hbm,
    out_ref,
    qv, resv, wv, w_mate, kx, vx, dl, dr, dx, att, am_far, am_near, routes_far,
    mixed_att, acc, ysend, yrecv, send, own, peer, comb, ret, hid_own, hid_send, hid_recv,
    wsend, wrecv, fin, gv, uv, dv, dv_mate,
    ls, hs, hr, ms, mr, ys, yr, zs, zr, xs, xr, gs, gr, bs, br, ws, wr, ds, dr_sem,
):
    sp = lax.axis_index("sp")
    tp = lax.axis_index("tp")
    sp_count = lax.axis_size("sp")
    gz, side = sp // 2, sp % 2
    x_mate = {"sp": gz * 2 + 1 - side}
    mate = tp + 1 - 2 * (tp % 2)
    core = tp % 2
    across = (tp + 2) % 4
    mate_across = (mate + 2) % 4
    after = (sp + 1) % sp_count
    before = (sp + sp_count - 1) % sp_count
    order = plane_order(gz)
    here = groups - 1
    away = [k for k in range(groups) if k != here]
    rows, width = out_ref.shape
    cap = rows // groups
    hw = width // halves
    cw = width // 4
    blocks = k_hbm.shape[0]
    home_blocks = blocks // 4
    half = blocks // 2
    kv_heads = k_hbm.shape[2] // HD
    ratio = q_hbm.shape[1] // k_hbm.shape[2]
    heads = q_hbm.shape[1]
    f32, bf = jnp.float32, jnp.bfloat16
    mesh_id = pl.DeviceIdType.MESH

    def remote(src, dst, s_sem, r_sem, where):
        return pltpu.make_async_remote_copy(
            src_ref=src, dst_ref=dst, send_sem=s_sem, recv_sem=r_sem,
            device_id=where, device_id_type=mesh_id,
        )

    end = (gz == 0) | (gz == groups - 1)

    def pick_one(at_end, at_middle):
        return at_end if at_end == at_middle else jnp.where(end, at_end, at_middle)

    emit_order = [pick_one(a, b) for a, b in ((0, 2), (1, 3), (2, 0), (3, 1))]
    serve_order = [pick_one(a, b) for a, b in ((2, 0), (1, 3), (0, 2), (3, 1))]

    def to_plane(k):
        plane = order[3]
        for i in range(groups - 1):
            plane = jnp.where(k == i, order[i], plane)
        return {"sp": plane * 2 + side}

    barrier = pltpu.get_barrier_semaphore()
    partners = [{"sp": after}, {"sp": before}, {"tp": mate}, {"tp": across}, x_mate]
    partners += [to_plane(k) for k in away]
    for where in partners:
        pl.semaphore_signal(barrier, inc=1, device_id=where, device_id_type=mesh_id)
    loads = [
        pltpu.make_async_copy(src, dst, ls.at[i])
        for i, (src, dst) in enumerate((
            (k_hbm, kx.at[pl.ds(1, blocks)]), (v_hbm, vx.at[pl.ds(1, blocks)]), (q_hbm, qv),
            (w_hbm, wv), (res_hbm, resv), (gate_hbm.at[0], gv), (up_hbm.at[0], uv),
            (down_hbm.at[0], dv),
        ))
    ]
    for load in loads:
        load.start()
    for b in range(blocks):
        dx[b + 1] = jnp.broadcast_to(doc_ref[b:b + 1, :].astype(f32), (8, WINDOW))

    slot = slots_of(routes_ref[...], order, cap)
    ri = lax.broadcasted_iota(jnp.int32, (rows, rows), 0)
    ci = lax.broadcasted_iota(jnp.int32, (rows, rows), 1)
    slot_col = jnp.sum(jnp.where(ri == ci, slot, 0.0), axis=1, keepdims=True)
    spread = jnp.where(slot_col == ci.astype(f32), 1.0, 0.0)
    weight_rows = []
    for parity in (side, 1 - side):
        w_row = jnp.where(routes_ref[0:1, :] % 2 == parity, rw_ref[0:1, :], rw_ref[1:2, :])
        w_col = jnp.sum(jnp.where(ri == ci, w_row, 0.0), axis=1, keepdims=True)
        weight_rows.append(jnp.sum(spread * w_col, axis=0, keepdims=True))
    sub8 = lax.broadcasted_iota(jnp.int32, (8, rows), 0)
    wsend[...] = jnp.where(
        sub8 == 0, weight_rows[0], jnp.where(sub8 == 1, weight_rows[1], 0.0)
    )

    wrecv[here] = wsend[...]

    loads[0].wait()
    loads[1].wait()
    pl.semaphore_wait(barrier, len(partners))
    pending = []

    def go(copy):
        copy.start()
        pending.append(copy)
        return copy

    halo = [
        go(remote(src, dst, hs.at[i], hr.at[i], {"sp": where}))
        for i, (src, dst, where) in enumerate((
            (kx.at[blocks], kx.at[0], after), (vx.at[blocks], vx.at[0], after),
            (doc_ref, dl, after),
            (kx.at[1], kx.at[blocks + 1], before), (vx.at[1], vx.at[blocks + 1], before),
            (doc_ref, dr, before),
        ))
    ]
    w_copy = go(remote(w_hbm, w_mate, ms.at[0], mr.at[0], {"tp": mate}))
    r_copy = go(remote(routes_ref, routes_far, ms.at[3], mr.at[3], {"tp": across}))
    for k in away:
        go(remote(wsend, wrecv.at[k], ws.at[k], wr.at[k], to_plane(k)))
    ff = dv.shape[0]
    own_half = pl.ds(core * (ff // 2), ff // 2)
    d_copy = go(remote(down_hbm.at[0, own_half], dv_mate.at[own_half], ds.at[0], dr_sem.at[0], x_mate))

    qi = lax.broadcasted_iota(jnp.int32, (WINDOW, 3 * WINDOW), 0)
    ki = lax.broadcasted_iota(jnp.int32, (WINDOW, 3 * WINDOW), 1)
    band = (ki >= qi) & (ki <= qi + 2 * WINDOW)
    eye = lax.broadcasted_iota(jnp.int32, (WINDOW, WINDOW), 0) == lax.broadcasted_iota(
        jnp.int32, (WINDOW, WINDOW), 1
    )

    def attend_block(b):
        own_docs = dx[b + 1][0:1]
        key_docs = jnp.concatenate([dx[b][0:1], own_docs, dx[b + 2][0:1]], axis=1)
        query_docs = jnp.sum(jnp.where(eye, own_docs, 0.0), axis=1, keepdims=True)
        bias = jnp.where(band & (key_docs == query_docs), 0.0, neg_fill)
        keys = kx[pl.ds(b, 3)].reshape(3 * WINDOW, kv_heads * HD)
        values = vx[pl.ds(b, 3)].reshape(3 * WINDOW, kv_heads * HD)
        home = b // home_blocks
        to_rows = pl.ds(pl.multiple_of((b % home_blocks) * WINDOW, WINDOW), WINDOW)
        from_rows = pl.ds(pl.multiple_of(b * WINDOW, WINDOW), WINDOW)
        for g in range(kv_heads):
            span = slice(g * ratio * HD, (g + 1) * ratio * HD)
            q = qv[from_rows, span] * jnp.asarray(HD ** (-0.5), bf)
            stacked = jnp.concatenate([q[:, r * HD:(r + 1) * HD] for r in range(ratio)], axis=0)
            scores = lax.dot_general(
                stacked, keys[:, g * HD:(g + 1) * HD], (((1,), (1,)), ((), ())),
                preferred_element_type=f32,
            )
            vg = values[:, g * HD:(g + 1) * HD]
            parts = []
            for r in range(ratio):
                sink = sink_ref[g * ratio + r]
                s = scores[r * WINDOW:(r + 1) * WINDOW] + bias
                top = jnp.maximum(jnp.max(s, axis=1, keepdims=True), sink)
                e = jnp.exp(s - top)
                den = jnp.sum(e, axis=1, keepdims=True) + jnp.exp(sink - top)
                o = jnp.dot(e.astype(bf), vg, preferred_element_type=f32)
                parts.append((o / den).astype(bf))
            att[home, to_rows, span] = jnp.concatenate(parts, axis=1)

    def far_step(i, carry):
        @pl.when(i == half - 1)
        def _():
            for copy in halo:
                copy.wait_recv()
            left = dl[blocks - 1:blocks, :].astype(f32)
            right = dr[0:1, :].astype(f32)
            left = jnp.where(sp == 0, -1.0, left)
            right = jnp.where(sp == sp_count - 1, -1.0, right)
            dx[0] = jnp.broadcast_to(left, (8, WINDOW))
            dx[blocks + 1] = jnp.broadcast_to(right, (8, WINDOW))

        attend_block(jnp.where(tp < 2, half + i, half - 1 - i))
        return carry

    def pick_of(slot_row):
        return jnp.where(ri.astype(f32) == slot_row, 1.0, 0.0).astype(bf)

    def gather_rows(pick, mine, mates):
        mixed_att[:, :heads] = jnp.dot(pick, mine, preferred_element_type=f32).astype(bf)
        mixed_att[:, heads:] = jnp.dot(pick, mates, preferred_element_type=f32).astype(bf)

    def project(cols):
        part = jnp.dot(mixed_att[:, :heads], wv[:, cols], preferred_element_type=f32)
        return part + jnp.dot(mixed_att[:, heads:], w_mate[:, cols], preferred_element_type=f32)

    loads[2].wait()
    with jax.named_scope("attn_far"):
        lax.fori_loop(0, half, far_step, 0)
    far_copy = go(remote(att.at[mate_across], am_far, ms.at[1], mr.at[1], {"tp": mate}))
    with jax.named_scope("wait_far"):
        r_copy.wait_recv()
        pick_far = pick_of(slots_of(routes_far[...], order, cap))
        loads[3].wait()
        w_copy.wait_recv()
        far_copy.wait_recv()
    with jax.named_scope("far_proj"):
        gather_rows(pick_far, att[across], am_far[...])

        def y_copy(k, h):
            return remote(
                ysend.at[h, k], yrecv.at[h, k], ys.at[h, k], yr.at[h, k], {"tp": across}
            )

        per = 4 // halves
        for h in range(halves):
            for c in range(per):
                cols = slice(h * hw + c * cw, h * hw + (c + 1) * cw)
                part = project(cols).astype(bf).reshape(groups, cap, cw)
                ysend[h, :, :, c * cw:(c + 1) * cw] = part
            if h < halves - 1:
                go(y_copy(emit_order[0], h))
        go(y_copy(emit_order[0], halves - 1))
        for k in emit_order[1:]:
            for h in range(halves):
                go(y_copy(k, h))

    def near_step(i, carry):
        attend_block(jnp.where(tp < 2, half - 1 - i, half + i))
        return carry

    with jax.named_scope("attn_near"):
        lax.fori_loop(0, half, near_step, 0)
    near_copy = go(remote(att.at[mate], am_near, ms.at[2], mr.at[2], {"tp": mate}))
    for i in range(4, 8):
        loads[i].wait()
    with jax.named_scope("wait_near"):
        pick = pick_of(slot)
        near_copy.wait_recv()
    def near_project(h):
        with jax.named_scope("near_proj%d" % h):
            for c in range(per):
                cols = slice(h * hw + c * cw, h * hw + (c + 1) * cw)
                part = project(cols)
                part += jnp.dot(pick, resv[:, cols], preferred_element_type=f32)
                acc[:, :, cols] = part.reshape(groups, cap, cw)

    def z_copy(k, h):
        return remote(send.at[h, k], own.at[h, k], zs.at[h, k], zr.at[h, k], to_plane(k))

    def x_copy(k, h):
        return remote(own.at[h, k], peer.at[h, k], xs.at[h, k], xr.at[h, k], x_mate)

    def hid_copy(k):
        return remote(hid_send.at[k], hid_recv.at[k], gs.at[k], gr.at[k], x_mate)

    def back_copy(k, h):
        return remote(comb.at[h, k], ret.at[h, k], bs.at[h, k], br.at[h, k], to_plane(k))

    def travels(step, i, action):
        if i % 2:
            pl.when(step[i] != here)(action)
        else:
            action()

    def emit(i, h):
        k = emit_order[i]
        with jax.named_scope("y%d_%d" % (i, h)):
            y_copy(k, h).wait_recv()
        cols = slice(h * hw, (h + 1) * hw)
        piece = (acc[k, :, cols] + yrecv[h, k].astype(f32)).astype(bf)
        send[h, k] = piece
        if i % 2:
            @pl.when(k == here)
            def _():
                own[h, here] = piece
        travels(emit_order, i, lambda: z_copy(k, h).start())

    def relay(i, h):
        k = serve_order[i]
        with jax.named_scope("z%d_%d" % (i, h)):
            travels(serve_order, i, lambda: z_copy(k, h).wait_recv())
        go(x_copy(k, h))

    def hidden_of(parts):
        squares = gate_act = up_act = 0.0
        for h in range(halves):
            span = slice(h * hw, (h + 1) * hw)
            wide = jnp.concatenate([buf[h, k] for buf, k in parts], axis=0).astype(f32)
            squares = squares + jnp.sum(wide * wide, axis=1, keepdims=True)
            block = (wide * gain_ref[:, span]).astype(bf)
            gate_act = gate_act + jnp.dot(block, gv[span, :], preferred_element_type=f32)
            up_act = up_act + jnp.dot(block, uv[span, :], preferred_element_type=f32)
        scale = lax.rsqrt(squares / width + eps_norm)
        g = gate_act * scale
        return (g / (1.0 + jnp.exp(-g)) * (up_act * scale)).astype(bf)

    def experts(i):
        parts = []
        if i < groups:
            parts.append((own, serve_order[i]))
        if i:
            k = serve_order[i - 1]
            with jax.named_scope("x%d" % i):
                for h in range(halves):
                    x_copy(k, h).wait_recv()
            parts.append((peer, k))
        with jax.named_scope("experts%d" % i):
            result = hidden_of(parts)
            if i:
                hid_send[k] = result[-cap:]
                go(hid_copy(k))
            if i < groups:
                hid_own[serve_order[i]] = result[:cap]

    sub_c = lax.broadcasted_iota(jnp.int32, (cap, rows), 0)
    lane_c = lax.broadcasted_iota(jnp.int32, (cap, rows), 1)

    def combine(i):
        k = serve_order[i]
        with jax.named_scope("hid%d" % i):
            hid_copy(k).wait_recv()
            travels(serve_order, i, lambda: remote(
                wsend, wrecv.at[k], ws.at[k], wr.at[k], x_mate
            ).wait_recv())
        with jax.named_scope("down%d" % i):
            table = wrecv[k]
            chosen = lane_c == sub_c + k * cap
            w_own = jnp.sum(jnp.where(chosen, table[0:1, :], 0.0), axis=1, keepdims=True)
            w_peer = jnp.sum(jnp.where(chosen, table[1:2, :], 0.0), axis=1, keepdims=True)
            mine, theirs = hid_own[k], hid_recv[k]
            for h in range(halves):
                for c in range(per):
                    cols = slice(h * hw + c * cw, h * hw + (c + 1) * cw)
                    total = jnp.dot(mine, dv[:, cols], preferred_element_type=f32) * w_own
                    total += jnp.dot(theirs, dv_mate[:, cols], preferred_element_type=f32) * w_peer
                    comb[h, k, :, c * cw:(c + 1) * cw] = total.astype(bf)
                travels(serve_order, i, lambda h=h: back_copy(k, h).start())

    def finish(k, h):
        if k == here:
            back = comb[h, k]
        else:
            with jax.named_scope("r%d_%d" % (k, h)):
                back_copy(k, h).wait_recv()
            back = ret[h, k]
        total = send[h, k].astype(f32) + back.astype(f32)
        fin[k * cap:(k + 1) * cap, h * hw:(h + 1) * hw] = total.astype(bf)

    gather_rows(pick, att[tp], am_near[...])
    for h in range(halves):
        near_project(h)
        emit(0, h)
    for i in (1, 2):
        for h in range(halves):
            emit(i, h)
            relay(i - 1, h)
        experts(i - 1)
    for h in range(halves):
        emit(3, h)
        relay(2, h)
    with jax.named_scope("dmate"):
        d_copy.wait_recv()
    d_fwd = go(remote(
        dv_mate.at[own_half], dv_mate.at[own_half], ds.at[1], dr_sem.at[1], {"tp": mate}
    ))
    experts(2)
    d_fwd.wait_recv()
    for h in range(halves - 1):
        relay(3, h)
    combine(0)
    relay(3, halves - 1)
    experts(3)
    combine(1)
    experts(4)
    combine(2)
    combine(3)
    for k in (0, 2, here, 1):
        for h in range(halves):
            finish(k, h)
    with jax.named_scope("out"):
        spread_b = spread.astype(bf)
        for c in range(4):
            cols = slice(c * cw, (c + 1) * cw)
            out_ref[:, cols] = jnp.dot(
                spread_b, fin[:, cols], preferred_element_type=f32
            ).astype(bf)
    with jax.named_scope("sends"):
        for k in away:
            for h in range(halves):
                z_copy(k, h).wait_send()
                back_copy(k, h).wait_send()
        for copy in pending:
            copy.wait_send()


def front_kernel(
    chunks, extra, entered, emit,
    sink_ref, q_ref, k_ref, v_ref, doc_ref, res_ref, w_ref,
    out_ref,
    kx, vx, dl, dr, dx, att, am_far, am_near, w_mate, acc, ysend, yrecv,
    hs, hr, ms, mr, ys, yr,
):
    sp = lax.axis_index("sp")
    tp = lax.axis_index("tp")
    sp_count = lax.axis_size("sp")
    mate = tp + 1 - 2 * (tp % 2)
    across = (tp + 2) % 4
    mate_across = (mate + 2) % 4
    after = (sp + 1) % sp_count
    before = (sp + sp_count - 1) % sp_count
    blocks = q_ref.shape[0] // WINDOW
    home_blocks = blocks // 4
    half = blocks // 2
    kv_heads = k_ref.shape[1] // HD
    ratio = q_ref.shape[1] // k_ref.shape[1]
    width = out_ref.shape[1]
    cw = width // chunks
    f32, bf = jnp.float32, jnp.bfloat16
    mesh_id = pl.DeviceIdType.MESH

    def remote(src, dst, ss, rs, where):
        return pltpu.make_async_remote_copy(
            src_ref=src, dst_ref=dst, send_sem=ss, recv_sem=rs,
            device_id=where, device_id_type=mesh_id,
        )

    barrier = pltpu.get_barrier_semaphore()
    for where in ({"sp": after}, {"sp": before}, {"tp": mate}, {"tp": across}):
        pl.semaphore_signal(barrier, inc=1, device_id=where, device_id_type=mesh_id)
    for b in range(blocks):
        kx[b + 1] = k_ref[b * WINDOW:(b + 1) * WINDOW, :]
        vx[b + 1] = v_ref[b * WINDOW:(b + 1) * WINDOW, :]
        dx[b + 1] = jnp.broadcast_to(doc_ref[b:b + 1, :].astype(f32), (8, WINDOW))
    pl.semaphore_wait(barrier, 4 + extra)

    tail = pl.ds((blocks - 1) * WINDOW, WINDOW)
    lead = pl.ds(0, WINDOW)
    halo = [
        remote(k_ref.at[tail], kx.at[0], hs.at[0], hr.at[0], {"sp": after}),
        remote(v_ref.at[tail], vx.at[0], hs.at[1], hr.at[1], {"sp": after}),
        remote(doc_ref, dl, hs.at[2], hr.at[2], {"sp": after}),
        remote(k_ref.at[lead], kx.at[blocks + 1], hs.at[3], hr.at[3], {"sp": before}),
        remote(v_ref.at[lead], vx.at[blocks + 1], hs.at[4], hr.at[4], {"sp": before}),
        remote(doc_ref, dr, hs.at[5], hr.at[5], {"sp": before}),
    ]
    for copy in halo:
        copy.start()
    w_copy = remote(w_ref, w_mate, ms.at[0], mr.at[0], {"tp": mate})
    w_copy.start()
    if entered is not None:
        entered()

    qi = lax.broadcasted_iota(jnp.int32, (WINDOW, 3 * WINDOW), 0)
    ki = lax.broadcasted_iota(jnp.int32, (WINDOW, 3 * WINDOW), 1)
    band = (ki >= qi) & (ki <= qi + 2 * WINDOW)
    eye = lax.broadcasted_iota(jnp.int32, (WINDOW, WINDOW), 0) == lax.broadcasted_iota(
        jnp.int32, (WINDOW, WINDOW), 1
    )

    def attend_block(b):
        own_docs = dx[b + 1][0:1]
        key_docs = jnp.concatenate([dx[b][0:1], own_docs, dx[b + 2][0:1]], axis=1)
        query_docs = jnp.sum(jnp.where(eye, own_docs, 0.0), axis=1, keepdims=True)
        bias = jnp.where(band & (key_docs == query_docs), 0.0, neg_fill)
        keys = kx[pl.ds(b, 3)].reshape(3 * WINDOW, kv_heads * HD)
        values = vx[pl.ds(b, 3)].reshape(3 * WINDOW, kv_heads * HD)
        home = b // home_blocks
        to_rows = pl.ds(pl.multiple_of((b % home_blocks) * WINDOW, WINDOW), WINDOW)
        from_rows = pl.ds(pl.multiple_of(b * WINDOW, WINDOW), WINDOW)
        for g in range(kv_heads):
            span = slice(g * ratio * HD, (g + 1) * ratio * HD)
            q = q_ref[from_rows, span] * jnp.asarray(HD ** (-0.5), bf)
            stacked = jnp.concatenate([q[:, r * HD:(r + 1) * HD] for r in range(ratio)], axis=0)
            scores = lax.dot_general(
                stacked, keys[:, g * HD:(g + 1) * HD], (((1,), (1,)), ((), ())),
                preferred_element_type=f32,
            )
            vg = values[:, g * HD:(g + 1) * HD]
            parts = []
            for r in range(ratio):
                sink = sink_ref[g * ratio + r]
                s = scores[r * WINDOW:(r + 1) * WINDOW] + bias
                top = jnp.maximum(jnp.max(s, axis=1, keepdims=True), sink)
                e = jnp.exp(s - top)
                den = jnp.sum(e, axis=1, keepdims=True) + jnp.exp(sink - top)
                o = jnp.dot(e.astype(bf), vg, preferred_element_type=f32)
                parts.append((o / den).astype(bf))
            att[home, to_rows, span] = jnp.concatenate(parts, axis=1)

    def far_step(i, carry):
        @pl.when(i == half - 1)
        def _():
            for copy in halo:
                copy.wait_recv()
            left = dl[blocks - 1:blocks, :].astype(f32)
            right = dr[0:1, :].astype(f32)
            left = jnp.where(sp == 0, -1.0, left)
            right = jnp.where(sp == sp_count - 1, -1.0, right)
            dx[0] = jnp.broadcast_to(left, (8, WINDOW))
            dx[blocks + 1] = jnp.broadcast_to(right, (8, WINDOW))

        attend_block(jnp.where(tp < 2, half + i, half - 1 - i))
        return carry

    lax.fori_loop(0, half, far_step, 0)
    far_copy = remote(att.at[mate_across], am_far, ms.at[1], mr.at[1], {"tp": mate})
    far_copy.start()
    w_copy.wait_recv()
    far_copy.wait_recv()
    sent = []
    for c in range(chunks):
        cols = slice(c * cw, (c + 1) * cw)
        part = jnp.dot(att[across], w_ref[:, cols], preferred_element_type=f32)
        part += jnp.dot(am_far[...], w_mate[:, cols], preferred_element_type=f32)
        ysend[c] = part.astype(bf)
        copy = remote(ysend.at[c], yrecv.at[c], ys.at[c], yr.at[c], {"tp": across})
        copy.start()
        sent.append(copy)

    def near_step(i, carry):
        attend_block(jnp.where(tp < 2, half - 1 - i, half + i))
        return carry

    lax.fori_loop(0, half, near_step, 0)
    near_copy = remote(att.at[mate], am_near, ms.at[2], mr.at[2], {"tp": mate})
    near_copy.start()
    near_copy.wait_recv()
    for c in range(chunks):
        cols = slice(c * cw, (c + 1) * cw)
        part = jnp.dot(att[tp], w_ref[:, cols], preferred_element_type=f32)
        part += jnp.dot(am_near[...], w_mate[:, cols], preferred_element_type=f32)
        acc[:, cols] = part + res_ref[:, cols].astype(f32)
    for c in range(chunks):
        cols = slice(c * cw, (c + 1) * cw)
        sent[c].wait_recv()
        out_ref[:, cols] = (acc[:, cols] + yrecv[c].astype(f32)).astype(bf)
        if emit is not None:
            emit(c)
    for copy in halo + [w_copy, far_copy, near_copy] + sent:
        copy.wait_send()


def front_scratch(queries, key_rows, residual, out_weight):
    rows, width = residual.shape
    local, heads_width = queries.shape
    kv_width = key_rows.shape[1]
    blocks = local // WINDOW
    bf, f32 = jnp.bfloat16, jnp.float32
    dma = pltpu.SemaphoreType.DMA
    return [
            pltpu.VMEM((blocks + 2, WINDOW, kv_width), bf),
            pltpu.VMEM((blocks + 2, WINDOW, kv_width), bf),
            pltpu.VMEM((blocks, WINDOW), jnp.int32),
            pltpu.VMEM((blocks, WINDOW), jnp.int32),
            pltpu.VMEM((blocks + 2, 8, WINDOW), f32),
            pltpu.VMEM((4, rows, heads_width), bf),
            pltpu.VMEM((rows, heads_width), bf),
            pltpu.VMEM((rows, heads_width), bf),
            pltpu.VMEM(out_weight.shape, bf),
            pltpu.VMEM((rows, width), f32),
            pltpu.VMEM((CHUNKS, rows, width // CHUNKS), bf),
            pltpu.VMEM((CHUNKS, rows, width // CHUNKS), bf),
            dma((6,)), dma((6,)), dma((3,)), dma((3,)), dma((CHUNKS,)), dma((CHUNKS,)),
    ]


def front(queries, key_rows, value_rows, doc_ids, sink_logit, residual, out_weight):
    rows, width = residual.shape
    local, heads_width = queries.shape
    kv_width = key_rows.shape[1]
    blocks = local // WINDOW
    bf, f32 = jnp.bfloat16, jnp.float32
    dma = pltpu.SemaphoreType.DMA
    vm = pl.BlockSpec(memory_space=pltpu.VMEM)
    docs = doc_ids.reshape(blocks, WINDOW)
    return pl.pallas_call(
        functools.partial(front_kernel, CHUNKS, 0, None, None),
        out_shape=jax.ShapeDtypeStruct((rows, width), bf),
        in_specs=[pl.BlockSpec(memory_space=pltpu.SMEM)] + [vm] * 6,
        out_specs=vm,
        scratch_shapes=front_scratch(queries, key_rows, residual, out_weight),
        compiler_params=pltpu.CompilerParams(
            collective_id=4, has_side_effects=True, vmem_limit_bytes=48 * 1024 * 1024
        ),
        name="front",
    )(sink_logit, queries, key_rows, value_rows, docs, residual, out_weight)


def pair_routed(routes, gate_weight):
    count = lax.axis_size("sp")
    experts = count * gate_weight.shape[0]
    return (
        gate_weight.shape[0] == 1
        and routes.shape[1] == 2
        and experts == 2 * GROUPS
    )


def mixture(
    queries, key_rows, value_rows, doc_ids, sink_logit, residual, out_weight,
    norm_gain, routes, route_weights, gate_weight, up_weight, down_weight,
):
    rows, width = residual.shape
    blocks = queries.shape[0] // WINDOW
    heads = queries.shape[1]
    kv_width = key_rows.shape[1]
    docs = doc_ids.reshape(blocks, WINDOW)
    ff = gate_weight.shape[2]
    groups = lax.axis_size("sp") // 2
    cap, hw = rows // groups, width // HALVES
    bf, f32, i32 = jnp.bfloat16, jnp.float32, jnp.int32
    pieces = pltpu.VMEM((HALVES, groups, cap, hw), bf)
    hidden = pltpu.VMEM((groups, cap, ff), bf)
    dma = pltpu.SemaphoreType.DMA
    vm = pl.BlockSpec(memory_space=pltpu.VMEM)
    hbm = pl.BlockSpec(memory_space=pl.ANY)
    edge = pltpu.VMEM((blocks + 2, WINDOW, kv_width), bf)
    per_piece = dma((HALVES, groups))
    return pl.pallas_call(
        functools.partial(moe_kernel, groups, HALVES),
        out_shape=jax.ShapeDtypeStruct((rows, width), bf),
        in_specs=[pl.BlockSpec(memory_space=pltpu.SMEM)] + [vm] * 4 + [hbm] * 8,
        out_specs=vm,
        scratch_shapes=[
            pltpu.VMEM(queries.shape, bf), pltpu.VMEM((rows, width), bf),
            pltpu.VMEM(out_weight.shape, bf), pltpu.VMEM(out_weight.shape, bf),
            edge, edge,
            pltpu.VMEM((blocks, WINDOW), i32), pltpu.VMEM((blocks, WINDOW), i32),
            pltpu.VMEM((blocks + 2, 8, WINDOW), f32),
            pltpu.VMEM((4, rows, heads), bf),
            pltpu.VMEM((rows, heads), bf), pltpu.VMEM((rows, heads), bf),
            pltpu.VMEM(routes.shape[::-1], i32),
            pltpu.VMEM((rows, 2 * heads), bf),
            pltpu.VMEM((groups, cap, width), f32),
            pieces, pieces, pieces, pieces, pieces, pieces, pieces,
            hidden, hidden, hidden,
            pltpu.VMEM((8, rows), f32), pltpu.VMEM((groups, 8, rows), f32),
            pltpu.VMEM((rows, width), bf),
            pltpu.VMEM((width, ff), bf), pltpu.VMEM((width, ff), bf),
            pltpu.VMEM((ff, width), bf), pltpu.VMEM((ff, width), bf),
            dma((8,)), dma((6,)), dma((6,)), dma((4,)), dma((4,)),
            per_piece, per_piece, per_piece, per_piece, per_piece, per_piece,
            dma((groups,)), dma((groups,)), per_piece, per_piece,
            dma((groups,)), dma((groups,)), dma((2,)), dma((2,)),
        ],
        compiler_params=pltpu.CompilerParams(
            collective_id=3, has_side_effects=True, vmem_limit_bytes=56 * 1024 * 1024
        ),
        name="mixture",
    )(
        sink_logit, docs, routes.T, route_weights.T, norm_gain[None, :],
        queries, key_rows.reshape(blocks, WINDOW, kv_width),
        value_rows.reshape(blocks, WINDOW, kv_width), residual, out_weight,
        gate_weight, up_weight, down_weight,
    )


def fits_front(queries):
    return lax.axis_size("tp") == 4 and queries.shape[0] % (8 * WINDOW) == 0


def stream_of(
    queries, key_rows, value_rows, doc_ids, sink_logit, residual, out_weight
):
    local_rows = queries.shape[0]
    if fits_front(queries):
        return front(queries, key_rows, value_rows, doc_ids, sink_logit, residual, out_weight)
    anchor = lax.axis_index("sp") * local_rows
    extent = local_rows * lax.axis_size("sp")
    doc_float = doc_ids.astype(jnp.bfloat16)
    block_rows = min(512, local_rows)
    padded_keys, padded_values, padded_docs = fetch_margins(key_rows, value_rows, doc_float)
    block_parts = []
    for row_start in range(0, local_rows, block_rows):
        key_end = row_start + block_rows + 2 * WINDOW
        block_parts.append(
            attend(
                queries[row_start : row_start + block_rows],
                padded_keys[row_start:key_end],
                padded_values[row_start:key_end],
                doc_float[row_start : row_start + block_rows],
                padded_docs[row_start:key_end],
                anchor + row_start,
                anchor + row_start - WINDOW,
                sink_logit,
                extent,
            )
        )
    attended = jnp.concatenate(block_parts, axis=0)
    regrouped = lax.all_to_all(attended, "tp", split_axis=0, concat_axis=1, tiled=True)
    shard_rows = out_weight.shape[0]
    initial = jnp.zeros((regrouped.shape[0], out_weight.shape[1]), jnp.float32)
    running = initial
    weight_piece = lax.all_gather(out_weight, "tp", axis=0, tiled=True)
    for shard_index in range(weight_piece.shape[0] // shard_rows):
        columns = lax.dynamic_slice_in_dim(regrouped, shard_index * shard_rows, shard_rows, 1)
        partial_value = jnp.dot(
            columns,
            weight_piece[shard_index * shard_rows : (shard_index + 1) * shard_rows],
            preferred_element_type=jnp.float32,
        )
        running = running + partial_value.astype(jnp.bfloat16).astype(jnp.float32)
    stream = (residual.astype(jnp.float32) + running).astype(jnp.bfloat16)
    return stream


def per_device(
    queries,
    key_rows,
    value_rows,
    doc_ids,
    sink_logit,
    residual,
    out_weight,
    norm_gain,
    gate_weight,
    up_weight,
    down_weight,
    routes,
    route_weights,
):
    front_args = (
        queries, key_rows, value_rows, doc_ids, sink_logit, residual, out_weight
    )
    if pair_routed(routes, gate_weight) and fits_front(queries):
        return mixture(
            *front_args, norm_gain, routes, route_weights, gate_weight, up_weight, down_weight
        )
    stream = stream_of(*front_args)
    stream_f = stream.astype(jnp.float32)
    scale = lax.rsqrt(jnp.mean(stream_f * stream_f, axis=1, keepdims=True) + eps_norm)
    normed = (stream_f * scale * norm_gain[None, :]).astype(jnp.bfloat16)
    home_rows = normed.shape[0]
    width = normed.shape[1]
    route_count = routes.shape[1]
    expert_count = lax.axis_size("sp") * gate_weight.shape[0]
    capacity = route_count * home_rows // expert_count
    flat_routes = routes.reshape(-1)
    one_hot = (flat_routes[:, None] == jnp.arange(expert_count, dtype=jnp.int32)[None, :]).astype(
        jnp.int32
    )
    earlier = jnp.cumsum(one_hot, axis=0) - one_hot
    slot_rank = jnp.sum(earlier * one_hot, axis=1)
    slot_index = flat_routes * capacity + slot_rank
    source_row = (
        jnp.zeros((expert_count * capacity,), jnp.int32)
        .at[slot_index]
        .set(jnp.arange(home_rows * route_count, dtype=jnp.int32) // route_count)
    )
    outgoing = normed[source_row].reshape(expert_count, capacity, width)
    incoming = lax.all_to_all(outgoing, "sp", split_axis=0, concat_axis=0, tiled=True)
    flat_rows = incoming.reshape(-1, width)
    gate_act = jnp.dot(flat_rows, gate_weight[0], preferred_element_type=jnp.float32)
    up_act = jnp.dot(flat_rows, up_weight[0], preferred_element_type=jnp.float32)
    hidden = (jax.nn.silu(gate_act) * up_act).astype(jnp.bfloat16)
    produced = jnp.dot(hidden, down_weight[0], preferred_element_type=jnp.float32).astype(
        jnp.bfloat16
    )
    returned = lax.all_to_all(
        produced.reshape(incoming.shape), "sp", split_axis=0, concat_axis=0, tiled=True
    )
    route_out = returned.reshape(-1, width)[slot_index].reshape(home_rows, route_count, width)
    weighted = jnp.sum(route_weights[:, :, None] * route_out.astype(jnp.float32), axis=1)
    return (stream_f + weighted).astype(jnp.bfloat16)


def solution(mesh):
    return jax.shard_map(
        per_device,
        mesh=mesh,
        in_specs=(
            P("sp", "tp"),
            P("sp", "tp"),
            P("sp", "tp"),
            P("sp"),
            P("tp"),
            P(("sp", "tp"), None),
            P("tp", None),
            P(),
            P("sp", None, None),
            P("sp", None, None),
            P("sp", None, None),
            P(("sp", "tp"), None),
            P(("sp", "tp"), None),
        ),
        out_specs=P(("sp", "tp"), None),
        check_vma=False,
    )
```

```python
import functools

import jax
import jax.numpy as jnp
from jax import lax
from jax.experimental import pallas as pl
from jax.experimental.pallas import tpu as pltpu
from jax.sharding import PartitionSpec as P

HD = 64
WINDOW = 128
GROUPS = 4
CHUNKS = 4
HALVES = 2


neg_fill = -1e30
eps_norm = 1e-06


def extended(block, sides, width):
    for axis, dim in sides:
        count = lax.axis_size(axis)
        forward = [(i, i + 1) for i in range(count - 1)]
        backward = [(target, source) for source, target in forward]
        low = lax.ppermute(
            lax.slice_in_dim(block, block.shape[dim] - width, None, axis=dim), axis, forward
        )
        high = lax.ppermute(lax.slice_in_dim(block, 0, width, axis=dim), axis, backward)
        block = jnp.concatenate([low, block, high], axis=dim)
    return block


def attend(
    query_part,
    key_part,
    value_part,
    query_docs,
    key_docs,
    query_start,
    key_start,
    sink_logit,
    extent,
):
    query_count = query_part.shape[0]
    key_count = key_part.shape[0]
    groups = key_part.shape[1] // HD
    head_ratio = sink_logit.shape[0] // groups
    query_heads = query_part.reshape(query_count, groups, head_ratio, HD)
    key_heads = key_part.reshape(key_count, groups, HD)
    value_heads = value_part.reshape(key_count, groups, HD)
    scores = jnp.einsum(
        "qgrd,kgd->grqk", query_heads, key_heads, preferred_element_type=jnp.float32
    ) * HD ** (-0.5)
    query_pos = query_start + jnp.arange(query_count, dtype=jnp.int32)
    key_pos = key_start + jnp.arange(key_count, dtype=jnp.int32)
    inside = (key_pos >= 0) & (key_pos < extent)
    allowed = (
        (jnp.abs(query_pos[:, None] - key_pos[None, :]) <= WINDOW)
        & (query_docs[:, None] == key_docs[None, :])
        & inside[None, :]
    )
    masked = jnp.where(allowed[None, None], scores, neg_fill)
    sink_col = sink_logit.reshape(groups, head_ratio)[:, :, None, None]
    row_top = jnp.maximum(jnp.max(masked, axis=3, keepdims=True), sink_col)
    exponent = jnp.where(allowed[None, None], jnp.exp(masked - row_top), 0.0)
    denominator = jnp.sum(exponent, axis=3, keepdims=True) + jnp.exp(sink_col - row_top)
    attn_weight = (exponent / denominator).astype(jnp.bfloat16)
    attended = jnp.einsum(
        "grqk,kgd->qgrd", attn_weight, value_heads, preferred_element_type=jnp.float32
    )
    return attended.astype(jnp.bfloat16).reshape(query_count, -1)


def fetch_margins(key_rows, value_rows, doc_float):
    return (
        extended(key_rows, (("sp", 0),), WINDOW),
        extended(value_rows, (("sp", 0),), WINDOW),
        extended(doc_float, (("sp", 0),), WINDOW),
    )


def plane_order(gz):
    return [(gz + 2) % 4, 3 - gz, gz + 1 - 2 * (gz % 2), gz]


def slots_of(routes, order, cap):
    rows = routes.shape[1]
    f32, bf = jnp.float32, jnp.bfloat16
    group_of = routes[0:1, :] // 2
    sub = lax.broadcasted_iota(jnp.int32, (8, rows), 0)
    wanted = jnp.full((8, rows), -1, jnp.int32)
    for k, plane in enumerate(order):
        wanted = jnp.where(sub == k, plane, wanted)
    one_hot = jnp.where(group_of == wanted, 1.0, 0.0)
    ri = lax.broadcasted_iota(jnp.int32, (rows, rows), 0)
    ci = lax.broadcasted_iota(jnp.int32, (rows, rows), 1)
    above = jnp.where(ri < ci, 1.0, 0.0).astype(bf)
    ranks = jnp.dot(one_hot.astype(bf), above, preferred_element_type=f32)
    base = sub.astype(f32) * cap
    return jnp.sum((ranks + base) * one_hot, axis=0, keepdims=True)


def moe_kernel(
    groups, halves,
    sink_hbm, doc_hbm, routes_hbm, rw_hbm, gain_hbm,
    q_hbm, k_hbm, v_hbm, res_hbm, w_hbm, gate_hbm, up_hbm, down_hbm,
    moved_hbm, spread_hbm,
    fin, spread_ref, sink_ref, doc_ref, routes_ref, rw_ref, gain_ref,
    qv, resv, wv, w_mate, kx, vx, dl, dr, dx, att, am_far, am_near, routes_far,
    mixed_att, acc, ysend, yrecv, send, own, peer, comb, ret, hid_own, hid_send, hid_recv,
    wsend, wrecv, gv, uv, dv, dv_mate,
    ls, hs, hr, ms, mr, ys, yr, zs, zr, xs, xr, gs, gr, bs, br, ws, wr, ds, dr_sem, outs,
):
    sp = lax.axis_index("sp")
    tp = lax.axis_index("tp")
    sp_count = lax.axis_size("sp")
    gz, side = sp // 2, sp % 2
    x_mate = {"sp": gz * 2 + 1 - side}
    mate = tp + 1 - 2 * (tp % 2)
    core = tp % 2
    across = (tp + 2) % 4
    mate_across = (mate + 2) % 4
    after = (sp + 1) % sp_count
    before = (sp + sp_count - 1) % sp_count
    order = plane_order(gz)
    here = groups - 1
    away = [k for k in range(groups) if k != here]
    rows, width = fin.shape
    cap = rows // groups
    hw = width // halves
    cw = width // 4
    blocks = k_hbm.shape[0]
    home_blocks = blocks // 4
    half = blocks // 2
    kv_heads = k_hbm.shape[2] // HD
    ratio = q_hbm.shape[1] // k_hbm.shape[2]
    heads = q_hbm.shape[1]
    f32, bf = jnp.float32, jnp.bfloat16
    mesh_id = pl.DeviceIdType.MESH

    def remote(src, dst, s_sem, r_sem, where):
        return pltpu.make_async_remote_copy(
            src_ref=src, dst_ref=dst, send_sem=s_sem, recv_sem=r_sem,
            device_id=where, device_id_type=mesh_id,
        )

    end = (gz == 0) | (gz == groups - 1)

    def pick_one(at_end, at_middle):
        return at_end if at_end == at_middle else jnp.where(end, at_end, at_middle)

    emit_order = [pick_one(a, b) for a, b in ((0, 2), (1, 0), (2, 1), (here, here))]
    serve_order = [pick_one(a, b) for a, b in ((2, 0), (1, 2), (0, 1), (here, here))]

    def to_plane(k):
        plane = order[3]
        for i in range(groups - 1):
            plane = jnp.where(k == i, order[i], plane)
        return {"sp": plane * 2 + side}

    barrier = pltpu.get_barrier_semaphore()
    partners = [{"sp": after}, {"sp": before}, {"tp": mate}, {"tp": across}, x_mate]
    partners += [to_plane(k) for k in away]
    for where in partners:
        pl.semaphore_signal(barrier, inc=1, device_id=where, device_id_type=mesh_id)
    pairs = (
        (k_hbm, kx.at[pl.ds(1, blocks)]), (v_hbm, vx.at[pl.ds(1, blocks)]),
        (doc_hbm, doc_ref), (routes_hbm, routes_ref), (rw_hbm, rw_ref), (sink_hbm, sink_ref),
        (q_hbm, qv), (w_hbm, wv), (gain_hbm, gain_ref), (res_hbm, resv),
        (gate_hbm.at[0], gv), (up_hbm.at[0], uv), (down_hbm.at[0], dv),
    )
    loads = [pltpu.make_async_copy(src, dst, ls.at[i]) for i, (src, dst) in enumerate(pairs)]
    for load in loads[:7]:
        load.start()

    @pl.when(sp == 0)
    def _():
        kx[0] = jnp.zeros(kx.shape[1:], bf)
        vx[0] = jnp.zeros(vx.shape[1:], bf)

    @pl.when(sp == sp_count - 1)
    def _():
        kx[blocks + 1] = jnp.zeros(kx.shape[1:], bf)
        vx[blocks + 1] = jnp.zeros(vx.shape[1:], bf)

    for load in loads[:5]:
        load.wait()
    with jax.named_scope("barrier"):
        pl.semaphore_wait(barrier, len(partners))
    pending = []

    def go(copy):
        copy.start()
        pending.append(copy)
        return copy

    def halo_of(i, src, dst, where):
        return remote(src, dst, hs.at[i], hr.at[i], {"sp": where})

    to_after = [
        halo_of(0, kx.at[blocks], kx.at[0], after),
        halo_of(1, vx.at[blocks], vx.at[0], after),
        halo_of(2, doc_ref, dl, after),
    ]
    to_before = [
        halo_of(3, kx.at[1], kx.at[blocks + 1], before),
        halo_of(4, vx.at[1], vx.at[blocks + 1], before),
        halo_of(5, doc_ref, dr, before),
    ]

    @pl.when(sp > 0)
    def _():
        for copy in to_before:
            copy.start()

    @pl.when(sp < sp_count - 1)
    def _():
        for copy in to_after:
            copy.start()

    r_copy = go(remote(routes_ref, routes_far, ms.at[3], mr.at[3], {"tp": across}))
    ff = dv.shape[0]
    quarter, eighth = ff // 4, ff // 8
    chip = tp // 2
    d_rows = [
        pl.ds(pl.multiple_of(start, eighth), count) for start, count in (
            ((2 + chip) * quarter + core * eighth, eighth), (core * quarter, quarter),
            ((3 - chip) * quarter + core * eighth, eighth),
        )
    ]

    def d_part(i, source, sem, where):
        return remote(
            source.at[d_rows[i]], dv_mate.at[d_rows[i]], ds.at[sem], dr_sem.at[sem], where
        )

    from_x = [go(d_part(i, down_hbm.at[0], i, x_mate)) for i in range(2)]
    w_copy = remote(w_hbm, w_mate, ms.at[0], mr.at[0], {"tp": mate})
    for b in range(blocks):
        dx[b + 1] = jnp.broadcast_to(doc_ref[b:b + 1, :].astype(f32), (8, WINDOW))

    def left_halo():
        @pl.when(sp > 0)
        def _():
            for copy in to_after:
                copy.wait_recv()
        left = jnp.where(sp == 0, -1.0, dl[blocks - 1:blocks, :].astype(f32))
        dx[0] = jnp.broadcast_to(left, (8, WINDOW))

    def right_halo():
        @pl.when(sp < sp_count - 1)
        def _():
            for copy in to_before:
                copy.wait_recv()
        right = jnp.where(sp == sp_count - 1, -1.0, dr[0:1, :].astype(f32))
        dx[blocks + 1] = jnp.broadcast_to(right, (8, WINDOW))

    slot = slots_of(routes_ref[...], order, cap)
    ri = lax.broadcasted_iota(jnp.int32, (rows, rows), 0)
    ci = lax.broadcasted_iota(jnp.int32, (rows, rows), 1)
    slot_col = jnp.sum(jnp.where(ri == ci, slot, 0.0), axis=1, keepdims=True)
    spread = jnp.where(slot_col == ci.astype(f32), 1.0, 0.0)
    weight_rows = []
    for parity in (side, 1 - side):
        w_row = jnp.where(routes_ref[0:1, :] % 2 == parity, rw_ref[0:1, :], rw_ref[1:2, :])
        w_col = jnp.sum(jnp.where(ri == ci, w_row, 0.0), axis=1, keepdims=True)
        weight_rows.append(jnp.sum(spread * w_col, axis=0, keepdims=True))
    sub8 = lax.broadcasted_iota(jnp.int32, (8, rows), 0)
    wsend[...] = jnp.where(
        sub8 == 0, weight_rows[0], jnp.where(sub8 == 1, weight_rows[1], 0.0)
    )

    wrecv[here] = wsend[...]

    for k in away:
        go(remote(wsend, wrecv.at[k], ws.at[k], wr.at[k], to_plane(k)))

    qi = lax.broadcasted_iota(jnp.int32, (WINDOW, 3 * WINDOW), 0)
    ki = lax.broadcasted_iota(jnp.int32, (WINDOW, 3 * WINDOW), 1)
    band = (ki >= qi) & (ki <= qi + 2 * WINDOW)
    eye = lax.broadcasted_iota(jnp.int32, (WINDOW, WINDOW), 0) == lax.broadcasted_iota(
        jnp.int32, (WINDOW, WINDOW), 1
    )

    low = lax.broadcasted_iota(jnp.int32, (3 * WINDOW, kv_heads * HD), 1) < HD
    low_q = lax.broadcasted_iota(jnp.int32, (WINDOW, kv_heads * HD), 1) < HD
    zero, one = jnp.zeros((), bf), jnp.ones((), bf)

    def attend_block(b):
        own_docs = dx[b + 1][0:1]
        key_docs = jnp.concatenate([dx[b][0:1], own_docs, dx[b + 2][0:1]], axis=1)
        query_docs = jnp.sum(jnp.where(eye, own_docs, 0.0), axis=1, keepdims=True)
        bias = jnp.where(band & (key_docs == query_docs), 0.0, neg_fill)
        keys = kx[pl.ds(b, 3)].reshape(3 * WINDOW, kv_heads * HD)
        values = vx[pl.ds(b, 3)].reshape(3 * WINDOW, kv_heads * HD)
        key_two = jnp.concatenate(
            [jnp.where(low, keys, zero), jnp.where(low, zero, keys)], axis=0
        )
        value_two = jnp.concatenate([
            jnp.concatenate([jnp.where(low, values, zero), jnp.where(low, one, zero)], axis=1),
            jnp.concatenate([jnp.where(low, zero, values), jnp.where(low, zero, one)], axis=1),
        ], axis=0)
        home = b // home_blocks
        to_rows = pl.ds(pl.multiple_of((b % home_blocks) * WINDOW, WINDOW), WINDOW)
        from_rows = pl.ds(pl.multiple_of(b * WINDOW, WINDOW), WINDOW)
        q = qv[from_rows, :] * jnp.asarray(HD ** (-0.5), bf)
        parts = [None] * (2 * ratio)
        for r in range(ratio):
            pair = jnp.concatenate(
                [q[:, r * HD:(r + 1) * HD], q[:, (ratio + r) * HD:(ratio + r + 1) * HD]], axis=1
            )
            scores = lax.dot_general(
                pair, key_two, (((1,), (1,)), ((), ())), preferred_element_type=f32
            )
            exps, sinks = [], []
            for g in range(2):
                sink = sink_ref[g * ratio + r]
                s = scores[:, g * 3 * WINDOW:(g + 1) * 3 * WINDOW] + bias
                top = jnp.maximum(jnp.max(s, axis=1, keepdims=True), sink)
                exps.append(jnp.exp(s - top).astype(bf))
                sinks.append(jnp.exp(sink - top))
            o = jnp.dot(jnp.concatenate(exps, axis=1), value_two, preferred_element_type=f32)
            den = o[:, 2 * HD:] + jnp.where(low_q, sinks[0], sinks[1])
            both = (o[:, :2 * HD] / den).astype(bf)
            parts[r], parts[ratio + r] = both[:, :HD], both[:, HD:]
        att[home, to_rows, :] = jnp.concatenate(parts, axis=1)

    def far_step(i, carry):
        @pl.when(i == 1)
        def _():
            w_copy.start()

        @pl.when((i == half - 1) & (tp < 2))
        def _():
            right_halo()

        @pl.when((i == half - 1) & (tp >= 2))
        def _():
            left_halo()

        attend_block(jnp.where(tp < 2, half + i, half - 1 - i))
        return carry

    def pick_of(slot_row):
        return jnp.where(ri.astype(f32) == slot_row, 1.0, 0.0).astype(bf)

    def gather_rows(pick, mine, mates):
        mixed_att[:, :heads] = jnp.dot(pick, mine, preferred_element_type=f32).astype(bf)
        mixed_att[:, heads:] = jnp.dot(pick, mates, preferred_element_type=f32).astype(bf)

    def project(cols):
        part = jnp.dot(mixed_att[:, :heads], wv[:, cols], preferred_element_type=f32)
        return part + jnp.dot(mixed_att[:, heads:], w_mate[:, cols], preferred_element_type=f32)

    def near_step(i, carry):
        own_turn = tp * home_blocks + i - home_blocks
        attend_block(jnp.where(i < home_blocks, mate * home_blocks + i, own_turn))
        return carry

    loads[5].wait()
    loads[6].wait()
    loads[7].start()
    with jax.named_scope("attn_far"):
        lax.fori_loop(0, half, far_step, 0)
    pending.append(w_copy)
    far_copy = go(remote(att.at[mate_across], am_far, ms.at[1], mr.at[1], {"tp": mate}))
    for load in loads[8:]:
        load.start()
    with jax.named_scope("attn_first"):
        pl.when(tp < 2)(left_halo)
        pl.when(tp >= 2)(right_halo)
        near_step(0, 0)
    with jax.named_scope("wait_far"):
        r_copy.wait_recv()
        pick_far = pick_of(slots_of(routes_far[...], order, cap))
        loads[7].wait()
        w_copy.wait_recv()
        far_copy.wait_recv()
    with jax.named_scope("far_proj"):
        gather_rows(pick_far, att[across], am_far[...])

        def y_copy(k, h):
            return remote(
                ysend.at[h, k], yrecv.at[h, k], ys.at[h, k], yr.at[h, k], {"tp": across}
            )

        per = 4 // halves
        for h in range(halves):
            for c in range(per):
                cols = slice(h * hw + c * cw, h * hw + (c + 1) * cw)
                part = project(cols).astype(bf).reshape(groups, cap, cw)
                ysend[h, :, :, c * cw:(c + 1) * cw] = part
            if h < halves - 1:
                go(y_copy(emit_order[0], h))
        go(y_copy(emit_order[0], halves - 1))
        for k in emit_order[1:here]:
            for h in range(halves):
                go(y_copy(k, h))

    with jax.named_scope("attn_near"):
        lax.fori_loop(1, home_blocks, near_step, 0)
        near_copy = go(remote(att.at[mate], am_near, ms.at[2], mr.at[2], {"tp": mate}))
        from_x[0].wait_recv()
        go(d_part(0, dv_mate, 2, {"tp": across}))
        for h in range(halves):
            go(y_copy(here, h))
        lax.fori_loop(home_blocks, half, near_step, 0)
    for load in loads[8:]:
        load.wait()
    with jax.named_scope("wait_near"):
        pick = pick_of(slot)
        near_copy.wait_recv()
    def near_project(h):
        with jax.named_scope("near_proj%d" % h):
            for c in range(per):
                cols = slice(h * hw + c * cw, h * hw + (c + 1) * cw)
                part = project(cols)
                part += jnp.dot(pick, resv[:, cols], preferred_element_type=f32)
                acc[:, :, cols] = part.reshape(groups, cap, cw)

    def z_copy(k, h):
        return remote(send.at[h, k], own.at[h, k], zs.at[h, k], zr.at[h, k], to_plane(k))

    def x_copy(k, h):
        return remote(own.at[h, k], peer.at[h, k], xs.at[h, k], xr.at[h, k], x_mate)

    def hid_copy(k):
        return remote(hid_send.at[k], hid_recv.at[k], gs.at[k], gr.at[k], x_mate)

    def back_copy(k, h):
        return remote(comb.at[h, k], ret.at[h, k], bs.at[h, k], br.at[h, k], to_plane(k))

    def emit(i, h):
        k = emit_order[i]
        with jax.named_scope("y%d_%d" % (i, h)):
            y_copy(k, h).wait_recv()
        cols = slice(h * hw, (h + 1) * hw)
        piece = (acc[k, :, cols] + yrecv[h, k].astype(f32)).astype(bf)
        send[h, k] = piece
        if i == here:
            own[h, here] = piece
        else:
            z_copy(k, h).start()

    def relay(i, h):
        k = serve_order[i]
        if i != here:
            with jax.named_scope("z%d_%d" % (i, h)):
                z_copy(k, h).wait_recv()
        go(x_copy(k, h))

    def hidden_of(parts):
        squares = gate_act = up_act = 0.0
        for h in range(halves):
            span = slice(h * hw, (h + 1) * hw)
            wide = jnp.concatenate([buf[h, k] for buf, k in parts], axis=0).astype(f32)
            squares = squares + jnp.sum(wide * wide, axis=1, keepdims=True)
            block = (wide * gain_ref[:, span]).astype(bf)
            gate_act = gate_act + jnp.dot(block, gv[span, :], preferred_element_type=f32)
            up_act = up_act + jnp.dot(block, uv[span, :], preferred_element_type=f32)
        scale = lax.rsqrt(squares / width + eps_norm)
        g = gate_act * scale
        return (g / (1.0 + jnp.exp(-g)) * (up_act * scale)).astype(bf)

    def experts(i):
        parts = []
        if i < groups:
            parts.append((own, serve_order[i]))
        if i:
            k = serve_order[i - 1]
            with jax.named_scope("x%d" % i):
                for h in range(halves):
                    x_copy(k, h).wait_recv()
            parts.append((peer, k))
        with jax.named_scope("experts%d" % i):
            result = hidden_of(parts)
            if i:
                hid_send[k] = result[-cap:]
                go(hid_copy(k))
            if i < groups:
                hid_own[serve_order[i]] = result[:cap]

    sub_c = lax.broadcasted_iota(jnp.int32, (cap, rows), 0)
    lane_c = lax.broadcasted_iota(jnp.int32, (cap, rows), 1)

    def combine(i):
        k = serve_order[i]
        with jax.named_scope("hid%d" % i):
            hid_copy(k).wait_recv()
            if i != here:
                remote(wsend, wrecv.at[k], ws.at[k], wr.at[k], x_mate).wait_recv()
        with jax.named_scope("down%d" % i):
            table = wrecv[k]
            chosen = lane_c == sub_c + k * cap
            w_own = jnp.sum(jnp.where(chosen, table[0:1, :], 0.0), axis=1, keepdims=True)
            w_peer = jnp.sum(jnp.where(chosen, table[1:2, :], 0.0), axis=1, keepdims=True)
            mine, theirs = hid_own[k], hid_recv[k]
            for h in range(halves):
                for c in range(per):
                    cols = slice(h * hw + c * cw, h * hw + (c + 1) * cw)
                    total = jnp.dot(mine, dv[:, cols], preferred_element_type=f32) * w_own
                    total += jnp.dot(theirs, dv_mate[:, cols], preferred_element_type=f32) * w_peer
                    comb[h, k, :, c * cw:(c + 1) * cw] = total.astype(bf)
                if i != here:
                    back_copy(k, h).start()

    def finish(k, h):
        if k == here:
            back = comb[h, k]
        else:
            with jax.named_scope("r%d_%d" % (k, h)):
                back_copy(k, h).wait_recv()
            back = ret[h, k]
        total = send[h, k].astype(f32) + back.astype(f32)
        block = (slice(k * cap, (k + 1) * cap), slice(h * hw, (h + 1) * hw))
        fin[block] = total.astype(bf)
        store = pltpu.make_async_copy(fin.at[block], moved_hbm.at[block], outs.at[k * halves + h])
        store.start()
        stores.append(store)

    spread_ref[...] = spread.astype(bf)
    stores = [pltpu.make_async_copy(spread_ref, spread_hbm, outs.at[groups * halves])]
    stores[0].start()
    gather_rows(pick, att[tp], am_near[...])
    for h in range(halves):
        near_project(h)
        emit(0, h)
    for h in range(halves):
        emit(1, h)
        relay(0, h)
    from_x[1].wait_recv()
    to_mate = [go(d_part(j, dv_mate, 3 + j, {"tp": mate})) for j in range(2)]
    experts(0)
    for h in range(halves):
        emit(2, h)
        relay(1, h)
    experts(1)
    for h in range(halves - 1):
        relay(2, h)
    with jax.named_scope("dmate"):
        d_part(2, dv_mate, 2, {"tp": across}).wait_recv()
        to_mate.append(go(d_part(2, dv_mate, 5, {"tp": mate})))
    emit(here, 0)
    for copy in to_mate:
        copy.wait_recv()
    combine(0)
    relay(2, halves - 1)
    experts(2)
    for h in range(1, halves):
        emit(here, h)
    for h in range(halves):
        relay(here, h)
    combine(1)
    experts(3)
    combine(2)
    experts(4)
    combine(here)
    for k in (0, 2, here, 1):
        for h in range(halves):
            finish(k, h)
    for store in stores:
        store.wait()
    with jax.named_scope("sends"):
        for k in away:
            for h in range(halves):
                z_copy(k, h).wait_send()
                back_copy(k, h).wait_send()
        @pl.when(sp > 0)
        def _():
            for copy in to_before:
                copy.wait_send()

        @pl.when(sp < sp_count - 1)
        def _():
            for copy in to_after:
                copy.wait_send()

        for copy in pending:
            copy.wait_send()


def place_kernel(spread_hbm, rows_hbm, out_hbm, spread, moved, out, ls, ss):
    parts = ls.shape[0] - 1
    cw = out.shape[1] // parts
    cols = [slice(c * cw, (c + 1) * cw) for c in range(parts)]
    first = pltpu.make_async_copy(spread_hbm, spread, ls.at[parts])
    first.start()
    loads = [
        pltpu.make_async_copy(rows_hbm.at[:, c], moved.at[:, c], ls.at[i])
        for i, c in enumerate(cols)
    ]
    stores = [
        pltpu.make_async_copy(out.at[:, c], out_hbm.at[:, c], ss.at[i])
        for i, c in enumerate(cols)
    ]
    for load in loads:
        load.start()
    first.wait()
    for c, load, store in zip(cols, loads, stores):
        load.wait()
        out[:, c] = jnp.dot(
            spread[...], moved[:, c], preferred_element_type=jnp.float32
        ).astype(out.dtype)
        store.start()
    for store in stores:
        store.wait()


def front_kernel(
    chunks, extra, entered, emit,
    sink_ref, q_ref, k_ref, v_ref, doc_ref, res_ref, w_ref,
    out_ref,
    kx, vx, dl, dr, dx, att, am_far, am_near, w_mate, acc, ysend, yrecv,
    hs, hr, ms, mr, ys, yr,
):
    sp = lax.axis_index("sp")
    tp = lax.axis_index("tp")
    sp_count = lax.axis_size("sp")
    mate = tp + 1 - 2 * (tp % 2)
    across = (tp + 2) % 4
    mate_across = (mate + 2) % 4
    after = (sp + 1) % sp_count
    before = (sp + sp_count - 1) % sp_count
    blocks = q_ref.shape[0] // WINDOW
    home_blocks = blocks // 4
    half = blocks // 2
    kv_heads = k_ref.shape[1] // HD
    ratio = q_ref.shape[1] // k_ref.shape[1]
    width = out_ref.shape[1]
    cw = width // chunks
    f32, bf = jnp.float32, jnp.bfloat16
    mesh_id = pl.DeviceIdType.MESH

    def remote(src, dst, ss, rs, where):
        return pltpu.make_async_remote_copy(
            src_ref=src, dst_ref=dst, send_sem=ss, recv_sem=rs,
            device_id=where, device_id_type=mesh_id,
        )

    barrier = pltpu.get_barrier_semaphore()
    for where in ({"sp": after}, {"sp": before}, {"tp": mate}, {"tp": across}):
        pl.semaphore_signal(barrier, inc=1, device_id=where, device_id_type=mesh_id)
    for b in range(blocks):
        kx[b + 1] = k_ref[b * WINDOW:(b + 1) * WINDOW, :]
        vx[b + 1] = v_ref[b * WINDOW:(b + 1) * WINDOW, :]
        dx[b + 1] = jnp.broadcast_to(doc_ref[b:b + 1, :].astype(f32), (8, WINDOW))
    pl.semaphore_wait(barrier, 4 + extra)

    tail = pl.ds((blocks - 1) * WINDOW, WINDOW)
    lead = pl.ds(0, WINDOW)
    halo = [
        remote(k_ref.at[tail], kx.at[0], hs.at[0], hr.at[0], {"sp": after}),
        remote(v_ref.at[tail], vx.at[0], hs.at[1], hr.at[1], {"sp": after}),
        remote(doc_ref, dl, hs.at[2], hr.at[2], {"sp": after}),
        remote(k_ref.at[lead], kx.at[blocks + 1], hs.at[3], hr.at[3], {"sp": before}),
        remote(v_ref.at[lead], vx.at[blocks + 1], hs.at[4], hr.at[4], {"sp": before}),
        remote(doc_ref, dr, hs.at[5], hr.at[5], {"sp": before}),
    ]
    for copy in halo:
        copy.start()
    w_copy = remote(w_ref, w_mate, ms.at[0], mr.at[0], {"tp": mate})
    w_copy.start()
    if entered is not None:
        entered()

    qi = lax.broadcasted_iota(jnp.int32, (WINDOW, 3 * WINDOW), 0)
    ki = lax.broadcasted_iota(jnp.int32, (WINDOW, 3 * WINDOW), 1)
    band = (ki >= qi) & (ki <= qi + 2 * WINDOW)
    eye = lax.broadcasted_iota(jnp.int32, (WINDOW, WINDOW), 0) == lax.broadcasted_iota(
        jnp.int32, (WINDOW, WINDOW), 1
    )

    def attend_block(b):
        own_docs = dx[b + 1][0:1]
        key_docs = jnp.concatenate([dx[b][0:1], own_docs, dx[b + 2][0:1]], axis=1)
        query_docs = jnp.sum(jnp.where(eye, own_docs, 0.0), axis=1, keepdims=True)
        bias = jnp.where(band & (key_docs == query_docs), 0.0, neg_fill)
        keys = kx[pl.ds(b, 3)].reshape(3 * WINDOW, kv_heads * HD)
        values = vx[pl.ds(b, 3)].reshape(3 * WINDOW, kv_heads * HD)
        home = b // home_blocks
        to_rows = pl.ds(pl.multiple_of((b % home_blocks) * WINDOW, WINDOW), WINDOW)
        from_rows = pl.ds(pl.multiple_of(b * WINDOW, WINDOW), WINDOW)
        for g in range(kv_heads):
            span = slice(g * ratio * HD, (g + 1) * ratio * HD)
            q = q_ref[from_rows, span] * jnp.asarray(HD ** (-0.5), bf)
            stacked = jnp.concatenate([q[:, r * HD:(r + 1) * HD] for r in range(ratio)], axis=0)
            scores = lax.dot_general(
                stacked, keys[:, g * HD:(g + 1) * HD], (((1,), (1,)), ((), ())),
                preferred_element_type=f32,
            )
            vg = values[:, g * HD:(g + 1) * HD]
            parts = []
            for r in range(ratio):
                sink = sink_ref[g * ratio + r]
                s = scores[r * WINDOW:(r + 1) * WINDOW] + bias
                top = jnp.maximum(jnp.max(s, axis=1, keepdims=True), sink)
                e = jnp.exp(s - top)
                den = jnp.sum(e, axis=1, keepdims=True) + jnp.exp(sink - top)
                o = jnp.dot(e.astype(bf), vg, preferred_element_type=f32)
                parts.append((o / den).astype(bf))
            att[home, to_rows, span] = jnp.concatenate(parts, axis=1)

    def far_step(i, carry):
        @pl.when(i == half - 1)
        def _():
            for copy in halo:
                copy.wait_recv()
            left = dl[blocks - 1:blocks, :].astype(f32)
            right = dr[0:1, :].astype(f32)
            left = jnp.where(sp == 0, -1.0, left)
            right = jnp.where(sp == sp_count - 1, -1.0, right)
            dx[0] = jnp.broadcast_to(left, (8, WINDOW))
            dx[blocks + 1] = jnp.broadcast_to(right, (8, WINDOW))

        attend_block(jnp.where(tp < 2, half + i, half - 1 - i))
        return carry

    lax.fori_loop(0, half, far_step, 0)
    far_copy = remote(att.at[mate_across], am_far, ms.at[1], mr.at[1], {"tp": mate})
    far_copy.start()
    w_copy.wait_recv()
    far_copy.wait_recv()
    sent = []
    for c in range(chunks):
        cols = slice(c * cw, (c + 1) * cw)
        part = jnp.dot(att[across], w_ref[:, cols], preferred_element_type=f32)
        part += jnp.dot(am_far[...], w_mate[:, cols], preferred_element_type=f32)
        ysend[c] = part.astype(bf)
        copy = remote(ysend.at[c], yrecv.at[c], ys.at[c], yr.at[c], {"tp": across})
        copy.start()
        sent.append(copy)

    def near_step(i, carry):
        attend_block(jnp.where(tp < 2, half - 1 - i, half + i))
        return carry

    lax.fori_loop(0, half, near_step, 0)
    near_copy = remote(att.at[mate], am_near, ms.at[2], mr.at[2], {"tp": mate})
    near_copy.start()
    near_copy.wait_recv()
    for c in range(chunks):
        cols = slice(c * cw, (c + 1) * cw)
        part = jnp.dot(att[tp], w_ref[:, cols], preferred_element_type=f32)
        part += jnp.dot(am_near[...], w_mate[:, cols], preferred_element_type=f32)
        acc[:, cols] = part + res_ref[:, cols].astype(f32)
    for c in range(chunks):
        cols = slice(c * cw, (c + 1) * cw)
        sent[c].wait_recv()
        out_ref[:, cols] = (acc[:, cols] + yrecv[c].astype(f32)).astype(bf)
        if emit is not None:
            emit(c)
    for copy in halo + [w_copy, far_copy, near_copy] + sent:
        copy.wait_send()


def front_scratch(queries, key_rows, residual, out_weight):
    rows, width = residual.shape
    local, heads_width = queries.shape
    kv_width = key_rows.shape[1]
    blocks = local // WINDOW
    bf, f32 = jnp.bfloat16, jnp.float32
    dma = pltpu.SemaphoreType.DMA
    return [
            pltpu.VMEM((blocks + 2, WINDOW, kv_width), bf),
            pltpu.VMEM((blocks + 2, WINDOW, kv_width), bf),
            pltpu.VMEM((blocks, WINDOW), jnp.int32),
            pltpu.VMEM((blocks, WINDOW), jnp.int32),
            pltpu.VMEM((blocks + 2, 8, WINDOW), f32),
            pltpu.VMEM((4, rows, heads_width), bf),
            pltpu.VMEM((rows, heads_width), bf),
            pltpu.VMEM((rows, heads_width), bf),
            pltpu.VMEM(out_weight.shape, bf),
            pltpu.VMEM((rows, width), f32),
            pltpu.VMEM((CHUNKS, rows, width // CHUNKS), bf),
            pltpu.VMEM((CHUNKS, rows, width // CHUNKS), bf),
            dma((6,)), dma((6,)), dma((3,)), dma((3,)), dma((CHUNKS,)), dma((CHUNKS,)),
    ]


def front(queries, key_rows, value_rows, doc_ids, sink_logit, residual, out_weight):
    rows, width = residual.shape
    local, heads_width = queries.shape
    kv_width = key_rows.shape[1]
    blocks = local // WINDOW
    bf, f32 = jnp.bfloat16, jnp.float32
    dma = pltpu.SemaphoreType.DMA
    vm = pl.BlockSpec(memory_space=pltpu.VMEM)
    docs = doc_ids.reshape(blocks, WINDOW)
    return pl.pallas_call(
        functools.partial(front_kernel, CHUNKS, 0, None, None),
        out_shape=jax.ShapeDtypeStruct((rows, width), bf),
        in_specs=[pl.BlockSpec(memory_space=pltpu.SMEM)] + [vm] * 6,
        out_specs=vm,
        scratch_shapes=front_scratch(queries, key_rows, residual, out_weight),
        compiler_params=pltpu.CompilerParams(
            collective_id=4, has_side_effects=True, vmem_limit_bytes=48 * 1024 * 1024
        ),
        name="front",
    )(sink_logit, queries, key_rows, value_rows, docs, residual, out_weight)


def pair_routed(routes, gate_weight):
    count = lax.axis_size("sp")
    experts = count * gate_weight.shape[0]
    return (
        gate_weight.shape[0] == 1
        and routes.shape[1] == 2
        and experts == 2 * GROUPS
    )


def mixture(
    queries, key_rows, value_rows, doc_ids, sink_logit, residual, out_weight,
    norm_gain, routes, route_weights, gate_weight, up_weight, down_weight,
):
    rows, width = residual.shape
    blocks = queries.shape[0] // WINDOW
    heads = queries.shape[1]
    kv_width = key_rows.shape[1]
    docs = doc_ids.reshape(blocks, WINDOW)
    ff = gate_weight.shape[2]
    groups = lax.axis_size("sp") // 2
    cap, hw = rows // groups, width // HALVES
    bf, f32, i32 = jnp.bfloat16, jnp.float32, jnp.int32
    pieces = pltpu.VMEM((HALVES, groups, cap, hw), bf)
    hidden = pltpu.VMEM((groups, cap, ff), bf)
    dma = pltpu.SemaphoreType.DMA
    hbm = pl.BlockSpec(memory_space=pl.ANY)
    edge = pltpu.VMEM((blocks + 2, WINDOW, kv_width), bf)
    per_piece = dma((HALVES, groups))
    moved, spread = pl.pallas_call(
        functools.partial(moe_kernel, groups, HALVES),
        out_shape=(
            jax.ShapeDtypeStruct((rows, width), bf), jax.ShapeDtypeStruct((rows, rows), bf)
        ),
        in_specs=[hbm] * 13,
        out_specs=(hbm, hbm),
        scratch_shapes=[
            pltpu.VMEM((rows, width), bf), pltpu.VMEM((rows, rows), bf),
            pltpu.SMEM(sink_logit.shape, f32), pltpu.VMEM(docs.shape, i32),
            pltpu.VMEM(routes.shape[::-1], i32), pltpu.VMEM(routes.shape[::-1], f32),
            pltpu.VMEM((1, width), f32),
            pltpu.VMEM(queries.shape, bf), pltpu.VMEM((rows, width), bf),
            pltpu.VMEM(out_weight.shape, bf), pltpu.VMEM(out_weight.shape, bf),
            edge, edge,
            pltpu.VMEM((blocks, WINDOW), i32), pltpu.VMEM((blocks, WINDOW), i32),
            pltpu.VMEM((blocks + 2, 8, WINDOW), f32),
            pltpu.VMEM((4, rows, heads), bf),
            pltpu.VMEM((rows, heads), bf), pltpu.VMEM((rows, heads), bf),
            pltpu.VMEM(routes.shape[::-1], i32),
            pltpu.VMEM((rows, 2 * heads), bf),
            pltpu.VMEM((groups, cap, width), f32),
            pieces, pieces, pieces, pieces, pieces, pieces, pieces,
            hidden, hidden, hidden,
            pltpu.VMEM((8, rows), f32), pltpu.VMEM((groups, 8, rows), f32),
            pltpu.VMEM((width, ff), bf), pltpu.VMEM((width, ff), bf),
            pltpu.VMEM((ff, width), bf), pltpu.VMEM((ff, width), bf),
            dma((13,)), dma((6,)), dma((6,)), dma((4,)), dma((4,)),
            per_piece, per_piece, per_piece, per_piece, per_piece, per_piece,
            dma((groups,)), dma((groups,)), per_piece, per_piece,
            dma((groups,)), dma((groups,)), dma((6,)), dma((6,)),
            dma((groups * HALVES + 1,)),
        ],
        compiler_params=pltpu.CompilerParams(
            collective_id=3, has_side_effects=True, vmem_limit_bytes=56 * 1024 * 1024
        ),
        name="mixture",
    )(
        sink_logit, docs, routes.T, route_weights.T, norm_gain[None, :],
        queries, key_rows.reshape(blocks, WINDOW, kv_width),
        value_rows.reshape(blocks, WINDOW, kv_width), residual, out_weight,
        gate_weight, up_weight, down_weight,
    )
    return pl.pallas_call(
        place_kernel,
        out_shape=jax.ShapeDtypeStruct((rows, width), bf),
        in_specs=[hbm, hbm],
        out_specs=hbm,
        scratch_shapes=[
            pltpu.VMEM((rows, rows), bf), pltpu.VMEM((rows, width), bf),
            pltpu.VMEM((rows, width), bf), dma((5,)), dma((4,)),
        ],
        name="place",
    )(spread, moved)


def fits_front(queries):
    return lax.axis_size("tp") == 4 and queries.shape[0] % (8 * WINDOW) == 0


def stream_of(
    queries, key_rows, value_rows, doc_ids, sink_logit, residual, out_weight
):
    local_rows = queries.shape[0]
    if fits_front(queries):
        return front(queries, key_rows, value_rows, doc_ids, sink_logit, residual, out_weight)
    anchor = lax.axis_index("sp") * local_rows
    extent = local_rows * lax.axis_size("sp")
    doc_float = doc_ids.astype(jnp.bfloat16)
    block_rows = min(512, local_rows)
    padded_keys, padded_values, padded_docs = fetch_margins(key_rows, value_rows, doc_float)
    block_parts = []
    for row_start in range(0, local_rows, block_rows):
        key_end = row_start + block_rows + 2 * WINDOW
        block_parts.append(
            attend(
                queries[row_start : row_start + block_rows],
                padded_keys[row_start:key_end],
                padded_values[row_start:key_end],
                doc_float[row_start : row_start + block_rows],
                padded_docs[row_start:key_end],
                anchor + row_start,
                anchor + row_start - WINDOW,
                sink_logit,
                extent,
            )
        )
    attended = jnp.concatenate(block_parts, axis=0)
    regrouped = lax.all_to_all(attended, "tp", split_axis=0, concat_axis=1, tiled=True)
    shard_rows = out_weight.shape[0]
    initial = jnp.zeros((regrouped.shape[0], out_weight.shape[1]), jnp.float32)
    running = initial
    weight_piece = lax.all_gather(out_weight, "tp", axis=0, tiled=True)
    for shard_index in range(weight_piece.shape[0] // shard_rows):
        columns = lax.dynamic_slice_in_dim(regrouped, shard_index * shard_rows, shard_rows, 1)
        partial_value = jnp.dot(
            columns,
            weight_piece[shard_index * shard_rows : (shard_index + 1) * shard_rows],
            preferred_element_type=jnp.float32,
        )
        running = running + partial_value.astype(jnp.bfloat16).astype(jnp.float32)
    stream = (residual.astype(jnp.float32) + running).astype(jnp.bfloat16)
    return stream


def per_device(
    queries,
    key_rows,
    value_rows,
    doc_ids,
    sink_logit,
    residual,
    out_weight,
    norm_gain,
    gate_weight,
    up_weight,
    down_weight,
    routes,
    route_weights,
):
    front_args = (
        queries, key_rows, value_rows, doc_ids, sink_logit, residual, out_weight
    )
    if pair_routed(routes, gate_weight) and fits_front(queries):
        return mixture(
            *front_args, norm_gain, routes, route_weights, gate_weight, up_weight, down_weight
        )
    stream = stream_of(*front_args)
    stream_f = stream.astype(jnp.float32)
    scale = lax.rsqrt(jnp.mean(stream_f * stream_f, axis=1, keepdims=True) + eps_norm)
    normed = (stream_f * scale * norm_gain[None, :]).astype(jnp.bfloat16)
    home_rows = normed.shape[0]
    width = normed.shape[1]
    route_count = routes.shape[1]
    expert_count = lax.axis_size("sp") * gate_weight.shape[0]
    capacity = route_count * home_rows // expert_count
    flat_routes = routes.reshape(-1)
    one_hot = (flat_routes[:, None] == jnp.arange(expert_count, dtype=jnp.int32)[None, :]).astype(
        jnp.int32
    )
    earlier = jnp.cumsum(one_hot, axis=0) - one_hot
    slot_rank = jnp.sum(earlier * one_hot, axis=1)
    slot_index = flat_routes * capacity + slot_rank
    source_row = (
        jnp.zeros((expert_count * capacity,), jnp.int32)
        .at[slot_index]
        .set(jnp.arange(home_rows * route_count, dtype=jnp.int32) // route_count)
    )
    outgoing = normed[source_row].reshape(expert_count, capacity, width)
    incoming = lax.all_to_all(outgoing, "sp", split_axis=0, concat_axis=0, tiled=True)
    flat_rows = incoming.reshape(-1, width)
    gate_act = jnp.dot(flat_rows, gate_weight[0], preferred_element_type=jnp.float32)
    up_act = jnp.dot(flat_rows, up_weight[0], preferred_element_type=jnp.float32)
    hidden = (jax.nn.silu(gate_act) * up_act).astype(jnp.bfloat16)
    produced = jnp.dot(hidden, down_weight[0], preferred_element_type=jnp.float32).astype(
        jnp.bfloat16
    )
    returned = lax.all_to_all(
        produced.reshape(incoming.shape), "sp", split_axis=0, concat_axis=0, tiled=True
    )
    route_out = returned.reshape(-1, width)[slot_index].reshape(home_rows, route_count, width)
    weighted = jnp.sum(route_weights[:, :, None] * route_out.astype(jnp.float32), axis=1)
    return (stream_f + weighted).astype(jnp.bfloat16)


def solution(mesh):
    return jax.shard_map(
        per_device,
        mesh=mesh,
        in_specs=(
            P("sp", "tp"),
            P("sp", "tp"),
            P("sp", "tp"),
            P("sp"),
            P("tp"),
            P(("sp", "tp"), None),
            P("tp", None),
            P(),
            P("sp", None, None),
            P("sp", None, None),
            P("sp", None, None),
            P(("sp", "tp"), None),
            P(("sp", "tp"), None),
        ),
        out_specs=P(("sp", "tp"), None),
        check_vma=False,
    )
```

```python
import functools

import jax
import jax.numpy as jnp
from jax import lax
from jax.experimental import pallas as pl
from jax.experimental.pallas import tpu as pltpu
from jax.sharding import PartitionSpec as P

HD = 64
WINDOW = 128
GROUPS = 4
CHUNKS = 4
HALVES = 2


neg_fill = -1e30
eps_norm = 1e-06


def extended(block, sides, width):
    for axis, dim in sides:
        count = lax.axis_size(axis)
        forward = [(i, i + 1) for i in range(count - 1)]
        backward = [(target, source) for source, target in forward]
        low = lax.ppermute(
            lax.slice_in_dim(block, block.shape[dim] - width, None, axis=dim), axis, forward
        )
        high = lax.ppermute(lax.slice_in_dim(block, 0, width, axis=dim), axis, backward)
        block = jnp.concatenate([low, block, high], axis=dim)
    return block


def attend(
    query_part,
    key_part,
    value_part,
    query_docs,
    key_docs,
    query_start,
    key_start,
    sink_logit,
    extent,
):
    query_count = query_part.shape[0]
    key_count = key_part.shape[0]
    groups = key_part.shape[1] // HD
    head_ratio = sink_logit.shape[0] // groups
    query_heads = query_part.reshape(query_count, groups, head_ratio, HD)
    key_heads = key_part.reshape(key_count, groups, HD)
    value_heads = value_part.reshape(key_count, groups, HD)
    scores = jnp.einsum(
        "qgrd,kgd->grqk", query_heads, key_heads, preferred_element_type=jnp.float32
    ) * HD ** (-0.5)
    query_pos = query_start + jnp.arange(query_count, dtype=jnp.int32)
    key_pos = key_start + jnp.arange(key_count, dtype=jnp.int32)
    inside = (key_pos >= 0) & (key_pos < extent)
    allowed = (
        (jnp.abs(query_pos[:, None] - key_pos[None, :]) <= WINDOW)
        & (query_docs[:, None] == key_docs[None, :])
        & inside[None, :]
    )
    masked = jnp.where(allowed[None, None], scores, neg_fill)
    sink_col = sink_logit.reshape(groups, head_ratio)[:, :, None, None]
    row_top = jnp.maximum(jnp.max(masked, axis=3, keepdims=True), sink_col)
    exponent = jnp.where(allowed[None, None], jnp.exp(masked - row_top), 0.0)
    denominator = jnp.sum(exponent, axis=3, keepdims=True) + jnp.exp(sink_col - row_top)
    attn_weight = (exponent / denominator).astype(jnp.bfloat16)
    attended = jnp.einsum(
        "grqk,kgd->qgrd", attn_weight, value_heads, preferred_element_type=jnp.float32
    )
    return attended.astype(jnp.bfloat16).reshape(query_count, -1)


def fetch_margins(key_rows, value_rows, doc_float):
    return (
        extended(key_rows, (("sp", 0),), WINDOW),
        extended(value_rows, (("sp", 0),), WINDOW),
        extended(doc_float, (("sp", 0),), WINDOW),
    )


def plane_order(gz):
    return [(gz + 2) % 4, 3 - gz, gz + 1 - 2 * (gz % 2), gz]


def slots_of(routes, order, cap):
    rows = routes.shape[1]
    f32, bf = jnp.float32, jnp.bfloat16
    group_of = routes[0:1, :] // 2
    sub = lax.broadcasted_iota(jnp.int32, (8, rows), 0)
    wanted = jnp.full((8, rows), -1, jnp.int32)
    for k, plane in enumerate(order):
        wanted = jnp.where(sub == k, plane, wanted)
    one_hot = jnp.where(group_of == wanted, 1.0, 0.0)
    ri = lax.broadcasted_iota(jnp.int32, (rows, rows), 0)
    ci = lax.broadcasted_iota(jnp.int32, (rows, rows), 1)
    above = jnp.where(ri < ci, 1.0, 0.0).astype(bf)
    ranks = jnp.dot(one_hot.astype(bf), above, preferred_element_type=f32)
    base = sub.astype(f32) * cap
    return jnp.sum((ranks + base) * one_hot, axis=0, keepdims=True)


def moe_kernel(
    groups, halves,
    sink_hbm, doc_hbm, routes_hbm, rw_hbm, gain_hbm,
    q_hbm, k_hbm, v_hbm, res_hbm, w_hbm, gate_hbm, up_hbm, down_hbm,
    moved_hbm, spread_hbm,
    fin, spread_ref, sink_ref, doc_ref, routes_ref, rw_ref, gain_ref,
    qv, resv, wv, w_mate, kx, vx, dl, dr, dx, att, am_far, am_near, routes_far,
    mixed_att, acc, ysend, yrecv, send, own, peer, comb, ret, hid_own, hid_send, hid_recv,
    wsend, wrecv, gv, uv, dv, dv_mate,
    ls, hs, hr, ms, mr, ys, yr, zs, zr, xs, xr, gs, gr, bs, br, ws, wr, ds, dr_sem, outs,
):
    sp = lax.axis_index("sp")
    tp = lax.axis_index("tp")
    sp_count = lax.axis_size("sp")
    gz, side = sp // 2, sp % 2
    x_mate = {"sp": gz * 2 + 1 - side}
    mate = tp + 1 - 2 * (tp % 2)
    core = tp % 2
    across = (tp + 2) % 4
    mate_across = (mate + 2) % 4
    after = (sp + 1) % sp_count
    before = (sp + sp_count - 1) % sp_count
    order = plane_order(gz)
    here = groups - 1
    away = [k for k in range(groups) if k != here]
    rows, width = fin.shape
    cap = rows // groups
    hw = width // halves
    cw = width // 4
    blocks = k_hbm.shape[0]
    home_blocks = blocks // 4
    half = blocks // 2
    kv_heads = k_hbm.shape[2] // HD
    ratio = q_hbm.shape[1] // k_hbm.shape[2]
    heads = q_hbm.shape[1]
    f32, bf = jnp.float32, jnp.bfloat16
    mesh_id = pl.DeviceIdType.MESH

    def remote(src, dst, s_sem, r_sem, where):
        return pltpu.make_async_remote_copy(
            src_ref=src, dst_ref=dst, send_sem=s_sem, recv_sem=r_sem,
            device_id=where, device_id_type=mesh_id,
        )

    end = (gz == 0) | (gz == groups - 1)

    def pick_one(at_end, at_middle):
        return at_end if at_end == at_middle else jnp.where(end, at_end, at_middle)

    emit_order = [pick_one(a, b) for a, b in ((1, 2), (0, 0), (2, 1), (here, here))]
    serve_order = [pick_one(a, b) for a, b in ((1, 0), (2, 2), (0, 1), (here, here))]

    def to_plane(k):
        plane = order[3]
        for i in range(groups - 1):
            plane = jnp.where(k == i, order[i], plane)
        return {"sp": plane * 2 + side}

    barrier = pltpu.get_barrier_semaphore()
    partners = [{"sp": after}, {"sp": before}, {"tp": mate}, {"tp": across}, x_mate]
    partners += [to_plane(k) for k in away]
    for where in partners:
        pl.semaphore_signal(barrier, inc=1, device_id=where, device_id_type=mesh_id)
    pairs = (
        (k_hbm, kx.at[pl.ds(1, blocks)]), (v_hbm, vx.at[pl.ds(1, blocks)]),
        (doc_hbm, doc_ref), (routes_hbm, routes_ref), (rw_hbm, rw_ref), (sink_hbm, sink_ref),
        (q_hbm, qv), (w_hbm, wv), (gain_hbm, gain_ref), (res_hbm, resv),
        (gate_hbm.at[0], gv), (up_hbm.at[0], uv), (down_hbm.at[0], dv),
    )
    loads = [pltpu.make_async_copy(src, dst, ls.at[i]) for i, (src, dst) in enumerate(pairs)]
    for load in loads[:7]:
        load.start()

    @pl.when(sp == 0)
    def _():
        kx[0] = jnp.zeros(kx.shape[1:], bf)
        vx[0] = jnp.zeros(vx.shape[1:], bf)

    @pl.when(sp == sp_count - 1)
    def _():
        kx[blocks + 1] = jnp.zeros(kx.shape[1:], bf)
        vx[blocks + 1] = jnp.zeros(vx.shape[1:], bf)

    for load in loads[:5]:
        load.wait()
    with jax.named_scope("barrier"):
        pl.semaphore_wait(barrier, len(partners))
    pending = []

    def go(copy):
        copy.start()
        pending.append(copy)
        return copy

    def halo_of(i, src, dst, where):
        return remote(src, dst, hs.at[i], hr.at[i], {"sp": where})

    to_after = [
        halo_of(0, kx.at[blocks], kx.at[0], after),
        halo_of(1, vx.at[blocks], vx.at[0], after),
        halo_of(2, doc_ref, dl, after),
    ]
    to_before = [
        halo_of(3, kx.at[1], kx.at[blocks + 1], before),
        halo_of(4, vx.at[1], vx.at[blocks + 1], before),
        halo_of(5, doc_ref, dr, before),
    ]

    def send_before():
        @pl.when(sp > 0)
        def _():
            for copy in to_before:
                copy.start()

    def send_after():
        @pl.when(sp < sp_count - 1)
        def _():
            for copy in to_after:
                copy.start()

    pl.when(tp < 2)(send_before)
    pl.when(tp >= 2)(send_after)
    r_copy = go(remote(routes_ref, routes_far, ms.at[3], mr.at[3], {"tp": across}))
    ff = dv.shape[0]
    quarter, eighth = ff // 4, ff // 8
    chip = tp // 2
    d_rows = [
        pl.ds(pl.multiple_of(start, eighth), count) for start, count in (
            ((2 + chip) * quarter + core * eighth, eighth), (core * quarter, quarter),
            ((3 - chip) * quarter + core * eighth, eighth),
        )
    ]

    def d_part(i, source, sem, where):
        return remote(
            source.at[d_rows[i]], dv_mate.at[d_rows[i]], ds.at[sem], dr_sem.at[sem], where
        )

    from_x = [d_part(i, down_hbm.at[0], i, x_mate) for i in range(2)]
    w_copy = remote(w_hbm, w_mate, ms.at[0], mr.at[0], {"tp": mate})
    for b in range(blocks):
        dx[b + 1] = jnp.broadcast_to(doc_ref[b:b + 1, :].astype(f32), (8, WINDOW))

    def left_halo():
        @pl.when(sp > 0)
        def _():
            for copy in to_after:
                copy.wait_recv()
        left = jnp.where(sp == 0, -1.0, dl[blocks - 1:blocks, :].astype(f32))
        dx[0] = jnp.broadcast_to(left, (8, WINDOW))

    def right_halo():
        @pl.when(sp < sp_count - 1)
        def _():
            for copy in to_before:
                copy.wait_recv()
        right = jnp.where(sp == sp_count - 1, -1.0, dr[0:1, :].astype(f32))
        dx[blocks + 1] = jnp.broadcast_to(right, (8, WINDOW))

    slot = slots_of(routes_ref[...], order, cap)
    ri = lax.broadcasted_iota(jnp.int32, (rows, rows), 0)
    ci = lax.broadcasted_iota(jnp.int32, (rows, rows), 1)
    slot_col = jnp.sum(jnp.where(ri == ci, slot, 0.0), axis=1, keepdims=True)
    spread = jnp.where(slot_col == ci.astype(f32), 1.0, 0.0)
    weight_rows = []
    for parity in (side, 1 - side):
        w_row = jnp.where(routes_ref[0:1, :] % 2 == parity, rw_ref[0:1, :], rw_ref[1:2, :])
        w_col = jnp.sum(jnp.where(ri == ci, w_row, 0.0), axis=1, keepdims=True)
        weight_rows.append(jnp.sum(spread * w_col, axis=0, keepdims=True))
    sub8 = lax.broadcasted_iota(jnp.int32, (8, rows), 0)
    wsend[...] = jnp.where(
        sub8 == 0, weight_rows[0], jnp.where(sub8 == 1, weight_rows[1], 0.0)
    )

    wrecv[here] = wsend[...]

    for k in away:
        go(remote(wsend, wrecv.at[k], ws.at[k], wr.at[k], to_plane(k)))

    qi = lax.broadcasted_iota(jnp.int32, (WINDOW, 3 * WINDOW), 0)
    ki = lax.broadcasted_iota(jnp.int32, (WINDOW, 3 * WINDOW), 1)
    band = (ki >= qi) & (ki <= qi + 2 * WINDOW)
    eye = lax.broadcasted_iota(jnp.int32, (WINDOW, WINDOW), 0) == lax.broadcasted_iota(
        jnp.int32, (WINDOW, WINDOW), 1
    )

    low = lax.broadcasted_iota(jnp.int32, (3 * WINDOW, kv_heads * HD), 1) < HD
    low_q = lax.broadcasted_iota(jnp.int32, (WINDOW, kv_heads * HD), 1) < HD
    zero, one = jnp.zeros((), bf), jnp.ones((), bf)

    def attend_block(b):
        own_docs = dx[b + 1][0:1]
        key_docs = jnp.concatenate([dx[b][0:1], own_docs, dx[b + 2][0:1]], axis=1)
        query_docs = jnp.sum(jnp.where(eye, own_docs, 0.0), axis=1, keepdims=True)
        bias = jnp.where(band & (key_docs == query_docs), 0.0, neg_fill)
        keys = kx[pl.ds(b, 3)].reshape(3 * WINDOW, kv_heads * HD)
        values = vx[pl.ds(b, 3)].reshape(3 * WINDOW, kv_heads * HD)
        key_two = jnp.concatenate(
            [jnp.where(low, keys, zero), jnp.where(low, zero, keys)], axis=0
        )
        value_two = jnp.concatenate([
            jnp.concatenate([jnp.where(low, values, zero), jnp.where(low, one, zero)], axis=1),
            jnp.concatenate([jnp.where(low, zero, values), jnp.where(low, zero, one)], axis=1),
        ], axis=0)
        home = b // home_blocks
        to_rows = pl.ds(pl.multiple_of((b % home_blocks) * WINDOW, WINDOW), WINDOW)
        from_rows = pl.ds(pl.multiple_of(b * WINDOW, WINDOW), WINDOW)
        q = qv[from_rows, :] * jnp.asarray(HD ** (-0.5), bf)
        parts = [None] * (2 * ratio)
        for r in range(ratio):
            pair = jnp.concatenate(
                [q[:, r * HD:(r + 1) * HD], q[:, (ratio + r) * HD:(ratio + r + 1) * HD]], axis=1
            )
            scores = lax.dot_general(
                pair, key_two, (((1,), (1,)), ((), ())), preferred_element_type=f32
            )
            exps, sinks = [], []
            for g in range(2):
                sink = sink_ref[g * ratio + r]
                s = scores[:, g * 3 * WINDOW:(g + 1) * 3 * WINDOW] + bias
                top = jnp.maximum(jnp.max(s, axis=1, keepdims=True), sink)
                exps.append(jnp.exp(s - top).astype(bf))
                sinks.append(jnp.exp(sink - top))
            o = jnp.dot(jnp.concatenate(exps, axis=1), value_two, preferred_element_type=f32)
            den = o[:, 2 * HD:] + jnp.where(low_q, sinks[0], sinks[1])
            both = (o[:, :2 * HD] / den).astype(bf)
            parts[r], parts[ratio + r] = both[:, :HD], both[:, HD:]
        att[home, to_rows, :] = jnp.concatenate(parts, axis=1)

    early = (tp == 1) | (tp == 2)
    far_copy = remote(att.at[mate_across], am_far, ms.at[1], mr.at[1], {"tp": mate})
    near_copy = remote(att.at[mate], am_near, ms.at[2], mr.at[2], {"tp": mate})

    low_side = tp < 2
    starts = [
        jnp.where(low_side, half, home_blocks), jnp.where(low_side, home_blocks, half),
        jnp.where(low_side, half + home_blocks, 0), jnp.where(low_side, 0, half + home_blocks),
    ]

    def attend_home(start):
        for j in range(home_blocks):
            attend_block(start + j)

    def first_pairs(i, carry):
        @pl.when(i == 0)
        def _():
            w_copy.start()

        @pl.when((i == 1) & early)
        def _():
            far_copy.start()

        @pl.when((i == 1) & low_side)
        def _():
            send_after()

        @pl.when((i == 1) & jnp.logical_not(low_side))
        def _():
            send_before()

        @pl.when(i == 1)
        def _():
            for copy in from_x:
                copy.start()

        @pl.when((i == 2) & jnp.logical_not(early))
        def _():
            near_copy.start()

        @pl.when((i == 2) & low_side)
        def _():
            with jax.named_scope("halo_right"):
                right_halo()

        @pl.when((i == 2) & jnp.logical_not(low_side))
        def _():
            with jax.named_scope("halo_left"):
                left_halo()

        attend_home(jnp.where(i == 0, starts[0], jnp.where(i == 1, starts[1], starts[2])))
        return carry

    def pick_of(slot_row):
        return jnp.where(ri.astype(f32) == slot_row, 1.0, 0.0).astype(bf)

    def gather_mine(pick, rows_in):
        mixed_att[:, :heads] = jnp.dot(pick, rows_in, preferred_element_type=f32).astype(bf)

    def gather_mates(pick, rows_in):
        mixed_att[:, heads:] = jnp.dot(pick, rows_in, preferred_element_type=f32).astype(bf)

    def project_mine(cols):
        return jnp.dot(mixed_att[:, :heads], wv[:, cols], preferred_element_type=f32)

    def project_mates(cols):
        return jnp.dot(mixed_att[:, heads:], w_mate[:, cols], preferred_element_type=f32)

    def project(cols):
        return project_mine(cols) + project_mates(cols)

    loads[5].wait()
    loads[6].wait()
    loads[7].start()
    with jax.named_scope("attn_far"):
        lax.fori_loop(0, 3, first_pairs, 0)
    pl.when(jnp.logical_not(early))(far_copy.start)
    pending += [w_copy, far_copy, near_copy] + from_x
    for load in loads[8:]:
        load.start()
    per = 4 // halves
    with jax.named_scope("far_mine"):
        r_copy.wait_recv()
        pick_far = pick_of(slots_of(routes_far[...], order, cap))
        gather_mine(pick_far, att[across])
        loads[7].wait()
        for c in range(per):
            cols = slice(c * cw, (c + 1) * cw)
            acc[:, :, cols] = project_mine(cols).reshape(groups, cap, cw)
    with jax.named_scope("wait_far"):
        w_copy.wait_recv()
        far_copy.wait_recv()
    with jax.named_scope("far_proj"):
        gather_mates(pick_far, am_far[...])

        def y_copy(k, h):
            return remote(
                ysend.at[h, k], yrecv.at[h, k], ys.at[h, k], yr.at[h, k], {"tp": across}
            )

        for h in range(halves):
            for c in range(per):
                cols = slice(h * hw + c * cw, h * hw + (c + 1) * cw)
                if h:
                    part = project(cols).reshape(groups, cap, cw)
                else:
                    part = project_mates(cols).reshape(groups, cap, cw) + acc[:, :, cols]
                ysend[h, :, :, c * cw:(c + 1) * cw] = part.astype(bf)
            if h < halves - 1:
                go(y_copy(emit_order[0], h))
        go(y_copy(emit_order[0], halves - 1))
        for k in emit_order[1:here]:
            for h in range(halves):
                go(y_copy(k, h))

    with jax.named_scope("attn_near"):
        pl.when(tp < 2)(left_halo)
        pl.when(tp >= 2)(right_halo)
        attend_home(starts[3])
        pl.when(early)(near_copy.start)
    for load in loads[8:]:
        load.wait()
    pick = pick_of(slot)
    spread_ref[...] = spread.astype(bf)
    stores = [pltpu.make_async_copy(spread_ref, spread_hbm, outs.at[groups * halves])]
    stores[0].start()
    with jax.named_scope("near_mine"):
        gather_mine(pick, att[tp])
        for c in range(4):
            cols = slice(c * cw, (c + 1) * cw)
            part = project_mine(cols)
            part += jnp.dot(pick, resv[:, cols], preferred_element_type=f32)
            acc[:, :, cols] = part.reshape(groups, cap, cw)
    with jax.named_scope("wait_near"):
        near_copy.wait_recv()
    gather_mates(pick, am_near[...])

    def near_project(h):
        with jax.named_scope("near_proj%d" % h):
            for c in range(per):
                cols = slice(h * hw + c * cw, h * hw + (c + 1) * cw)
                acc[:, :, cols] += project_mates(cols).reshape(groups, cap, cw)

    def z_copy(k, h):
        return remote(send.at[h, k], own.at[h, k], zs.at[h, k], zr.at[h, k], to_plane(k))

    def x_copy(k, h):
        return remote(own.at[h, k], peer.at[h, k], xs.at[h, k], xr.at[h, k], x_mate)

    def hid_copy(k):
        return remote(hid_send.at[k], hid_recv.at[k], gs.at[k], gr.at[k], x_mate)

    def back_copy(k, h):
        return remote(comb.at[h, k], ret.at[h, k], bs.at[h, k], br.at[h, k], to_plane(k))

    def emit(i, h):
        k = emit_order[i]
        with jax.named_scope("y%d_%d" % (i, h)):
            y_copy(k, h).wait_recv()
        cols = slice(h * hw, (h + 1) * hw)
        piece = (acc[k, :, cols] + yrecv[h, k].astype(f32)).astype(bf)
        send[h, k] = piece
        if i == here:
            own[h, here] = piece
        else:
            z_copy(k, h).start()

    def relay(i, h):
        k = serve_order[i]
        if i != here:
            with jax.named_scope("z%d_%d" % (i, h)):
                z_copy(k, h).wait_recv()
        go(x_copy(k, h))

    def relay_when(here_now, i, h):
        k = serve_order[i]

        @pl.when(here_now)
        def _():
            z_copy(k, h).wait_recv()
            x_copy(k, h).start()

        return x_copy(k, h)

    def hidden_of(parts):
        squares = gate_act = up_act = 0.0
        for h in range(halves):
            span = slice(h * hw, (h + 1) * hw)
            wide = jnp.concatenate([buf[h, k] for buf, k in parts], axis=0).astype(f32)
            squares = squares + jnp.sum(wide * wide, axis=1, keepdims=True)
            block = (wide * gain_ref[:, span]).astype(bf)
            gate_act = gate_act + jnp.dot(block, gv[span, :], preferred_element_type=f32)
            up_act = up_act + jnp.dot(block, uv[span, :], preferred_element_type=f32)
        scale = lax.rsqrt(squares / width + eps_norm)
        g = gate_act * scale
        return (g / (1.0 + jnp.exp(-g)) * (up_act * scale)).astype(bf)

    def experts(i):
        k = serve_order[i]
        with jax.named_scope("x%d" % i):
            for h in range(halves):
                x_copy(k, h).wait_recv()
        with jax.named_scope("experts%d" % i):
            result = hidden_of([(own, k), (peer, k)])
            hid_send[k] = result[cap:]
            go(hid_copy(k))
            hid_own[k] = result[:cap]

    sub_c = lax.broadcasted_iota(jnp.int32, (cap, rows), 0)
    lane_c = lax.broadcasted_iota(jnp.int32, (cap, rows), 1)

    def combine(i):
        k = serve_order[i]
        with jax.named_scope("hid%d" % i):
            hid_copy(k).wait_recv()
            if i != here:
                remote(wsend, wrecv.at[k], ws.at[k], wr.at[k], x_mate).wait_recv()
        with jax.named_scope("down%d" % i):
            table = wrecv[k]
            chosen = lane_c == sub_c + k * cap
            w_own = jnp.sum(jnp.where(chosen, table[0:1, :], 0.0), axis=1, keepdims=True)
            w_peer = jnp.sum(jnp.where(chosen, table[1:2, :], 0.0), axis=1, keepdims=True)
            mine, theirs = hid_own[k], hid_recv[k]
            for h in range(halves):
                for c in range(per):
                    cols = slice(h * hw + c * cw, h * hw + (c + 1) * cw)
                    total = jnp.dot(mine, dv[:, cols], preferred_element_type=f32) * w_own
                    total += jnp.dot(theirs, dv_mate[:, cols], preferred_element_type=f32) * w_peer
                    comb[h, k, :, c * cw:(c + 1) * cw] = total.astype(bf)
                if i != here:
                    back_copy(k, h).start()

    def finish(k, h):
        if k == here:
            back = comb[h, k]
        else:
            with jax.named_scope("r%d_%d" % (k, h)):
                back_copy(k, h).wait_recv()
            back = ret[h, k]
        total = send[h, k].astype(f32) + back.astype(f32)
        block = (slice(k * cap, (k + 1) * cap), slice(h * hw, (h + 1) * hw))
        fin[block] = total.astype(bf)
        store = pltpu.make_async_copy(fin.at[block], moved_hbm.at[block], outs.at[k * halves + h])
        store.start()
        stores.append(store)

    for h in range(halves):
        near_project(h)
        emit(0, h)
    from_x[0].wait_recv()
    go(d_part(0, dv_mate, 2, {"tp": across}))
    for h in range(halves):
        go(y_copy(here, h))
    emit(1, 0)
    relay(0, 0)
    emit(1, 1)
    relay(0, 1)
    for h in range(halves):
        emit(2, h)
        relay(1, h)
    from_x[1].wait_recv()
    to_mate = [go(d_part(j, dv_mate, 3 + j, {"tp": mate})) for j in range(2)]
    experts(0)
    relay(2, 0)
    for h in range(1, halves):
        relay_when(end, 2, h)
    with jax.named_scope("dmate"):
        d_part(2, dv_mate, 2, {"tp": across}).wait_recv()
        to_mate.append(go(d_part(2, dv_mate, 5, {"tp": mate})))
    experts(1)
    for copy in to_mate:
        copy.wait_recv()
    combine(0)
    late = [relay_when(jnp.logical_not(end), 2, h) for h in range(1, halves)]
    pending += late
    emit(here, 0)
    relay(here, 0)
    emit(here, 1)
    experts(2)
    relay(here, 1)
    combine(1)
    combine(2)
    experts(here)
    combine(here)
    for k in (0, 2, here, 1):
        for h in range(halves):
            finish(k, h)
    for store in stores:
        store.wait()
    with jax.named_scope("sends"):
        for k in away:
            for h in range(halves):
                z_copy(k, h).wait_send()
                back_copy(k, h).wait_send()
        @pl.when(sp > 0)
        def _():
            for copy in to_before:
                copy.wait_send()

        @pl.when(sp < sp_count - 1)
        def _():
            for copy in to_after:
                copy.wait_send()

        for copy in pending:
            copy.wait_send()


def place_kernel(spread_hbm, rows_hbm, out_hbm, spread, moved, out, ls, ss):
    parts = ls.shape[0] - 1
    cw = out.shape[1] // parts
    cols = [slice(c * cw, (c + 1) * cw) for c in range(parts)]
    first = pltpu.make_async_copy(spread_hbm, spread, ls.at[parts])
    first.start()
    loads = [
        pltpu.make_async_copy(rows_hbm.at[:, c], moved.at[:, c], ls.at[i])
        for i, c in enumerate(cols)
    ]
    stores = [
        pltpu.make_async_copy(out.at[:, c], out_hbm.at[:, c], ss.at[i])
        for i, c in enumerate(cols)
    ]
    for load in loads:
        load.start()
    first.wait()
    for c, load, store in zip(cols, loads, stores):
        load.wait()
        out[:, c] = jnp.dot(
            spread[...], moved[:, c], preferred_element_type=jnp.float32
        ).astype(out.dtype)
        store.start()
    for store in stores:
        store.wait()


def front_kernel(
    chunks, extra, entered, emit,
    sink_ref, q_ref, k_ref, v_ref, doc_ref, res_ref, w_ref,
    out_ref,
    kx, vx, dl, dr, dx, att, am_far, am_near, w_mate, acc, ysend, yrecv,
    hs, hr, ms, mr, ys, yr,
):
    sp = lax.axis_index("sp")
    tp = lax.axis_index("tp")
    sp_count = lax.axis_size("sp")
    mate = tp + 1 - 2 * (tp % 2)
    across = (tp + 2) % 4
    mate_across = (mate + 2) % 4
    after = (sp + 1) % sp_count
    before = (sp + sp_count - 1) % sp_count
    blocks = q_ref.shape[0] // WINDOW
    home_blocks = blocks // 4
    half = blocks // 2
    kv_heads = k_ref.shape[1] // HD
    ratio = q_ref.shape[1] // k_ref.shape[1]
    width = out_ref.shape[1]
    cw = width // chunks
    f32, bf = jnp.float32, jnp.bfloat16
    mesh_id = pl.DeviceIdType.MESH

    def remote(src, dst, ss, rs, where):
        return pltpu.make_async_remote_copy(
            src_ref=src, dst_ref=dst, send_sem=ss, recv_sem=rs,
            device_id=where, device_id_type=mesh_id,
        )

    barrier = pltpu.get_barrier_semaphore()
    for where in ({"sp": after}, {"sp": before}, {"tp": mate}, {"tp": across}):
        pl.semaphore_signal(barrier, inc=1, device_id=where, device_id_type=mesh_id)
    for b in range(blocks):
        kx[b + 1] = k_ref[b * WINDOW:(b + 1) * WINDOW, :]
        vx[b + 1] = v_ref[b * WINDOW:(b + 1) * WINDOW, :]
        dx[b + 1] = jnp.broadcast_to(doc_ref[b:b + 1, :].astype(f32), (8, WINDOW))
    pl.semaphore_wait(barrier, 4 + extra)

    tail = pl.ds((blocks - 1) * WINDOW, WINDOW)
    lead = pl.ds(0, WINDOW)
    halo = [
        remote(k_ref.at[tail], kx.at[0], hs.at[0], hr.at[0], {"sp": after}),
        remote(v_ref.at[tail], vx.at[0], hs.at[1], hr.at[1], {"sp": after}),
        remote(doc_ref, dl, hs.at[2], hr.at[2], {"sp": after}),
        remote(k_ref.at[lead], kx.at[blocks + 1], hs.at[3], hr.at[3], {"sp": before}),
        remote(v_ref.at[lead], vx.at[blocks + 1], hs.at[4], hr.at[4], {"sp": before}),
        remote(doc_ref, dr, hs.at[5], hr.at[5], {"sp": before}),
    ]
    for copy in halo:
        copy.start()
    w_copy = remote(w_ref, w_mate, ms.at[0], mr.at[0], {"tp": mate})
    w_copy.start()
    if entered is not None:
        entered()

    qi = lax.broadcasted_iota(jnp.int32, (WINDOW, 3 * WINDOW), 0)
    ki = lax.broadcasted_iota(jnp.int32, (WINDOW, 3 * WINDOW), 1)
    band = (ki >= qi) & (ki <= qi + 2 * WINDOW)
    eye = lax.broadcasted_iota(jnp.int32, (WINDOW, WINDOW), 0) == lax.broadcasted_iota(
        jnp.int32, (WINDOW, WINDOW), 1
    )

    def attend_block(b):
        own_docs = dx[b + 1][0:1]
        key_docs = jnp.concatenate([dx[b][0:1], own_docs, dx[b + 2][0:1]], axis=1)
        query_docs = jnp.sum(jnp.where(eye, own_docs, 0.0), axis=1, keepdims=True)
        bias = jnp.where(band & (key_docs == query_docs), 0.0, neg_fill)
        keys = kx[pl.ds(b, 3)].reshape(3 * WINDOW, kv_heads * HD)
        values = vx[pl.ds(b, 3)].reshape(3 * WINDOW, kv_heads * HD)
        home = b // home_blocks
        to_rows = pl.ds(pl.multiple_of((b % home_blocks) * WINDOW, WINDOW), WINDOW)
        from_rows = pl.ds(pl.multiple_of(b * WINDOW, WINDOW), WINDOW)
        for g in range(kv_heads):
            span = slice(g * ratio * HD, (g + 1) * ratio * HD)
            q = q_ref[from_rows, span] * jnp.asarray(HD ** (-0.5), bf)
            stacked = jnp.concatenate([q[:, r * HD:(r + 1) * HD] for r in range(ratio)], axis=0)
            scores = lax.dot_general(
                stacked, keys[:, g * HD:(g + 1) * HD], (((1,), (1,)), ((), ())),
                preferred_element_type=f32,
            )
            vg = values[:, g * HD:(g + 1) * HD]
            parts = []
            for r in range(ratio):
                sink = sink_ref[g * ratio + r]
                s = scores[r * WINDOW:(r + 1) * WINDOW] + bias
                top = jnp.maximum(jnp.max(s, axis=1, keepdims=True), sink)
                e = jnp.exp(s - top)
                den = jnp.sum(e, axis=1, keepdims=True) + jnp.exp(sink - top)
                o = jnp.dot(e.astype(bf), vg, preferred_element_type=f32)
                parts.append((o / den).astype(bf))
            att[home, to_rows, span] = jnp.concatenate(parts, axis=1)

    def far_step(i, carry):
        @pl.when(i == half - 1)
        def _():
            for copy in halo:
                copy.wait_recv()
            left = dl[blocks - 1:blocks, :].astype(f32)
            right = dr[0:1, :].astype(f32)
            left = jnp.where(sp == 0, -1.0, left)
            right = jnp.where(sp == sp_count - 1, -1.0, right)
            dx[0] = jnp.broadcast_to(left, (8, WINDOW))
            dx[blocks + 1] = jnp.broadcast_to(right, (8, WINDOW))

        attend_block(jnp.where(tp < 2, half + i, half - 1 - i))
        return carry

    lax.fori_loop(0, half, far_step, 0)
    far_copy = remote(att.at[mate_across], am_far, ms.at[1], mr.at[1], {"tp": mate})
    far_copy.start()
    w_copy.wait_recv()
    far_copy.wait_recv()
    sent = []
    for c in range(chunks):
        cols = slice(c * cw, (c + 1) * cw)
        part = jnp.dot(att[across], w_ref[:, cols], preferred_element_type=f32)
        part += jnp.dot(am_far[...], w_mate[:, cols], preferred_element_type=f32)
        ysend[c] = part.astype(bf)
        copy = remote(ysend.at[c], yrecv.at[c], ys.at[c], yr.at[c], {"tp": across})
        copy.start()
        sent.append(copy)

    def near_step(i, carry):
        attend_block(jnp.where(tp < 2, half - 1 - i, half + i))
        return carry

    lax.fori_loop(0, half, near_step, 0)
    near_copy = remote(att.at[mate], am_near, ms.at[2], mr.at[2], {"tp": mate})
    near_copy.start()
    near_copy.wait_recv()
    for c in range(chunks):
        cols = slice(c * cw, (c + 1) * cw)
        part = jnp.dot(att[tp], w_ref[:, cols], preferred_element_type=f32)
        part += jnp.dot(am_near[...], w_mate[:, cols], preferred_element_type=f32)
        acc[:, cols] = part + res_ref[:, cols].astype(f32)
    for c in range(chunks):
        cols = slice(c * cw, (c + 1) * cw)
        sent[c].wait_recv()
        out_ref[:, cols] = (acc[:, cols] + yrecv[c].astype(f32)).astype(bf)
        if emit is not None:
            emit(c)
    for copy in halo + [w_copy, far_copy, near_copy] + sent:
        copy.wait_send()


def front_scratch(queries, key_rows, residual, out_weight):
    rows, width = residual.shape
    local, heads_width = queries.shape
    kv_width = key_rows.shape[1]
    blocks = local // WINDOW
    bf, f32 = jnp.bfloat16, jnp.float32
    dma = pltpu.SemaphoreType.DMA
    return [
            pltpu.VMEM((blocks + 2, WINDOW, kv_width), bf),
            pltpu.VMEM((blocks + 2, WINDOW, kv_width), bf),
            pltpu.VMEM((blocks, WINDOW), jnp.int32),
            pltpu.VMEM((blocks, WINDOW), jnp.int32),
            pltpu.VMEM((blocks + 2, 8, WINDOW), f32),
            pltpu.VMEM((4, rows, heads_width), bf),
            pltpu.VMEM((rows, heads_width), bf),
            pltpu.VMEM((rows, heads_width), bf),
            pltpu.VMEM(out_weight.shape, bf),
            pltpu.VMEM((rows, width), f32),
            pltpu.VMEM((CHUNKS, rows, width // CHUNKS), bf),
            pltpu.VMEM((CHUNKS, rows, width // CHUNKS), bf),
            dma((6,)), dma((6,)), dma((3,)), dma((3,)), dma((CHUNKS,)), dma((CHUNKS,)),
    ]


def front(queries, key_rows, value_rows, doc_ids, sink_logit, residual, out_weight):
    rows, width = residual.shape
    local, heads_width = queries.shape
    kv_width = key_rows.shape[1]
    blocks = local // WINDOW
    bf, f32 = jnp.bfloat16, jnp.float32
    dma = pltpu.SemaphoreType.DMA
    vm = pl.BlockSpec(memory_space=pltpu.VMEM)
    docs = doc_ids.reshape(blocks, WINDOW)
    return pl.pallas_call(
        functools.partial(front_kernel, CHUNKS, 0, None, None),
        out_shape=jax.ShapeDtypeStruct((rows, width), bf),
        in_specs=[pl.BlockSpec(memory_space=pltpu.SMEM)] + [vm] * 6,
        out_specs=vm,
        scratch_shapes=front_scratch(queries, key_rows, residual, out_weight),
        compiler_params=pltpu.CompilerParams(
            collective_id=4, has_side_effects=True, vmem_limit_bytes=48 * 1024 * 1024
        ),
        name="front",
    )(sink_logit, queries, key_rows, value_rows, docs, residual, out_weight)


def pair_routed(routes, gate_weight):
    count = lax.axis_size("sp")
    experts = count * gate_weight.shape[0]
    return (
        gate_weight.shape[0] == 1
        and routes.shape[1] == 2
        and experts == 2 * GROUPS
    )


def mixture(
    queries, key_rows, value_rows, doc_ids, sink_logit, residual, out_weight,
    norm_gain, routes, route_weights, gate_weight, up_weight, down_weight,
):
    rows, width = residual.shape
    blocks = queries.shape[0] // WINDOW
    heads = queries.shape[1]
    kv_width = key_rows.shape[1]
    docs = doc_ids.reshape(blocks, WINDOW)
    ff = gate_weight.shape[2]
    groups = lax.axis_size("sp") // 2
    cap, hw = rows // groups, width // HALVES
    bf, f32, i32 = jnp.bfloat16, jnp.float32, jnp.int32
    pieces = pltpu.VMEM((HALVES, groups, cap, hw), bf)
    hidden = pltpu.VMEM((groups, cap, ff), bf)
    dma = pltpu.SemaphoreType.DMA
    hbm = pl.BlockSpec(memory_space=pl.ANY)
    edge = pltpu.VMEM((blocks + 2, WINDOW, kv_width), bf)
    per_piece = dma((HALVES, groups))
    moved, spread = pl.pallas_call(
        functools.partial(moe_kernel, groups, HALVES),
        out_shape=(
            jax.ShapeDtypeStruct((rows, width), bf), jax.ShapeDtypeStruct((rows, rows), bf)
        ),
        in_specs=[hbm] * 13,
        out_specs=(hbm, hbm),
        scratch_shapes=[
            pltpu.VMEM((rows, width), bf), pltpu.VMEM((rows, rows), bf),
            pltpu.SMEM(sink_logit.shape, f32), pltpu.VMEM(docs.shape, i32),
            pltpu.VMEM(routes.shape[::-1], i32), pltpu.VMEM(routes.shape[::-1], f32),
            pltpu.VMEM((1, width), f32),
            pltpu.VMEM(queries.shape, bf), pltpu.VMEM((rows, width), bf),
            pltpu.VMEM(out_weight.shape, bf), pltpu.VMEM(out_weight.shape, bf),
            edge, edge,
            pltpu.VMEM((blocks, WINDOW), i32), pltpu.VMEM((blocks, WINDOW), i32),
            pltpu.VMEM((blocks + 2, 8, WINDOW), f32),
            pltpu.VMEM((4, rows, heads), bf),
            pltpu.VMEM((rows, heads), bf), pltpu.VMEM((rows, heads), bf),
            pltpu.VMEM(routes.shape[::-1], i32),
            pltpu.VMEM((rows, 2 * heads), bf),
            pltpu.VMEM((groups, cap, width), f32),
            pieces, pieces, pieces, pieces, pieces, pieces, pieces,
            hidden, hidden, hidden,
            pltpu.VMEM((8, rows), f32), pltpu.VMEM((groups, 8, rows), f32),
            pltpu.VMEM((width, ff), bf), pltpu.VMEM((width, ff), bf),
            pltpu.VMEM((ff, width), bf), pltpu.VMEM((ff, width), bf),
            dma((13,)), dma((6,)), dma((6,)), dma((4,)), dma((4,)),
            per_piece, per_piece, per_piece, per_piece, per_piece, per_piece,
            dma((groups,)), dma((groups,)), per_piece, per_piece,
            dma((groups,)), dma((groups,)), dma((6,)), dma((6,)),
            dma((groups * HALVES + 1,)),
        ],
        compiler_params=pltpu.CompilerParams(
            collective_id=3, has_side_effects=True, vmem_limit_bytes=56 * 1024 * 1024
        ),
        name="mixture",
    )(
        sink_logit, docs, routes.T, route_weights.T, norm_gain[None, :],
        queries, key_rows.reshape(blocks, WINDOW, kv_width),
        value_rows.reshape(blocks, WINDOW, kv_width), residual, out_weight,
        gate_weight, up_weight, down_weight,
    )
    return pl.pallas_call(
        place_kernel,
        out_shape=jax.ShapeDtypeStruct((rows, width), bf),
        in_specs=[hbm, hbm],
        out_specs=hbm,
        scratch_shapes=[
            pltpu.VMEM((rows, rows), bf), pltpu.VMEM((rows, width), bf),
            pltpu.VMEM((rows, width), bf), dma((5,)), dma((4,)),
        ],
        name="place",
    )(spread, moved)


def fits_front(queries):
    return lax.axis_size("tp") == 4 and queries.shape[0] % (8 * WINDOW) == 0


def stream_of(
    queries, key_rows, value_rows, doc_ids, sink_logit, residual, out_weight
):
    local_rows = queries.shape[0]
    if fits_front(queries):
        return front(queries, key_rows, value_rows, doc_ids, sink_logit, residual, out_weight)
    anchor = lax.axis_index("sp") * local_rows
    extent = local_rows * lax.axis_size("sp")
    doc_float = doc_ids.astype(jnp.bfloat16)
    block_rows = min(512, local_rows)
    padded_keys, padded_values, padded_docs = fetch_margins(key_rows, value_rows, doc_float)
    block_parts = []
    for row_start in range(0, local_rows, block_rows):
        key_end = row_start + block_rows + 2 * WINDOW
        block_parts.append(
            attend(
                queries[row_start : row_start + block_rows],
                padded_keys[row_start:key_end],
                padded_values[row_start:key_end],
                doc_float[row_start : row_start + block_rows],
                padded_docs[row_start:key_end],
                anchor + row_start,
                anchor + row_start - WINDOW,
                sink_logit,
                extent,
            )
        )
    attended = jnp.concatenate(block_parts, axis=0)
    regrouped = lax.all_to_all(attended, "tp", split_axis=0, concat_axis=1, tiled=True)
    shard_rows = out_weight.shape[0]
    initial = jnp.zeros((regrouped.shape[0], out_weight.shape[1]), jnp.float32)
    running = initial
    weight_piece = lax.all_gather(out_weight, "tp", axis=0, tiled=True)
    for shard_index in range(weight_piece.shape[0] // shard_rows):
        columns = lax.dynamic_slice_in_dim(regrouped, shard_index * shard_rows, shard_rows, 1)
        partial_value = jnp.dot(
            columns,
            weight_piece[shard_index * shard_rows : (shard_index + 1) * shard_rows],
            preferred_element_type=jnp.float32,
        )
        running = running + partial_value.astype(jnp.bfloat16).astype(jnp.float32)
    stream = (residual.astype(jnp.float32) + running).astype(jnp.bfloat16)
    return stream


def per_device(
    queries,
    key_rows,
    value_rows,
    doc_ids,
    sink_logit,
    residual,
    out_weight,
    norm_gain,
    gate_weight,
    up_weight,
    down_weight,
    routes,
    route_weights,
):
    front_args = (
        queries, key_rows, value_rows, doc_ids, sink_logit, residual, out_weight
    )
    if pair_routed(routes, gate_weight) and fits_front(queries):
        return mixture(
            *front_args, norm_gain, routes, route_weights, gate_weight, up_weight, down_weight
        )
    stream = stream_of(*front_args)
    stream_f = stream.astype(jnp.float32)
    scale = lax.rsqrt(jnp.mean(stream_f * stream_f, axis=1, keepdims=True) + eps_norm)
    normed = (stream_f * scale * norm_gain[None, :]).astype(jnp.bfloat16)
    home_rows = normed.shape[0]
    width = normed.shape[1]
    route_count = routes.shape[1]
    expert_count = lax.axis_size("sp") * gate_weight.shape[0]
    capacity = route_count * home_rows // expert_count
    flat_routes = routes.reshape(-1)
    one_hot = (flat_routes[:, None] == jnp.arange(expert_count, dtype=jnp.int32)[None, :]).astype(
        jnp.int32
    )
    earlier = jnp.cumsum(one_hot, axis=0) - one_hot
    slot_rank = jnp.sum(earlier * one_hot, axis=1)
    slot_index = flat_routes * capacity + slot_rank
    source_row = (
        jnp.zeros((expert_count * capacity,), jnp.int32)
        .at[slot_index]
        .set(jnp.arange(home_rows * route_count, dtype=jnp.int32) // route_count)
    )
    outgoing = normed[source_row].reshape(expert_count, capacity, width)
    incoming = lax.all_to_all(outgoing, "sp", split_axis=0, concat_axis=0, tiled=True)
    flat_rows = incoming.reshape(-1, width)
    gate_act = jnp.dot(flat_rows, gate_weight[0], preferred_element_type=jnp.float32)
    up_act = jnp.dot(flat_rows, up_weight[0], preferred_element_type=jnp.float32)
    hidden = (jax.nn.silu(gate_act) * up_act).astype(jnp.bfloat16)
    produced = jnp.dot(hidden, down_weight[0], preferred_element_type=jnp.float32).astype(
        jnp.bfloat16
    )
    returned = lax.all_to_all(
        produced.reshape(incoming.shape), "sp", split_axis=0, concat_axis=0, tiled=True
    )
    route_out = returned.reshape(-1, width)[slot_index].reshape(home_rows, route_count, width)
    weighted = jnp.sum(route_weights[:, :, None] * route_out.astype(jnp.float32), axis=1)
    return (stream_f + weighted).astype(jnp.bfloat16)


def solution(mesh):
    return jax.shard_map(
        per_device,
        mesh=mesh,
        in_specs=(
            P("sp", "tp"),
            P("sp", "tp"),
            P("sp", "tp"),
            P("sp"),
            P("tp"),
            P(("sp", "tp"), None),
            P("tp", None),
            P(),
            P("sp", None, None),
            P("sp", None, None),
            P("sp", None, None),
            P(("sp", "tp"), None),
            P(("sp", "tp"), None),
        ),
        out_specs=P(("sp", "tp"), None),
        check_vma=False,
    )
```

```python
import functools

import jax
import jax.numpy as jnp
from jax import lax
from jax.experimental import pallas as pl
from jax.experimental.pallas import tpu as pltpu
from jax.sharding import PartitionSpec as P

HD = 64
WINDOW = 128
GROUPS = 4
CHUNKS = 4
HALVES = 2


neg_fill = -1e30
eps_norm = 1e-06


def extended(block, sides, width):
    for axis, dim in sides:
        count = lax.axis_size(axis)
        forward = [(i, i + 1) for i in range(count - 1)]
        backward = [(target, source) for source, target in forward]
        low = lax.ppermute(
            lax.slice_in_dim(block, block.shape[dim] - width, None, axis=dim), axis, forward
        )
        high = lax.ppermute(lax.slice_in_dim(block, 0, width, axis=dim), axis, backward)
        block = jnp.concatenate([low, block, high], axis=dim)
    return block


def attend(
    query_part,
    key_part,
    value_part,
    query_docs,
    key_docs,
    query_start,
    key_start,
    sink_logit,
    extent,
):
    query_count = query_part.shape[0]
    key_count = key_part.shape[0]
    groups = key_part.shape[1] // HD
    head_ratio = sink_logit.shape[0] // groups
    query_heads = query_part.reshape(query_count, groups, head_ratio, HD)
    key_heads = key_part.reshape(key_count, groups, HD)
    value_heads = value_part.reshape(key_count, groups, HD)
    scores = jnp.einsum(
        "qgrd,kgd->grqk", query_heads, key_heads, preferred_element_type=jnp.float32
    ) * HD ** (-0.5)
    query_pos = query_start + jnp.arange(query_count, dtype=jnp.int32)
    key_pos = key_start + jnp.arange(key_count, dtype=jnp.int32)
    inside = (key_pos >= 0) & (key_pos < extent)
    allowed = (
        (jnp.abs(query_pos[:, None] - key_pos[None, :]) <= WINDOW)
        & (query_docs[:, None] == key_docs[None, :])
        & inside[None, :]
    )
    masked = jnp.where(allowed[None, None], scores, neg_fill)
    sink_col = sink_logit.reshape(groups, head_ratio)[:, :, None, None]
    row_top = jnp.maximum(jnp.max(masked, axis=3, keepdims=True), sink_col)
    exponent = jnp.where(allowed[None, None], jnp.exp(masked - row_top), 0.0)
    denominator = jnp.sum(exponent, axis=3, keepdims=True) + jnp.exp(sink_col - row_top)
    attn_weight = (exponent / denominator).astype(jnp.bfloat16)
    attended = jnp.einsum(
        "grqk,kgd->qgrd", attn_weight, value_heads, preferred_element_type=jnp.float32
    )
    return attended.astype(jnp.bfloat16).reshape(query_count, -1)


def fetch_margins(key_rows, value_rows, doc_float):
    return (
        extended(key_rows, (("sp", 0),), WINDOW),
        extended(value_rows, (("sp", 0),), WINDOW),
        extended(doc_float, (("sp", 0),), WINDOW),
    )


def plane_order(gz):
    return [(gz + 2) % 4, 3 - gz, gz + 1 - 2 * (gz % 2), gz]


def slots_of(routes, order, cap):
    rows = routes.shape[1]
    f32, bf = jnp.float32, jnp.bfloat16
    group_of = routes[0:1, :] // 2
    sub = lax.broadcasted_iota(jnp.int32, (8, rows), 0)
    wanted = jnp.full((8, rows), -1, jnp.int32)
    for k, plane in enumerate(order):
        wanted = jnp.where(sub == k, plane, wanted)
    one_hot = jnp.where(group_of == wanted, 1.0, 0.0)
    ri = lax.broadcasted_iota(jnp.int32, (rows, rows), 0)
    ci = lax.broadcasted_iota(jnp.int32, (rows, rows), 1)
    above = jnp.where(ri < ci, 1.0, 0.0).astype(bf)
    ranks = jnp.dot(one_hot.astype(bf), above, preferred_element_type=f32)
    base = sub.astype(f32) * cap
    return jnp.sum((ranks + base) * one_hot, axis=0, keepdims=True)


def moe_kernel(
    groups, halves,
    sink_hbm, doc_hbm, routes_hbm, rw_hbm, gain_hbm,
    q_hbm, k_hbm, v_hbm, res_hbm, w_hbm, gate_hbm, up_hbm, down_hbm,
    moved_hbm, spread_hbm,
    fin, spread_ref, sink_ref, doc_ref, routes_ref, rw_ref, gain_ref,
    qv, resv, wv, w_mate, kx, vx, dl, dr, dx, att, am_far, am_near, routes_far,
    mixed_att, acc, ysend, yrecv, send, own, peer, comb, ret, hid_own, hid_send, hid_recv,
    wsend, wrecv, gv, uv, dv, dv_mate,
    ls, hs, hr, ms, mr, ys, yr, zs, zr, xs, xr, gs, gr, bs, br, ws, wr, ds, dr_sem, outs, known,
):
    sp = lax.axis_index("sp")
    tp = lax.axis_index("tp")
    sp_count = lax.axis_size("sp")
    gz, side = sp // 2, sp % 2
    x_mate = {"sp": gz * 2 + 1 - side}
    mate = tp + 1 - 2 * (tp % 2)
    core = tp % 2
    across = (tp + 2) % 4
    mate_across = (mate + 2) % 4
    after = (sp + 1) % sp_count
    before = (sp + sp_count - 1) % sp_count
    order = plane_order(gz)
    here = groups - 1
    away = [k for k in range(groups) if k != here]
    rows, width = fin.shape
    cap = rows // groups
    hw = width // halves
    cw = width // 4
    blocks = k_hbm.shape[0]
    home_blocks = blocks // 4
    half = blocks // 2
    kv_heads = k_hbm.shape[2] // HD
    ratio = q_hbm.shape[1] // k_hbm.shape[2]
    heads = q_hbm.shape[1]
    f32, bf = jnp.float32, jnp.bfloat16
    mesh_id = pl.DeviceIdType.MESH

    def remote(src, dst, s_sem, r_sem, where):
        return pltpu.make_async_remote_copy(
            src_ref=src, dst_ref=dst, send_sem=s_sem, recv_sem=r_sem,
            device_id=where, device_id_type=mesh_id,
        )

    end = (gz == 0) | (gz == groups - 1)

    def pick_one(at_end, at_middle):
        return at_end if at_end == at_middle else jnp.where(end, at_end, at_middle)

    emit_order = [pick_one(a, b) for a, b in ((1, 2), (0, 0), (2, 1), (here, here))]
    serve_order = [pick_one(a, b) for a, b in ((1, 0), (2, 2), (0, 1), (here, here))]

    def to_plane(k):
        plane = order[3]
        for i in range(groups - 1):
            plane = jnp.where(k == i, order[i], plane)
        return {"sp": plane * 2 + side}

    barrier = pltpu.get_barrier_semaphore()

    def signal(sem, where):
        pl.semaphore_signal(sem, inc=1, device_id=where, device_id_type=mesh_id)

    for where in ({"tp": mate}, {"tp": across}, x_mate):
        signal(barrier, where)
    pl.when(sp > 0)(lambda: signal(barrier, {"sp": before}))
    pl.when(sp < sp_count - 1)(lambda: signal(barrier, {"sp": after}))
    pl.when(gz > 0)(lambda: signal(barrier, {"sp": sp - 2}))
    pl.when(gz < groups - 1)(lambda: signal(barrier, {"sp": sp + 2}))
    greeted = 7 - jnp.where((sp == 0) | (sp == sp_count - 1), 1, 0) - jnp.where(end, 1, 0)
    pairs = (
        (k_hbm, kx.at[pl.ds(1, blocks)]), (v_hbm, vx.at[pl.ds(1, blocks)]),
        (doc_hbm, doc_ref), (routes_hbm, routes_ref), (rw_hbm, rw_ref), (sink_hbm, sink_ref),
        (q_hbm, qv), (w_hbm, wv), (gain_hbm, gain_ref), (res_hbm, resv),
        (gate_hbm.at[0], gv), (up_hbm.at[0], uv), (down_hbm.at[0], dv),
    )
    loads = [pltpu.make_async_copy(src, dst, ls.at[i]) for i, (src, dst) in enumerate(pairs)]
    for load in loads[:7]:
        load.start()

    @pl.when(sp == 0)
    def _():
        kx[0] = jnp.zeros(kx.shape[1:], bf)
        vx[0] = jnp.zeros(vx.shape[1:], bf)

    @pl.when(sp == sp_count - 1)
    def _():
        kx[blocks + 1] = jnp.zeros(kx.shape[1:], bf)
        vx[blocks + 1] = jnp.zeros(vx.shape[1:], bf)

    for load in loads[:5]:
        load.wait()
    with jax.named_scope("barrier"):
        pl.semaphore_wait(barrier, greeted)

    @pl.when(jnp.logical_not(end))
    def _():
        signal(known, {"sp": sp - 2})
        signal(known, {"sp": sp + 2})

    pending = []

    def go(copy):
        copy.start()
        pending.append(copy)
        return copy

    def halo_of(i, src, dst, where):
        return remote(src, dst, hs.at[i], hr.at[i], {"sp": where})

    to_after = [
        halo_of(0, kx.at[blocks], kx.at[0], after),
        halo_of(1, vx.at[blocks], vx.at[0], after),
        halo_of(2, doc_ref, dl, after),
    ]
    to_before = [
        halo_of(3, kx.at[1], kx.at[blocks + 1], before),
        halo_of(4, vx.at[1], vx.at[blocks + 1], before),
        halo_of(5, doc_ref, dr, before),
    ]

    def send_before():
        @pl.when(sp > 0)
        def _():
            for copy in to_before:
                copy.start()

    def send_after():
        @pl.when(sp < sp_count - 1)
        def _():
            for copy in to_after:
                copy.start()

    pl.when(tp < 2)(send_before)
    pl.when(tp >= 2)(send_after)
    r_copy = go(remote(routes_ref, routes_far, ms.at[3], mr.at[3], {"tp": across}))
    ff = dv.shape[0]
    quarter, eighth = ff // 4, ff // 8
    chip = tp // 2
    d_rows = [
        pl.ds(pl.multiple_of(start, eighth), count) for start, count in (
            ((2 + chip) * quarter + core * eighth, eighth), (core * quarter, quarter),
            ((3 - chip) * quarter + core * eighth, eighth),
        )
    ]

    def d_part(i, source, sem, where):
        return remote(
            source.at[d_rows[i]], dv_mate.at[d_rows[i]], ds.at[sem], dr_sem.at[sem], where
        )

    from_x = [d_part(i, down_hbm.at[0], i, x_mate) for i in range(2)]
    w_copy = remote(w_hbm, w_mate, ms.at[0], mr.at[0], {"tp": mate})
    for b in range(blocks):
        dx[b + 1] = jnp.broadcast_to(doc_ref[b:b + 1, :].astype(f32), (8, WINDOW))

    def left_halo():
        @pl.when(sp > 0)
        def _():
            for copy in to_after:
                copy.wait_recv()
        left = jnp.where(sp == 0, -1.0, dl[blocks - 1:blocks, :].astype(f32))
        dx[0] = jnp.broadcast_to(left, (8, WINDOW))

    def right_halo():
        @pl.when(sp < sp_count - 1)
        def _():
            for copy in to_before:
                copy.wait_recv()
        right = jnp.where(sp == sp_count - 1, -1.0, dr[0:1, :].astype(f32))
        dx[blocks + 1] = jnp.broadcast_to(right, (8, WINDOW))

    ri = lax.broadcasted_iota(jnp.int32, (rows, rows), 0)
    ci = lax.broadcasted_iota(jnp.int32, (rows, rows), 1)
    qi = lax.broadcasted_iota(jnp.int32, (WINDOW, 3 * WINDOW), 0)
    ki = lax.broadcasted_iota(jnp.int32, (WINDOW, 3 * WINDOW), 1)
    band = (ki >= qi) & (ki <= qi + 2 * WINDOW)
    eye = lax.broadcasted_iota(jnp.int32, (WINDOW, WINDOW), 0) == lax.broadcasted_iota(
        jnp.int32, (WINDOW, WINDOW), 1
    )

    low = lax.broadcasted_iota(jnp.int32, (3 * WINDOW, kv_heads * HD), 1) < HD
    low_q = lax.broadcasted_iota(jnp.int32, (WINDOW, kv_heads * HD), 1) < HD
    zero, one = jnp.zeros((), bf), jnp.ones((), bf)

    def attend_block(b):
        own_docs = dx[b + 1][0:1]
        key_docs = jnp.concatenate([dx[b][0:1], own_docs, dx[b + 2][0:1]], axis=1)
        query_docs = jnp.sum(jnp.where(eye, own_docs, 0.0), axis=1, keepdims=True)
        bias = jnp.where(band & (key_docs == query_docs), 0.0, neg_fill)
        keys = kx[pl.ds(b, 3)].reshape(3 * WINDOW, kv_heads * HD)
        values = vx[pl.ds(b, 3)].reshape(3 * WINDOW, kv_heads * HD)
        key_two = jnp.concatenate(
            [jnp.where(low, keys, zero), jnp.where(low, zero, keys)], axis=0
        )
        value_two = jnp.concatenate([
            jnp.concatenate([jnp.where(low, values, zero), jnp.where(low, one, zero)], axis=1),
            jnp.concatenate([jnp.where(low, zero, values), jnp.where(low, zero, one)], axis=1),
        ], axis=0)
        home = b // home_blocks
        to_rows = pl.ds(pl.multiple_of((b % home_blocks) * WINDOW, WINDOW), WINDOW)
        from_rows = pl.ds(pl.multiple_of(b * WINDOW, WINDOW), WINDOW)
        q = qv[from_rows, :] * jnp.asarray(HD ** (-0.5), bf)
        parts = [None] * (2 * ratio)
        for r in range(ratio):
            pair = jnp.concatenate(
                [q[:, r * HD:(r + 1) * HD], q[:, (ratio + r) * HD:(ratio + r + 1) * HD]], axis=1
            )
            scores = lax.dot_general(
                pair, key_two, (((1,), (1,)), ((), ())), preferred_element_type=f32
            )
            exps, sinks = [], []
            for g in range(2):
                sink = sink_ref[g * ratio + r]
                s = scores[:, g * 3 * WINDOW:(g + 1) * 3 * WINDOW] + bias
                top = jnp.maximum(jnp.max(s, axis=1, keepdims=True), sink)
                exps.append(jnp.exp(s - top).astype(bf))
                sinks.append(jnp.exp(sink - top))
            o = jnp.dot(jnp.concatenate(exps, axis=1), value_two, preferred_element_type=f32)
            den = o[:, 2 * HD:] + jnp.where(low_q, sinks[0], sinks[1])
            both = (o[:, :2 * HD] / den).astype(bf)
            parts[r], parts[ratio + r] = both[:, :HD], both[:, HD:]
        att[home, to_rows, :] = jnp.concatenate(parts, axis=1)

    early = (tp == 1) | (tp == 2)
    far_copy = remote(att.at[mate_across], am_far, ms.at[1], mr.at[1], {"tp": mate})
    near_copy = remote(att.at[mate], am_near, ms.at[2], mr.at[2], {"tp": mate})

    low_side = tp < 2
    starts = [
        jnp.where(low_side, half, home_blocks), jnp.where(low_side, home_blocks, half),
        jnp.where(low_side, half + home_blocks, 0), jnp.where(low_side, 0, half + home_blocks),
    ]

    def attend_home(start):
        for j in range(home_blocks):
            attend_block(start + j)

    def first_pairs(i, carry):
        @pl.when(i == 0)
        def _():
            w_copy.start()

        @pl.when((i == 1) & early)
        def _():
            far_copy.start()

        @pl.when((i == 1) & low_side)
        def _():
            send_after()

        @pl.when((i == 1) & jnp.logical_not(low_side))
        def _():
            send_before()

        @pl.when(i == 1)
        def _():
            for copy in from_x:
                copy.start()

        @pl.when((i == 1) & jnp.logical_not(end))
        def _():
            pl.semaphore_wait(known, 1)
            signal(known, {"sp": (gz - 1) * (groups - 1) * 2 + side})

        @pl.when((i == 2) & jnp.logical_not(early))
        def _():
            near_copy.start()

        @pl.when((i == 2) & low_side)
        def _():
            with jax.named_scope("halo_right"):
                right_halo()

        @pl.when((i == 2) & jnp.logical_not(low_side))
        def _():
            with jax.named_scope("halo_left"):
                left_halo()

        attend_home(jnp.where(i == 0, starts[0], jnp.where(i == 1, starts[1], starts[2])))
        return carry

    def pick_of(slot_row):
        return jnp.where(ri.astype(f32) == slot_row, 1.0, 0.0).astype(bf)

    def gather_mine(pick, rows_in):
        mixed_att[:, :heads] = jnp.dot(pick, rows_in, preferred_element_type=f32).astype(bf)

    def gather_mates(pick, rows_in):
        mixed_att[:, heads:] = jnp.dot(pick, rows_in, preferred_element_type=f32).astype(bf)

    def project_mine(cols):
        return jnp.dot(mixed_att[:, :heads], wv[:, cols], preferred_element_type=f32)

    def project_mates(cols):
        return jnp.dot(mixed_att[:, heads:], w_mate[:, cols], preferred_element_type=f32)

    def project(cols):
        return project_mine(cols) + project_mates(cols)

    loads[5].wait()
    loads[6].wait()
    loads[7].start()
    with jax.named_scope("attn_far"):
        lax.fori_loop(0, 3, first_pairs, 0)
    pl.when(jnp.logical_not(early))(far_copy.start)
    pending += [w_copy, far_copy, near_copy] + from_x
    for load in loads[8:]:
        load.start()
    per = 4 // halves
    with jax.named_scope("far_mine"):
        r_copy.wait_recv()
        pick_far = pick_of(slots_of(routes_far[...], order, cap))
        gather_mine(pick_far, att[across])
        loads[7].wait()
        for c in range(per):
            cols = slice(c * cw, (c + 1) * cw)
            acc[:, :, cols] = project_mine(cols).reshape(groups, cap, cw)
    with jax.named_scope("wait_far"):
        w_copy.wait_recv()
        far_copy.wait_recv()
    with jax.named_scope("far_proj"):
        gather_mates(pick_far, am_far[...])

        def y_copy(k, h):
            return remote(
                ysend.at[h, k], yrecv.at[h, k], ys.at[h, k], yr.at[h, k], {"tp": across}
            )

        for h in range(halves):
            for c in range(per):
                cols = slice(h * hw + c * cw, h * hw + (c + 1) * cw)
                if h:
                    part = project(cols).reshape(groups, cap, cw)
                else:
                    part = project_mates(cols).reshape(groups, cap, cw) + acc[:, :, cols]
                ysend[h, :, :, c * cw:(c + 1) * cw] = part.astype(bf)
            if h < halves - 1:
                go(y_copy(emit_order[0], h))
        go(y_copy(emit_order[0], halves - 1))
        for k in emit_order[1:here]:
            for h in range(halves):
                go(y_copy(k, h))

    slot = slots_of(routes_ref[...], order, cap)
    slot_col = jnp.sum(jnp.where(ri == ci, slot, 0.0), axis=1, keepdims=True)
    spread = jnp.where(slot_col == ci.astype(f32), 1.0, 0.0)
    weight_rows = []
    for parity in (side, 1 - side):
        w_row = jnp.where(routes_ref[0:1, :] % 2 == parity, rw_ref[0:1, :], rw_ref[1:2, :])
        w_col = jnp.sum(jnp.where(ri == ci, w_row, 0.0), axis=1, keepdims=True)
        weight_rows.append(jnp.sum(spread * w_col, axis=0, keepdims=True))
    sub8 = lax.broadcasted_iota(jnp.int32, (8, rows), 0)
    wsend[...] = jnp.where(
        sub8 == 0, weight_rows[0], jnp.where(sub8 == 1, weight_rows[1], 0.0)
    )

    wrecv[here] = wsend[...]

    @pl.when(end)
    def _():
        pl.semaphore_wait(known, 2)

    for k in away:
        go(remote(wsend, wrecv.at[k], ws.at[k], wr.at[k], to_plane(k)))

    with jax.named_scope("attn_near"):
        pl.when(tp < 2)(left_halo)
        pl.when(tp >= 2)(right_halo)
        attend_home(starts[3])
        pl.when(early)(near_copy.start)
    for load in loads[8:]:
        load.wait()
    pick = pick_of(slot)
    spread_ref[...] = spread.astype(bf)
    stores = [pltpu.make_async_copy(spread_ref, spread_hbm, outs.at[groups * halves])]
    stores[0].start()
    with jax.named_scope("near_mine"):
        gather_mine(pick, att[tp])
        for c in range(4):
            cols = slice(c * cw, (c + 1) * cw)
            part = project_mine(cols)
            part += jnp.dot(pick, resv[:, cols], preferred_element_type=f32)
            acc[:, :, cols] = part.reshape(groups, cap, cw)
    with jax.named_scope("wait_near"):
        near_copy.wait_recv()
    gather_mates(pick, am_near[...])

    def near_project(h):
        with jax.named_scope("near_proj%d" % h):
            for c in range(per):
                cols = slice(h * hw + c * cw, h * hw + (c + 1) * cw)
                acc[:, :, cols] += project_mates(cols).reshape(groups, cap, cw)

    def z_copy(k, h):
        return remote(send.at[h, k], own.at[h, k], zs.at[h, k], zr.at[h, k], to_plane(k))

    def x_copy(k, h):
        return remote(own.at[h, k], peer.at[h, k], xs.at[h, k], xr.at[h, k], x_mate)

    def hid_copy(k):
        return remote(hid_send.at[k], hid_recv.at[k], gs.at[k], gr.at[k], x_mate)

    def back_copy(k, h):
        return remote(comb.at[h, k], ret.at[h, k], bs.at[h, k], br.at[h, k], to_plane(k))

    def emit(i, h):
        k = emit_order[i]
        with jax.named_scope("y%d_%d" % (i, h)):
            y_copy(k, h).wait_recv()
        cols = slice(h * hw, (h + 1) * hw)
        piece = (acc[k, :, cols] + yrecv[h, k].astype(f32)).astype(bf)
        send[h, k] = piece
        if i == here:
            own[h, here] = piece
        else:
            z_copy(k, h).start()

    def relay(i, h):
        k = serve_order[i]
        if i != here:
            with jax.named_scope("z%d_%d" % (i, h)):
                z_copy(k, h).wait_recv()
        go(x_copy(k, h))

    def relay_when(here_now, i, h):
        k = serve_order[i]

        @pl.when(here_now)
        def _():
            z_copy(k, h).wait_recv()
            x_copy(k, h).start()

        return x_copy(k, h)

    def hidden_of(parts):
        squares = gate_act = up_act = 0.0
        for h in range(halves):
            span = slice(h * hw, (h + 1) * hw)
            wide = jnp.concatenate([buf[h, k] for buf, k in parts], axis=0).astype(f32)
            squares = squares + jnp.sum(wide * wide, axis=1, keepdims=True)
            block = (wide * gain_ref[:, span]).astype(bf)
            gate_act = gate_act + jnp.dot(block, gv[span, :], preferred_element_type=f32)
            up_act = up_act + jnp.dot(block, uv[span, :], preferred_element_type=f32)
        scale = lax.rsqrt(squares / width + eps_norm)
        g = gate_act * scale
        return (g / (1.0 + jnp.exp(-g)) * (up_act * scale)).astype(bf)

    def experts(i):
        k = serve_order[i]
        with jax.named_scope("x%d" % i):
            for h in range(halves):
                x_copy(k, h).wait_recv()
        with jax.named_scope("experts%d" % i):
            result = hidden_of([(own, k), (peer, k)])
            hid_send[k] = result[cap:]
            go(hid_copy(k))
            hid_own[k] = result[:cap]

    sub_c = lax.broadcasted_iota(jnp.int32, (cap, rows), 0)
    lane_c = lax.broadcasted_iota(jnp.int32, (cap, rows), 1)

    def combine(i):
        k = serve_order[i]
        with jax.named_scope("hid%d" % i):
            hid_copy(k).wait_recv()
            if i != here:
                remote(wsend, wrecv.at[k], ws.at[k], wr.at[k], x_mate).wait_recv()
        with jax.named_scope("down%d" % i):
            table = wrecv[k]
            chosen = lane_c == sub_c + k * cap
            w_own = jnp.sum(jnp.where(chosen, table[0:1, :], 0.0), axis=1, keepdims=True)
            w_peer = jnp.sum(jnp.where(chosen, table[1:2, :], 0.0), axis=1, keepdims=True)
            mine, theirs = hid_own[k], hid_recv[k]
            for h in range(halves):
                for c in range(per):
                    cols = slice(h * hw + c * cw, h * hw + (c + 1) * cw)
                    total = jnp.dot(mine, dv[:, cols], preferred_element_type=f32) * w_own
                    total += jnp.dot(theirs, dv_mate[:, cols], preferred_element_type=f32) * w_peer
                    comb[h, k, :, c * cw:(c + 1) * cw] = total.astype(bf)
                if i != here:
                    back_copy(k, h).start()

    def finish(k, h):
        if k == here:
            back = comb[h, k]
        else:
            with jax.named_scope("r%d_%d" % (k, h)):
                back_copy(k, h).wait_recv()
            back = ret[h, k]
        total = send[h, k].astype(f32) + back.astype(f32)
        block = (slice(k * cap, (k + 1) * cap), slice(h * hw, (h + 1) * hw))
        fin[block] = total.astype(bf)
        store = pltpu.make_async_copy(fin.at[block], moved_hbm.at[block], outs.at[k * halves + h])
        store.start()
        stores.append(store)

    for h in range(halves):
        near_project(h)
        emit(0, h)
    from_x[0].wait_recv()
    go(d_part(0, dv_mate, 2, {"tp": across}))
    for h in range(halves):
        go(y_copy(here, h))
    emit(1, 0)
    relay(0, 0)
    emit(1, 1)
    relay(0, 1)
    for h in range(halves):
        emit(2, h)
        relay(1, h)
    from_x[1].wait_recv()
    to_mate = [go(d_part(j, dv_mate, 3 + j, {"tp": mate})) for j in range(2)]
    experts(0)
    relay(2, 0)
    for h in range(1, halves):
        relay_when(end, 2, h)
    with jax.named_scope("dmate"):
        d_part(2, dv_mate, 2, {"tp": across}).wait_recv()
        to_mate.append(go(d_part(2, dv_mate, 5, {"tp": mate})))
    experts(1)
    for copy in to_mate:
        copy.wait_recv()
    combine(0)
    late = [relay_when(jnp.logical_not(end), 2, h) for h in range(1, halves)]
    pending += late
    emit(here, 0)
    relay(here, 0)
    emit(here, 1)
    experts(2)
    relay(here, 1)
    combine(1)
    combine(2)
    experts(here)
    combine(here)
    for k in (0, 2, here, 1):
        for h in range(halves):
            finish(k, h)
    for store in stores:
        store.wait()
    with jax.named_scope("sends"):
        for k in away:
            for h in range(halves):
                z_copy(k, h).wait_send()
                back_copy(k, h).wait_send()
        @pl.when(sp > 0)
        def _():
            for copy in to_before:
                copy.wait_send()

        @pl.when(sp < sp_count - 1)
        def _():
            for copy in to_after:
                copy.wait_send()

        for copy in pending:
            copy.wait_send()


def place_kernel(spread_hbm, rows_hbm, out_hbm, spread, moved, out, ls, ss):
    parts = ls.shape[0] - 1
    cw = out.shape[1] // parts
    cols = [slice(c * cw, (c + 1) * cw) for c in range(parts)]
    first = pltpu.make_async_copy(spread_hbm, spread, ls.at[parts])
    first.start()
    loads = [
        pltpu.make_async_copy(rows_hbm.at[:, c], moved.at[:, c], ls.at[i])
        for i, c in enumerate(cols)
    ]
    stores = [
        pltpu.make_async_copy(out.at[:, c], out_hbm.at[:, c], ss.at[i])
        for i, c in enumerate(cols)
    ]
    for load in loads:
        load.start()
    first.wait()
    for c, load, store in zip(cols, loads, stores):
        load.wait()
        out[:, c] = jnp.dot(
            spread[...], moved[:, c], preferred_element_type=jnp.float32
        ).astype(out.dtype)
        store.start()
    for store in stores:
        store.wait()


def front_kernel(
    chunks, extra, entered, emit,
    sink_ref, q_ref, k_ref, v_ref, doc_ref, res_ref, w_ref,
    out_ref,
    kx, vx, dl, dr, dx, att, am_far, am_near, w_mate, acc, ysend, yrecv,
    hs, hr, ms, mr, ys, yr,
):
    sp = lax.axis_index("sp")
    tp = lax.axis_index("tp")
    sp_count = lax.axis_size("sp")
    mate = tp + 1 - 2 * (tp % 2)
    across = (tp + 2) % 4
    mate_across = (mate + 2) % 4
    after = (sp + 1) % sp_count
    before = (sp + sp_count - 1) % sp_count
    blocks = q_ref.shape[0] // WINDOW
    home_blocks = blocks // 4
    half = blocks // 2
    kv_heads = k_ref.shape[1] // HD
    ratio = q_ref.shape[1] // k_ref.shape[1]
    width = out_ref.shape[1]
    cw = width // chunks
    f32, bf = jnp.float32, jnp.bfloat16
    mesh_id = pl.DeviceIdType.MESH

    def remote(src, dst, ss, rs, where):
        return pltpu.make_async_remote_copy(
            src_ref=src, dst_ref=dst, send_sem=ss, recv_sem=rs,
            device_id=where, device_id_type=mesh_id,
        )

    barrier = pltpu.get_barrier_semaphore()
    for where in ({"sp": after}, {"sp": before}, {"tp": mate}, {"tp": across}):
        pl.semaphore_signal(barrier, inc=1, device_id=where, device_id_type=mesh_id)
    for b in range(blocks):
        kx[b + 1] = k_ref[b * WINDOW:(b + 1) * WINDOW, :]
        vx[b + 1] = v_ref[b * WINDOW:(b + 1) * WINDOW, :]
        dx[b + 1] = jnp.broadcast_to(doc_ref[b:b + 1, :].astype(f32), (8, WINDOW))
    pl.semaphore_wait(barrier, 4 + extra)

    tail = pl.ds((blocks - 1) * WINDOW, WINDOW)
    lead = pl.ds(0, WINDOW)
    halo = [
        remote(k_ref.at[tail], kx.at[0], hs.at[0], hr.at[0], {"sp": after}),
        remote(v_ref.at[tail], vx.at[0], hs.at[1], hr.at[1], {"sp": after}),
        remote(doc_ref, dl, hs.at[2], hr.at[2], {"sp": after}),
        remote(k_ref.at[lead], kx.at[blocks + 1], hs.at[3], hr.at[3], {"sp": before}),
        remote(v_ref.at[lead], vx.at[blocks + 1], hs.at[4], hr.at[4], {"sp": before}),
        remote(doc_ref, dr, hs.at[5], hr.at[5], {"sp": before}),
    ]
    for copy in halo:
        copy.start()
    w_copy = remote(w_ref, w_mate, ms.at[0], mr.at[0], {"tp": mate})
    w_copy.start()
    if entered is not None:
        entered()

    qi = lax.broadcasted_iota(jnp.int32, (WINDOW, 3 * WINDOW), 0)
    ki = lax.broadcasted_iota(jnp.int32, (WINDOW, 3 * WINDOW), 1)
    band = (ki >= qi) & (ki <= qi + 2 * WINDOW)
    eye = lax.broadcasted_iota(jnp.int32, (WINDOW, WINDOW), 0) == lax.broadcasted_iota(
        jnp.int32, (WINDOW, WINDOW), 1
    )

    def attend_block(b):
        own_docs = dx[b + 1][0:1]
        key_docs = jnp.concatenate([dx[b][0:1], own_docs, dx[b + 2][0:1]], axis=1)
        query_docs = jnp.sum(jnp.where(eye, own_docs, 0.0), axis=1, keepdims=True)
        bias = jnp.where(band & (key_docs == query_docs), 0.0, neg_fill)
        keys = kx[pl.ds(b, 3)].reshape(3 * WINDOW, kv_heads * HD)
        values = vx[pl.ds(b, 3)].reshape(3 * WINDOW, kv_heads * HD)
        home = b // home_blocks
        to_rows = pl.ds(pl.multiple_of((b % home_blocks) * WINDOW, WINDOW), WINDOW)
        from_rows = pl.ds(pl.multiple_of(b * WINDOW, WINDOW), WINDOW)
        for g in range(kv_heads):
            span = slice(g * ratio * HD, (g + 1) * ratio * HD)
            q = q_ref[from_rows, span] * jnp.asarray(HD ** (-0.5), bf)
            stacked = jnp.concatenate([q[:, r * HD:(r + 1) * HD] for r in range(ratio)], axis=0)
            scores = lax.dot_general(
                stacked, keys[:, g * HD:(g + 1) * HD], (((1,), (1,)), ((), ())),
                preferred_element_type=f32,
            )
            vg = values[:, g * HD:(g + 1) * HD]
            parts = []
            for r in range(ratio):
                sink = sink_ref[g * ratio + r]
                s = scores[r * WINDOW:(r + 1) * WINDOW] + bias
                top = jnp.maximum(jnp.max(s, axis=1, keepdims=True), sink)
                e = jnp.exp(s - top)
                den = jnp.sum(e, axis=1, keepdims=True) + jnp.exp(sink - top)
                o = jnp.dot(e.astype(bf), vg, preferred_element_type=f32)
                parts.append((o / den).astype(bf))
            att[home, to_rows, span] = jnp.concatenate(parts, axis=1)

    def far_step(i, carry):
        @pl.when(i == half - 1)
        def _():
            for copy in halo:
                copy.wait_recv()
            left = dl[blocks - 1:blocks, :].astype(f32)
            right = dr[0:1, :].astype(f32)
            left = jnp.where(sp == 0, -1.0, left)
            right = jnp.where(sp == sp_count - 1, -1.0, right)
            dx[0] = jnp.broadcast_to(left, (8, WINDOW))
            dx[blocks + 1] = jnp.broadcast_to(right, (8, WINDOW))

        attend_block(jnp.where(tp < 2, half + i, half - 1 - i))
        return carry

    lax.fori_loop(0, half, far_step, 0)
    far_copy = remote(att.at[mate_across], am_far, ms.at[1], mr.at[1], {"tp": mate})
    far_copy.start()
    w_copy.wait_recv()
    far_copy.wait_recv()
    sent = []
    for c in range(chunks):
        cols = slice(c * cw, (c + 1) * cw)
        part = jnp.dot(att[across], w_ref[:, cols], preferred_element_type=f32)
        part += jnp.dot(am_far[...], w_mate[:, cols], preferred_element_type=f32)
        ysend[c] = part.astype(bf)
        copy = remote(ysend.at[c], yrecv.at[c], ys.at[c], yr.at[c], {"tp": across})
        copy.start()
        sent.append(copy)

    def near_step(i, carry):
        attend_block(jnp.where(tp < 2, half - 1 - i, half + i))
        return carry

    lax.fori_loop(0, half, near_step, 0)
    near_copy = remote(att.at[mate], am_near, ms.at[2], mr.at[2], {"tp": mate})
    near_copy.start()
    near_copy.wait_recv()
    for c in range(chunks):
        cols = slice(c * cw, (c + 1) * cw)
        part = jnp.dot(att[tp], w_ref[:, cols], preferred_element_type=f32)
        part += jnp.dot(am_near[...], w_mate[:, cols], preferred_element_type=f32)
        acc[:, cols] = part + res_ref[:, cols].astype(f32)
    for c in range(chunks):
        cols = slice(c * cw, (c + 1) * cw)
        sent[c].wait_recv()
        out_ref[:, cols] = (acc[:, cols] + yrecv[c].astype(f32)).astype(bf)
        if emit is not None:
            emit(c)
    for copy in halo + [w_copy, far_copy, near_copy] + sent:
        copy.wait_send()


def front_scratch(queries, key_rows, residual, out_weight):
    rows, width = residual.shape
    local, heads_width = queries.shape
    kv_width = key_rows.shape[1]
    blocks = local // WINDOW
    bf, f32 = jnp.bfloat16, jnp.float32
    dma = pltpu.SemaphoreType.DMA
    return [
            pltpu.VMEM((blocks + 2, WINDOW, kv_width), bf),
            pltpu.VMEM((blocks + 2, WINDOW, kv_width), bf),
            pltpu.VMEM((blocks, WINDOW), jnp.int32),
            pltpu.VMEM((blocks, WINDOW), jnp.int32),
            pltpu.VMEM((blocks + 2, 8, WINDOW), f32),
            pltpu.VMEM((4, rows, heads_width), bf),
            pltpu.VMEM((rows, heads_width), bf),
            pltpu.VMEM((rows, heads_width), bf),
            pltpu.VMEM(out_weight.shape, bf),
            pltpu.VMEM((rows, width), f32),
            pltpu.VMEM((CHUNKS, rows, width // CHUNKS), bf),
            pltpu.VMEM((CHUNKS, rows, width // CHUNKS), bf),
            dma((6,)), dma((6,)), dma((3,)), dma((3,)), dma((CHUNKS,)), dma((CHUNKS,)),
    ]


def front(queries, key_rows, value_rows, doc_ids, sink_logit, residual, out_weight):
    rows, width = residual.shape
    local, heads_width = queries.shape
    kv_width = key_rows.shape[1]
    blocks = local // WINDOW
    bf, f32 = jnp.bfloat16, jnp.float32
    dma = pltpu.SemaphoreType.DMA
    vm = pl.BlockSpec(memory_space=pltpu.VMEM)
    docs = doc_ids.reshape(blocks, WINDOW)
    return pl.pallas_call(
        functools.partial(front_kernel, CHUNKS, 0, None, None),
        out_shape=jax.ShapeDtypeStruct((rows, width), bf),
        in_specs=[pl.BlockSpec(memory_space=pltpu.SMEM)] + [vm] * 6,
        out_specs=vm,
        scratch_shapes=front_scratch(queries, key_rows, residual, out_weight),
        compiler_params=pltpu.CompilerParams(
            collective_id=4, has_side_effects=True, vmem_limit_bytes=48 * 1024 * 1024
        ),
        name="front",
    )(sink_logit, queries, key_rows, value_rows, docs, residual, out_weight)


def pair_routed(routes, gate_weight):
    count = lax.axis_size("sp")
    experts = count * gate_weight.shape[0]
    return (
        gate_weight.shape[0] == 1
        and routes.shape[1] == 2
        and experts == 2 * GROUPS
    )


def mixture(
    queries, key_rows, value_rows, doc_ids, sink_logit, residual, out_weight,
    norm_gain, routes, route_weights, gate_weight, up_weight, down_weight,
):
    rows, width = residual.shape
    blocks = queries.shape[0] // WINDOW
    heads = queries.shape[1]
    kv_width = key_rows.shape[1]
    docs = doc_ids.reshape(blocks, WINDOW)
    ff = gate_weight.shape[2]
    groups = lax.axis_size("sp") // 2
    cap, hw = rows // groups, width // HALVES
    bf, f32, i32 = jnp.bfloat16, jnp.float32, jnp.int32
    pieces = pltpu.VMEM((HALVES, groups, cap, hw), bf)
    hidden = pltpu.VMEM((groups, cap, ff), bf)
    dma = pltpu.SemaphoreType.DMA
    hbm = pl.BlockSpec(memory_space=pl.ANY)
    edge = pltpu.VMEM((blocks + 2, WINDOW, kv_width), bf)
    per_piece = dma((HALVES, groups))
    moved, spread = pl.pallas_call(
        functools.partial(moe_kernel, groups, HALVES),
        out_shape=(
            jax.ShapeDtypeStruct((rows, width), bf), jax.ShapeDtypeStruct((rows, rows), bf)
        ),
        in_specs=[hbm] * 13,
        out_specs=(hbm, hbm),
        scratch_shapes=[
            pltpu.VMEM((rows, width), bf), pltpu.VMEM((rows, rows), bf),
            pltpu.SMEM(sink_logit.shape, f32), pltpu.VMEM(docs.shape, i32),
            pltpu.VMEM(routes.shape[::-1], i32), pltpu.VMEM(routes.shape[::-1], f32),
            pltpu.VMEM((1, width), f32),
            pltpu.VMEM(queries.shape, bf), pltpu.VMEM((rows, width), bf),
            pltpu.VMEM(out_weight.shape, bf), pltpu.VMEM(out_weight.shape, bf),
            edge, edge,
            pltpu.VMEM((blocks, WINDOW), i32), pltpu.VMEM((blocks, WINDOW), i32),
            pltpu.VMEM((blocks + 2, 8, WINDOW), f32),
            pltpu.VMEM((4, rows, heads), bf),
            pltpu.VMEM((rows, heads), bf), pltpu.VMEM((rows, heads), bf),
            pltpu.VMEM(routes.shape[::-1], i32),
            pltpu.VMEM((rows, 2 * heads), bf),
            pltpu.VMEM((groups, cap, width), f32),
            pieces, pieces, pieces, pieces, pieces, pieces, pieces,
            hidden, hidden, hidden,
            pltpu.VMEM((8, rows), f32), pltpu.VMEM((groups, 8, rows), f32),
            pltpu.VMEM((width, ff), bf), pltpu.VMEM((width, ff), bf),
            pltpu.VMEM((ff, width), bf), pltpu.VMEM((ff, width), bf),
            dma((13,)), dma((6,)), dma((6,)), dma((4,)), dma((4,)),
            per_piece, per_piece, per_piece, per_piece, per_piece, per_piece,
            dma((groups,)), dma((groups,)), per_piece, per_piece,
            dma((groups,)), dma((groups,)), dma((6,)), dma((6,)),
            dma((groups * HALVES + 1,)), pltpu.SemaphoreType.REGULAR,
        ],
        compiler_params=pltpu.CompilerParams(
            collective_id=3, has_side_effects=True, vmem_limit_bytes=56 * 1024 * 1024
        ),
        name="mixture",
    )(
        sink_logit, docs, routes.T, route_weights.T, norm_gain[None, :],
        queries, key_rows.reshape(blocks, WINDOW, kv_width),
        value_rows.reshape(blocks, WINDOW, kv_width), residual, out_weight,
        gate_weight, up_weight, down_weight,
    )
    return pl.pallas_call(
        place_kernel,
        out_shape=jax.ShapeDtypeStruct((rows, width), bf),
        in_specs=[hbm, hbm],
        out_specs=hbm,
        scratch_shapes=[
            pltpu.VMEM((rows, rows), bf), pltpu.VMEM((rows, width), bf),
            pltpu.VMEM((rows, width), bf), dma((5,)), dma((4,)),
        ],
        name="place",
    )(spread, moved)


def fits_front(queries):
    return lax.axis_size("tp") == 4 and queries.shape[0] % (8 * WINDOW) == 0


def stream_of(
    queries, key_rows, value_rows, doc_ids, sink_logit, residual, out_weight
):
    local_rows = queries.shape[0]
    if fits_front(queries):
        return front(queries, key_rows, value_rows, doc_ids, sink_logit, residual, out_weight)
    anchor = lax.axis_index("sp") * local_rows
    extent = local_rows * lax.axis_size("sp")
    doc_float = doc_ids.astype(jnp.bfloat16)
    block_rows = min(512, local_rows)
    padded_keys, padded_values, padded_docs = fetch_margins(key_rows, value_rows, doc_float)
    block_parts = []
    for row_start in range(0, local_rows, block_rows):
        key_end = row_start + block_rows + 2 * WINDOW
        block_parts.append(
            attend(
                queries[row_start : row_start + block_rows],
                padded_keys[row_start:key_end],
                padded_values[row_start:key_end],
                doc_float[row_start : row_start + block_rows],
                padded_docs[row_start:key_end],
                anchor + row_start,
                anchor + row_start - WINDOW,
                sink_logit,
                extent,
            )
        )
    attended = jnp.concatenate(block_parts, axis=0)
    regrouped = lax.all_to_all(attended, "tp", split_axis=0, concat_axis=1, tiled=True)
    shard_rows = out_weight.shape[0]
    initial = jnp.zeros((regrouped.shape[0], out_weight.shape[1]), jnp.float32)
    running = initial
    weight_piece = lax.all_gather(out_weight, "tp", axis=0, tiled=True)
    for shard_index in range(weight_piece.shape[0] // shard_rows):
        columns = lax.dynamic_slice_in_dim(regrouped, shard_index * shard_rows, shard_rows, 1)
        partial_value = jnp.dot(
            columns,
            weight_piece[shard_index * shard_rows : (shard_index + 1) * shard_rows],
            preferred_element_type=jnp.float32,
        )
        running = running + partial_value.astype(jnp.bfloat16).astype(jnp.float32)
    stream = (residual.astype(jnp.float32) + running).astype(jnp.bfloat16)
    return stream


def per_device(
    queries,
    key_rows,
    value_rows,
    doc_ids,
    sink_logit,
    residual,
    out_weight,
    norm_gain,
    gate_weight,
    up_weight,
    down_weight,
    routes,
    route_weights,
):
    front_args = (
        queries, key_rows, value_rows, doc_ids, sink_logit, residual, out_weight
    )
    if pair_routed(routes, gate_weight) and fits_front(queries):
        return mixture(
            *front_args, norm_gain, routes, route_weights, gate_weight, up_weight, down_weight
        )
    stream = stream_of(*front_args)
    stream_f = stream.astype(jnp.float32)
    scale = lax.rsqrt(jnp.mean(stream_f * stream_f, axis=1, keepdims=True) + eps_norm)
    normed = (stream_f * scale * norm_gain[None, :]).astype(jnp.bfloat16)
    home_rows = normed.shape[0]
    width = normed.shape[1]
    route_count = routes.shape[1]
    expert_count = lax.axis_size("sp") * gate_weight.shape[0]
    capacity = route_count * home_rows // expert_count
    flat_routes = routes.reshape(-1)
    one_hot = (flat_routes[:, None] == jnp.arange(expert_count, dtype=jnp.int32)[None, :]).astype(
        jnp.int32
    )
    earlier = jnp.cumsum(one_hot, axis=0) - one_hot
    slot_rank = jnp.sum(earlier * one_hot, axis=1)
    slot_index = flat_routes * capacity + slot_rank
    source_row = (
        jnp.zeros((expert_count * capacity,), jnp.int32)
        .at[slot_index]
        .set(jnp.arange(home_rows * route_count, dtype=jnp.int32) // route_count)
    )
    outgoing = normed[source_row].reshape(expert_count, capacity, width)
    incoming = lax.all_to_all(outgoing, "sp", split_axis=0, concat_axis=0, tiled=True)
    flat_rows = incoming.reshape(-1, width)
    gate_act = jnp.dot(flat_rows, gate_weight[0], preferred_element_type=jnp.float32)
    up_act = jnp.dot(flat_rows, up_weight[0], preferred_element_type=jnp.float32)
    hidden = (jax.nn.silu(gate_act) * up_act).astype(jnp.bfloat16)
    produced = jnp.dot(hidden, down_weight[0], preferred_element_type=jnp.float32).astype(
        jnp.bfloat16
    )
    returned = lax.all_to_all(
        produced.reshape(incoming.shape), "sp", split_axis=0, concat_axis=0, tiled=True
    )
    route_out = returned.reshape(-1, width)[slot_index].reshape(home_rows, route_count, width)
    weighted = jnp.sum(route_weights[:, :, None] * route_out.astype(jnp.float32), axis=1)
    return (stream_f + weighted).astype(jnp.bfloat16)


def solution(mesh):
    return jax.shard_map(
        per_device,
        mesh=mesh,
        in_specs=(
            P("sp", "tp"),
            P("sp", "tp"),
            P("sp", "tp"),
            P("sp"),
            P("tp"),
            P(("sp", "tp"), None),
            P("tp", None),
            P(),
            P("sp", None, None),
            P("sp", None, None),
            P("sp", None, None),
            P(("sp", "tp"), None),
            P(("sp", "tp"), None),
        ),
        out_specs=P(("sp", "tp"), None),
        check_vma=False,
    )
```

```python
import functools

import jax
import jax.numpy as jnp
from jax import lax
from jax.experimental import pallas as pl
from jax.experimental.pallas import tpu as pltpu
from jax.sharding import PartitionSpec as P

HD = 64
WINDOW = 128
GROUPS = 4
CHUNKS = 4
HALVES = 2


neg_fill = -1e30
eps_norm = 1e-06


def extended(block, sides, width):
    for axis, dim in sides:
        count = lax.axis_size(axis)
        forward = [(i, i + 1) for i in range(count - 1)]
        backward = [(target, source) for source, target in forward]
        low = lax.ppermute(
            lax.slice_in_dim(block, block.shape[dim] - width, None, axis=dim), axis, forward
        )
        high = lax.ppermute(lax.slice_in_dim(block, 0, width, axis=dim), axis, backward)
        block = jnp.concatenate([low, block, high], axis=dim)
    return block


def attend(
    query_part,
    key_part,
    value_part,
    query_docs,
    key_docs,
    query_start,
    key_start,
    sink_logit,
    extent,
):
    query_count = query_part.shape[0]
    key_count = key_part.shape[0]
    groups = key_part.shape[1] // HD
    head_ratio = sink_logit.shape[0] // groups
    query_heads = query_part.reshape(query_count, groups, head_ratio, HD)
    key_heads = key_part.reshape(key_count, groups, HD)
    value_heads = value_part.reshape(key_count, groups, HD)
    scores = jnp.einsum(
        "qgrd,kgd->grqk", query_heads, key_heads, preferred_element_type=jnp.float32
    ) * HD ** (-0.5)
    query_pos = query_start + jnp.arange(query_count, dtype=jnp.int32)
    key_pos = key_start + jnp.arange(key_count, dtype=jnp.int32)
    inside = (key_pos >= 0) & (key_pos < extent)
    allowed = (
        (jnp.abs(query_pos[:, None] - key_pos[None, :]) <= WINDOW)
        & (query_docs[:, None] == key_docs[None, :])
        & inside[None, :]
    )
    masked = jnp.where(allowed[None, None], scores, neg_fill)
    sink_col = sink_logit.reshape(groups, head_ratio)[:, :, None, None]
    row_top = jnp.maximum(jnp.max(masked, axis=3, keepdims=True), sink_col)
    exponent = jnp.where(allowed[None, None], jnp.exp(masked - row_top), 0.0)
    denominator = jnp.sum(exponent, axis=3, keepdims=True) + jnp.exp(sink_col - row_top)
    attn_weight = (exponent / denominator).astype(jnp.bfloat16)
    attended = jnp.einsum(
        "grqk,kgd->qgrd", attn_weight, value_heads, preferred_element_type=jnp.float32
    )
    return attended.astype(jnp.bfloat16).reshape(query_count, -1)


def fetch_margins(key_rows, value_rows, doc_float):
    return (
        extended(key_rows, (("sp", 0),), WINDOW),
        extended(value_rows, (("sp", 0),), WINDOW),
        extended(doc_float, (("sp", 0),), WINDOW),
    )


def plane_order(gz):
    return [(gz + 2) % 4, 3 - gz, gz + 1 - 2 * (gz % 2), gz]


def slots_of(routes, order, cap):
    rows = routes.shape[1]
    f32, bf = jnp.float32, jnp.bfloat16
    group_of = routes[0:1, :] // 2
    sub = lax.broadcasted_iota(jnp.int32, (8, rows), 0)
    wanted = jnp.full((8, rows), -1, jnp.int32)
    for k, plane in enumerate(order):
        wanted = jnp.where(sub == k, plane, wanted)
    one_hot = jnp.where(group_of == wanted, 1.0, 0.0)
    ri = lax.broadcasted_iota(jnp.int32, (rows, rows), 0)
    ci = lax.broadcasted_iota(jnp.int32, (rows, rows), 1)
    above = jnp.where(ri < ci, 1.0, 0.0).astype(bf)
    ranks = jnp.dot(one_hot.astype(bf), above, preferred_element_type=f32)
    base = sub.astype(f32) * cap
    return jnp.sum((ranks + base) * one_hot, axis=0, keepdims=True)


def moe_kernel(
    groups, halves,
    sink_hbm, doc_hbm, routes_hbm, rw_hbm, gain_hbm,
    q_hbm, k_hbm, v_hbm, res_hbm, w_hbm, gate_hbm, up_hbm, down_hbm,
    moved_hbm, spread_hbm,
    fin, spread_ref, sink_ref, doc_ref, routes_ref, rw_ref, gain_ref,
    qv, resv, wv, w_mate, kx, vx, dl, dr, dx, att, am_far, am_near, routes_far,
    mixed_att, acc, ysend, yrecv, send, own, peer, comb, ret, hid_own, hid_send, hid_recv,
    wsend, wrecv, gv, uv, dv, dv_mate,
    ls, hs, hr, ms, mr, ys, yr, zs, zr, xs, xr, gs, gr, bs, br, ws, wr, ds, dr_sem, outs, known,
):
    sp = lax.axis_index("sp")
    tp = lax.axis_index("tp")
    sp_count = lax.axis_size("sp")
    gz, side = sp // 2, sp % 2
    x_mate = {"sp": gz * 2 + 1 - side}
    mate = tp + 1 - 2 * (tp % 2)
    core = tp % 2
    across = (tp + 2) % 4
    mate_across = (mate + 2) % 4
    after = (sp + 1) % sp_count
    before = (sp + sp_count - 1) % sp_count
    order = plane_order(gz)
    here = groups - 1
    away = [k for k in range(groups) if k != here]
    rows, width = fin.shape
    cap = rows // groups
    hw = width // halves
    cw = width // 4
    blocks = k_hbm.shape[0]
    home_blocks = blocks // 4
    half = blocks // 2
    kv_heads = k_hbm.shape[2] // HD
    ratio = q_hbm.shape[1] // k_hbm.shape[2]
    heads = q_hbm.shape[1]
    f32, bf = jnp.float32, jnp.bfloat16
    mesh_id = pl.DeviceIdType.MESH

    def remote(src, dst, s_sem, r_sem, where):
        return pltpu.make_async_remote_copy(
            src_ref=src, dst_ref=dst, send_sem=s_sem, recv_sem=r_sem,
            device_id=where, device_id_type=mesh_id,
        )

    end = (gz == 0) | (gz == groups - 1)

    def pick_one(at_end, at_middle):
        return at_end if at_end == at_middle else jnp.where(end, at_end, at_middle)

    emit_order = [pick_one(a, b) for a, b in ((1, 2), (0, 0), (2, 1), (here, here))]
    serve_order = [pick_one(a, b) for a, b in ((1, 0), (2, 2), (0, 1), (here, here))]

    def to_plane(k):
        plane = order[3]
        for i in range(groups - 1):
            plane = jnp.where(k == i, order[i], plane)
        return {"sp": plane * 2 + side}

    barrier = pltpu.get_barrier_semaphore()

    def signal(sem, where):
        pl.semaphore_signal(sem, inc=1, device_id=where, device_id_type=mesh_id)

    for where in ({"tp": mate}, {"tp": across}, x_mate):
        signal(barrier, where)
    pl.when(sp > 0)(lambda: signal(barrier, {"sp": before}))
    pl.when(sp < sp_count - 1)(lambda: signal(barrier, {"sp": after}))
    pl.when(gz > 0)(lambda: signal(barrier, {"sp": sp - 2}))
    pl.when(gz < groups - 1)(lambda: signal(barrier, {"sp": sp + 2}))
    greeted = 7 - jnp.where((sp == 0) | (sp == sp_count - 1), 1, 0) - jnp.where(end, 1, 0)
    pairs = (
        (k_hbm, kx.at[pl.ds(1, blocks)]), (v_hbm, vx.at[pl.ds(1, blocks)]),
        (doc_hbm, doc_ref), (routes_hbm, routes_ref), (rw_hbm, rw_ref), (sink_hbm, sink_ref),
        (q_hbm, qv), (w_hbm, wv), (gain_hbm, gain_ref), (res_hbm, resv),
        (gate_hbm.at[0], gv), (up_hbm.at[0], uv), (down_hbm.at[0], dv),
    )
    loads = [pltpu.make_async_copy(src, dst, ls.at[i]) for i, (src, dst) in enumerate(pairs)]
    for load in loads[:7]:
        load.start()

    @pl.when(sp == 0)
    def _():
        kx[0] = jnp.zeros(kx.shape[1:], bf)
        vx[0] = jnp.zeros(vx.shape[1:], bf)

    @pl.when(sp == sp_count - 1)
    def _():
        kx[blocks + 1] = jnp.zeros(kx.shape[1:], bf)
        vx[blocks + 1] = jnp.zeros(vx.shape[1:], bf)

    for load in loads[:5]:
        load.wait()
    with jax.named_scope("barrier"):
        pl.semaphore_wait(barrier, greeted)

    @pl.when(jnp.logical_not(end))
    def _():
        signal(known, {"sp": sp - 2})
        signal(known, {"sp": sp + 2})

    pending = []

    def go(copy):
        copy.start()
        pending.append(copy)
        return copy

    def halo_of(i, src, dst, where):
        return remote(src, dst, hs.at[i], hr.at[i], {"sp": where})

    to_after = [
        halo_of(0, kx.at[blocks], kx.at[0], after),
        halo_of(1, vx.at[blocks], vx.at[0], after),
        halo_of(2, doc_ref, dl, after),
    ]
    to_before = [
        halo_of(3, kx.at[1], kx.at[blocks + 1], before),
        halo_of(4, vx.at[1], vx.at[blocks + 1], before),
        halo_of(5, doc_ref, dr, before),
    ]

    def send_before():
        @pl.when(sp > 0)
        def _():
            for copy in to_before:
                copy.start()

    def send_after():
        @pl.when(sp < sp_count - 1)
        def _():
            for copy in to_after:
                copy.start()

    pl.when(tp < 2)(send_before)
    pl.when(tp >= 2)(send_after)
    r_copy = go(remote(routes_ref, routes_far, ms.at[3], mr.at[3], {"tp": across}))
    ff = dv.shape[0]
    quarter, eighth = ff // 4, ff // 8
    chip = tp // 2
    d_rows = [
        pl.ds(pl.multiple_of(start, eighth), count) for start, count in (
            ((2 + chip) * quarter + core * eighth, eighth), (core * quarter, quarter),
            ((3 - chip) * quarter + core * eighth, eighth),
        )
    ]

    def d_part(i, source, sem, where):
        return remote(
            source.at[d_rows[i]], dv_mate.at[d_rows[i]], ds.at[sem], dr_sem.at[sem], where
        )

    from_x = [d_part(i, down_hbm.at[0], i, x_mate) for i in range(2)]
    w_copy = remote(w_hbm, w_mate, ms.at[0], mr.at[0], {"tp": mate})
    for b in range(blocks):
        dx[b + 1] = jnp.broadcast_to(doc_ref[b:b + 1, :].astype(f32), (8, WINDOW))

    def left_halo():
        @pl.when(sp > 0)
        def _():
            for copy in to_after:
                copy.wait_recv()
        left = jnp.where(sp == 0, -1.0, dl[blocks - 1:blocks, :].astype(f32))
        dx[0] = jnp.broadcast_to(left, (8, WINDOW))

    def right_halo():
        @pl.when(sp < sp_count - 1)
        def _():
            for copy in to_before:
                copy.wait_recv()
        right = jnp.where(sp == sp_count - 1, -1.0, dr[0:1, :].astype(f32))
        dx[blocks + 1] = jnp.broadcast_to(right, (8, WINDOW))

    ri = lax.broadcasted_iota(jnp.int32, (rows, rows), 0)
    ci = lax.broadcasted_iota(jnp.int32, (rows, rows), 1)
    qi = lax.broadcasted_iota(jnp.int32, (WINDOW, 3 * WINDOW), 0)
    ki = lax.broadcasted_iota(jnp.int32, (WINDOW, 3 * WINDOW), 1)
    band = (ki >= qi) & (ki <= qi + 2 * WINDOW)
    eye = lax.broadcasted_iota(jnp.int32, (WINDOW, WINDOW), 0) == lax.broadcasted_iota(
        jnp.int32, (WINDOW, WINDOW), 1
    )

    low = lax.broadcasted_iota(jnp.int32, (3 * WINDOW, kv_heads * HD), 1) < HD
    low_q = lax.broadcasted_iota(jnp.int32, (WINDOW, kv_heads * HD), 1) < HD
    zero, one = jnp.zeros((), bf), jnp.ones((), bf)

    def attend_block(b):
        own_docs = dx[b + 1][0:1]
        key_docs = jnp.concatenate([dx[b][0:1], own_docs, dx[b + 2][0:1]], axis=1)
        query_docs = jnp.sum(jnp.where(eye, own_docs, 0.0), axis=1, keepdims=True)
        bias = jnp.where(band & (key_docs == query_docs), 0.0, neg_fill)
        keys = kx[pl.ds(b, 3)].reshape(3 * WINDOW, kv_heads * HD)
        values = vx[pl.ds(b, 3)].reshape(3 * WINDOW, kv_heads * HD)
        key_two = jnp.concatenate(
            [jnp.where(low, keys, zero), jnp.where(low, zero, keys)], axis=0
        )
        value_two = jnp.concatenate([
            jnp.concatenate([jnp.where(low, values, zero), jnp.where(low, one, zero)], axis=1),
            jnp.concatenate([jnp.where(low, zero, values), jnp.where(low, zero, one)], axis=1),
        ], axis=0)
        home = b // home_blocks
        to_rows = pl.ds(pl.multiple_of((b % home_blocks) * WINDOW, WINDOW), WINDOW)
        from_rows = pl.ds(pl.multiple_of(b * WINDOW, WINDOW), WINDOW)
        q = qv[from_rows, :] * jnp.asarray(HD ** (-0.5), bf)
        parts = [None] * (2 * ratio)
        for r in range(ratio):
            pair = jnp.concatenate(
                [q[:, r * HD:(r + 1) * HD], q[:, (ratio + r) * HD:(ratio + r + 1) * HD]], axis=1
            )
            scores = lax.dot_general(
                pair, key_two, (((1,), (1,)), ((), ())), preferred_element_type=f32
            )
            exps, sinks = [], []
            for g in range(2):
                sink = sink_ref[g * ratio + r]
                s = scores[:, g * 3 * WINDOW:(g + 1) * 3 * WINDOW] + bias
                top = jnp.maximum(jnp.max(s, axis=1, keepdims=True), sink)
                exps.append(jnp.exp(s - top).astype(bf))
                sinks.append(jnp.exp(sink - top))
            o = jnp.dot(jnp.concatenate(exps, axis=1), value_two, preferred_element_type=f32)
            den = o[:, 2 * HD:] + jnp.where(low_q, sinks[0], sinks[1])
            both = (o[:, :2 * HD] / den).astype(bf)
            parts[r], parts[ratio + r] = both[:, :HD], both[:, HD:]
        att[home, to_rows, :] = jnp.concatenate(parts, axis=1)

    early = (tp == 1) | (tp == 2)
    far_copy = remote(att.at[mate_across], am_far, ms.at[1], mr.at[1], {"tp": mate})
    near_copy = remote(att.at[mate], am_near, ms.at[2], mr.at[2], {"tp": mate})

    low_side = tp < 2
    starts = [
        jnp.where(low_side, half, home_blocks), jnp.where(low_side, home_blocks, half),
        jnp.where(low_side, half + home_blocks, 0), jnp.where(low_side, 0, half + home_blocks),
    ]

    def attend_home(start):
        for j in range(home_blocks):
            attend_block(start + j)

    def first_pairs(i, carry):
        @pl.when(i == 0)
        def _():
            w_copy.start()

        @pl.when((i == 1) & early)
        def _():
            far_copy.start()

        @pl.when((i == 1) & low_side)
        def _():
            send_after()

        @pl.when((i == 1) & jnp.logical_not(low_side))
        def _():
            send_before()

        @pl.when((i == 1) & jnp.logical_not(end))
        def _():
            pl.semaphore_wait(known, 1)
            signal(known, {"sp": (gz - 1) * (groups - 1) * 2 + side})

        @pl.when((i == 2) & jnp.logical_not(early))
        def _():
            near_copy.start()

        @pl.when((i == 2) & low_side)
        def _():
            with jax.named_scope("halo_right"):
                right_halo()

        @pl.when((i == 2) & jnp.logical_not(low_side))
        def _():
            with jax.named_scope("halo_left"):
                left_halo()

        @pl.when(i == 2)
        def _():
            for copy in from_x:
                copy.start()

        attend_home(jnp.where(i == 0, starts[0], jnp.where(i == 1, starts[1], starts[2])))
        return carry

    def pick_of(slot_row):
        return jnp.where(ri.astype(f32) == slot_row, 1.0, 0.0).astype(bf)

    def gather_mine(pick, rows_in):
        mixed_att[:, :heads] = jnp.dot(pick, rows_in, preferred_element_type=f32).astype(bf)

    def gather_mates(pick, rows_in):
        mixed_att[:, heads:] = jnp.dot(pick, rows_in, preferred_element_type=f32).astype(bf)

    def project_mine(cols):
        return jnp.dot(mixed_att[:, :heads], wv[:, cols], preferred_element_type=f32)

    def project_mates(cols):
        return jnp.dot(mixed_att[:, heads:], w_mate[:, cols], preferred_element_type=f32)

    def project(cols):
        return project_mine(cols) + project_mates(cols)

    loads[5].wait()
    loads[6].wait()
    loads[7].start()
    with jax.named_scope("attn_far"):
        lax.fori_loop(0, 3, first_pairs, 0)
    pl.when(jnp.logical_not(early))(far_copy.start)
    pending += [w_copy, far_copy, near_copy] + from_x
    for load in loads[8:]:
        load.start()
    per = 4 // halves
    with jax.named_scope("far_mine"):
        r_copy.wait_recv()
        pick_far = pick_of(slots_of(routes_far[...], order, cap))
        gather_mine(pick_far, att[across])
        loads[7].wait()
        for c in range(per):
            cols = slice(c * cw, (c + 1) * cw)
            acc[:, :, cols] = project_mine(cols).reshape(groups, cap, cw)
    with jax.named_scope("wait_far"):
        w_copy.wait_recv()
        far_copy.wait_recv()
    with jax.named_scope("far_proj"):
        gather_mates(pick_far, am_far[...])

        def y_copy(k, h):
            return remote(
                ysend.at[h, k], yrecv.at[h, k], ys.at[h, k], yr.at[h, k], {"tp": across}
            )

        for h in range(halves):
            for c in range(per):
                cols = slice(h * hw + c * cw, h * hw + (c + 1) * cw)
                if h:
                    part = project(cols).reshape(groups, cap, cw)
                else:
                    part = project_mates(cols).reshape(groups, cap, cw) + acc[:, :, cols]
                ysend[h, :, :, c * cw:(c + 1) * cw] = part.astype(bf)
            if h < halves - 1:
                go(y_copy(emit_order[0], h))
        go(y_copy(emit_order[0], halves - 1))
        for k in emit_order[1:here]:
            for h in range(halves):
                go(y_copy(k, h))

    slot = slots_of(routes_ref[...], order, cap)
    slot_col = jnp.sum(jnp.where(ri == ci, slot, 0.0), axis=1, keepdims=True)
    spread = jnp.where(slot_col == ci.astype(f32), 1.0, 0.0)
    weight_rows = []
    for parity in (side, 1 - side):
        w_row = jnp.where(routes_ref[0:1, :] % 2 == parity, rw_ref[0:1, :], rw_ref[1:2, :])
        w_col = jnp.sum(jnp.where(ri == ci, w_row, 0.0), axis=1, keepdims=True)
        weight_rows.append(jnp.sum(spread * w_col, axis=0, keepdims=True))
    sub8 = lax.broadcasted_iota(jnp.int32, (8, rows), 0)
    wsend[...] = jnp.where(
        sub8 == 0, weight_rows[0], jnp.where(sub8 == 1, weight_rows[1], 0.0)
    )

    wrecv[here] = wsend[...]

    @pl.when(end)
    def _():
        pl.semaphore_wait(known, 2)

    for k in away:
        go(remote(wsend, wrecv.at[k], ws.at[k], wr.at[k], to_plane(k)))

    with jax.named_scope("attn_near"):
        pl.when(tp < 2)(left_halo)
        pl.when(tp >= 2)(right_halo)
        attend_home(starts[3])
        pl.when(early)(near_copy.start)
    for load in loads[8:]:
        load.wait()
    pick = pick_of(slot)
    spread_ref[...] = spread.astype(bf)
    stores = [pltpu.make_async_copy(spread_ref, spread_hbm, outs.at[groups * halves])]
    stores[0].start()
    with jax.named_scope("near_mine"):
        gather_mine(pick, att[tp])
        for c in range(4):
            cols = slice(c * cw, (c + 1) * cw)
            part = project_mine(cols)
            part += jnp.dot(pick, resv[:, cols], preferred_element_type=f32)
            acc[:, :, cols] = part.reshape(groups, cap, cw)
    with jax.named_scope("wait_near"):
        near_copy.wait_recv()
    gather_mates(pick, am_near[...])

    def near_project(h):
        with jax.named_scope("near_proj%d" % h):
            for c in range(per):
                cols = slice(h * hw + c * cw, h * hw + (c + 1) * cw)
                acc[:, :, cols] += project_mates(cols).reshape(groups, cap, cw)

    def z_copy(k, h):
        return remote(send.at[h, k], own.at[h, k], zs.at[h, k], zr.at[h, k], to_plane(k))

    def x_copy(k, h):
        return remote(own.at[h, k], peer.at[h, k], xs.at[h, k], xr.at[h, k], x_mate)

    def hid_copy(k):
        return remote(hid_send.at[k], hid_recv.at[k], gs.at[k], gr.at[k], x_mate)

    def back_copy(k, h):
        return remote(comb.at[h, k], ret.at[h, k], bs.at[h, k], br.at[h, k], to_plane(k))

    def emit(i, h):
        k = emit_order[i]
        with jax.named_scope("y%d_%d" % (i, h)):
            y_copy(k, h).wait_recv()
        cols = slice(h * hw, (h + 1) * hw)
        piece = (acc[k, :, cols] + yrecv[h, k].astype(f32)).astype(bf)
        send[h, k] = piece
        if i == here:
            own[h, here] = piece
        else:
            z_copy(k, h).start()

    def relay(i, h):
        k = serve_order[i]
        if i != here:
            with jax.named_scope("z%d_%d" % (i, h)):
                z_copy(k, h).wait_recv()
        go(x_copy(k, h))

    def relay_when(here_now, i, h):
        k = serve_order[i]

        @pl.when(here_now)
        def _():
            z_copy(k, h).wait_recv()
            x_copy(k, h).start()

        return x_copy(k, h)

    def hidden_of(parts):
        squares = gate_act = up_act = 0.0
        for h in range(halves):
            span = slice(h * hw, (h + 1) * hw)
            wide = jnp.concatenate([buf[h, k] for buf, k in parts], axis=0).astype(f32)
            squares = squares + jnp.sum(wide * wide, axis=1, keepdims=True)
            block = (wide * gain_ref[:, span]).astype(bf)
            gate_act = gate_act + jnp.dot(block, gv[span, :], preferred_element_type=f32)
            up_act = up_act + jnp.dot(block, uv[span, :], preferred_element_type=f32)
        scale = lax.rsqrt(squares / width + eps_norm)
        g = gate_act * scale
        return (g / (1.0 + jnp.exp(-g)) * (up_act * scale)).astype(bf)

    def experts(i):
        k = serve_order[i]
        with jax.named_scope("x%d" % i):
            for h in range(halves):
                x_copy(k, h).wait_recv()
        with jax.named_scope("experts%d" % i):
            result = hidden_of([(own, k), (peer, k)])
            hid_send[k] = result[cap:]
            go(hid_copy(k))
            hid_own[k] = result[:cap]

    sub_c = lax.broadcasted_iota(jnp.int32, (cap, rows), 0)
    lane_c = lax.broadcasted_iota(jnp.int32, (cap, rows), 1)

    def combine(i):
        k = serve_order[i]
        with jax.named_scope("hid%d" % i):
            hid_copy(k).wait_recv()
            if i != here:
                remote(wsend, wrecv.at[k], ws.at[k], wr.at[k], x_mate).wait_recv()
        with jax.named_scope("down%d" % i):
            table = wrecv[k]
            chosen = lane_c == sub_c + k * cap
            w_own = jnp.sum(jnp.where(chosen, table[0:1, :], 0.0), axis=1, keepdims=True)
            w_peer = jnp.sum(jnp.where(chosen, table[1:2, :], 0.0), axis=1, keepdims=True)
            mine, theirs = hid_own[k], hid_recv[k]
            for h in range(halves):
                for c in range(per):
                    cols = slice(h * hw + c * cw, h * hw + (c + 1) * cw)
                    total = jnp.dot(mine, dv[:, cols], preferred_element_type=f32) * w_own
                    total += jnp.dot(theirs, dv_mate[:, cols], preferred_element_type=f32) * w_peer
                    comb[h, k, :, c * cw:(c + 1) * cw] = total.astype(bf)
                if i != here:
                    back_copy(k, h).start()

    def finish(k, h):
        if k == here:
            back = comb[h, k]
        else:
            with jax.named_scope("r%d_%d" % (k, h)):
                back_copy(k, h).wait_recv()
            back = ret[h, k]
        total = send[h, k].astype(f32) + back.astype(f32)
        block = (slice(k * cap, (k + 1) * cap), slice(h * hw, (h + 1) * hw))
        fin[block] = total.astype(bf)
        store = pltpu.make_async_copy(fin.at[block], moved_hbm.at[block], outs.at[k * halves + h])
        store.start()
        stores.append(store)

    for h in range(halves):
        near_project(h)
        emit(0, h)
    from_x[0].wait_recv()
    go(d_part(0, dv_mate, 2, {"tp": across}))
    for h in range(halves):
        go(y_copy(here, h))
    emit(1, 0)
    relay(0, 0)
    emit(1, 1)
    relay(0, 1)
    for h in range(halves):
        emit(2, h)
        relay(1, h)
    from_x[1].wait_recv()
    to_mate = [go(d_part(j, dv_mate, 3 + j, {"tp": mate})) for j in range(2)]
    experts(0)
    relay(2, 0)
    for h in range(1, halves):
        relay_when(end, 2, h)
    with jax.named_scope("dmate"):
        d_part(2, dv_mate, 2, {"tp": across}).wait_recv()
        to_mate.append(go(d_part(2, dv_mate, 5, {"tp": mate})))
    experts(1)
    for copy in to_mate:
        copy.wait_recv()
    combine(0)
    late = [relay_when(jnp.logical_not(end), 2, h) for h in range(1, halves)]
    pending += late
    emit(here, 0)
    relay(here, 0)
    emit(here, 1)
    experts(2)
    relay(here, 1)
    combine(1)
    combine(2)
    experts(here)
    combine(here)
    for k in (0, 2, here, 1):
        for h in range(halves):
            finish(k, h)
    for store in stores:
        store.wait()
    with jax.named_scope("sends"):
        for k in away:
            for h in range(halves):
                z_copy(k, h).wait_send()
                back_copy(k, h).wait_send()
        @pl.when(sp > 0)
        def _():
            for copy in to_before:
                copy.wait_send()

        @pl.when(sp < sp_count - 1)
        def _():
            for copy in to_after:
                copy.wait_send()

        for copy in pending:
            copy.wait_send()


def place_kernel(spread_hbm, rows_hbm, out_hbm, spread, moved, out, ls, ss):
    parts = ls.shape[0] - 1
    cw = out.shape[1] // parts
    cols = [slice(c * cw, (c + 1) * cw) for c in range(parts)]
    first = pltpu.make_async_copy(spread_hbm, spread, ls.at[parts])
    first.start()
    loads = [
        pltpu.make_async_copy(rows_hbm.at[:, c], moved.at[:, c], ls.at[i])
        for i, c in enumerate(cols)
    ]
    stores = [
        pltpu.make_async_copy(out.at[:, c], out_hbm.at[:, c], ss.at[i])
        for i, c in enumerate(cols)
    ]
    for load in loads:
        load.start()
    first.wait()
    for c, load, store in zip(cols, loads, stores):
        load.wait()
        out[:, c] = jnp.dot(
            spread[...], moved[:, c], preferred_element_type=jnp.float32
        ).astype(out.dtype)
        store.start()
    for store in stores:
        store.wait()


def front_kernel(
    chunks, extra, entered, emit,
    sink_ref, q_ref, k_ref, v_ref, doc_ref, res_ref, w_ref,
    out_ref,
    kx, vx, dl, dr, dx, att, am_far, am_near, w_mate, acc, ysend, yrecv,
    hs, hr, ms, mr, ys, yr,
):
    sp = lax.axis_index("sp")
    tp = lax.axis_index("tp")
    sp_count = lax.axis_size("sp")
    mate = tp + 1 - 2 * (tp % 2)
    across = (tp + 2) % 4
    mate_across = (mate + 2) % 4
    after = (sp + 1) % sp_count
    before = (sp + sp_count - 1) % sp_count
    blocks = q_ref.shape[0] // WINDOW
    home_blocks = blocks // 4
    half = blocks // 2
    kv_heads = k_ref.shape[1] // HD
    ratio = q_ref.shape[1] // k_ref.shape[1]
    width = out_ref.shape[1]
    cw = width // chunks
    f32, bf = jnp.float32, jnp.bfloat16
    mesh_id = pl.DeviceIdType.MESH

    def remote(src, dst, ss, rs, where):
        return pltpu.make_async_remote_copy(
            src_ref=src, dst_ref=dst, send_sem=ss, recv_sem=rs,
            device_id=where, device_id_type=mesh_id,
        )

    barrier = pltpu.get_barrier_semaphore()
    for where in ({"sp": after}, {"sp": before}, {"tp": mate}, {"tp": across}):
        pl.semaphore_signal(barrier, inc=1, device_id=where, device_id_type=mesh_id)
    for b in range(blocks):
        kx[b + 1] = k_ref[b * WINDOW:(b + 1) * WINDOW, :]
        vx[b + 1] = v_ref[b * WINDOW:(b + 1) * WINDOW, :]
        dx[b + 1] = jnp.broadcast_to(doc_ref[b:b + 1, :].astype(f32), (8, WINDOW))
    pl.semaphore_wait(barrier, 4 + extra)

    tail = pl.ds((blocks - 1) * WINDOW, WINDOW)
    lead = pl.ds(0, WINDOW)
    halo = [
        remote(k_ref.at[tail], kx.at[0], hs.at[0], hr.at[0], {"sp": after}),
        remote(v_ref.at[tail], vx.at[0], hs.at[1], hr.at[1], {"sp": after}),
        remote(doc_ref, dl, hs.at[2], hr.at[2], {"sp": after}),
        remote(k_ref.at[lead], kx.at[blocks + 1], hs.at[3], hr.at[3], {"sp": before}),
        remote(v_ref.at[lead], vx.at[blocks + 1], hs.at[4], hr.at[4], {"sp": before}),
        remote(doc_ref, dr, hs.at[5], hr.at[5], {"sp": before}),
    ]
    for copy in halo:
        copy.start()
    w_copy = remote(w_ref, w_mate, ms.at[0], mr.at[0], {"tp": mate})
    w_copy.start()
    if entered is not None:
        entered()

    qi = lax.broadcasted_iota(jnp.int32, (WINDOW, 3 * WINDOW), 0)
    ki = lax.broadcasted_iota(jnp.int32, (WINDOW, 3 * WINDOW), 1)
    band = (ki >= qi) & (ki <= qi + 2 * WINDOW)
    eye = lax.broadcasted_iota(jnp.int32, (WINDOW, WINDOW), 0) == lax.broadcasted_iota(
        jnp.int32, (WINDOW, WINDOW), 1
    )

    def attend_block(b):
        own_docs = dx[b + 1][0:1]
        key_docs = jnp.concatenate([dx[b][0:1], own_docs, dx[b + 2][0:1]], axis=1)
        query_docs = jnp.sum(jnp.where(eye, own_docs, 0.0), axis=1, keepdims=True)
        bias = jnp.where(band & (key_docs == query_docs), 0.0, neg_fill)
        keys = kx[pl.ds(b, 3)].reshape(3 * WINDOW, kv_heads * HD)
        values = vx[pl.ds(b, 3)].reshape(3 * WINDOW, kv_heads * HD)
        home = b // home_blocks
        to_rows = pl.ds(pl.multiple_of((b % home_blocks) * WINDOW, WINDOW), WINDOW)
        from_rows = pl.ds(pl.multiple_of(b * WINDOW, WINDOW), WINDOW)
        for g in range(kv_heads):
            span = slice(g * ratio * HD, (g + 1) * ratio * HD)
            q = q_ref[from_rows, span] * jnp.asarray(HD ** (-0.5), bf)
            stacked = jnp.concatenate([q[:, r * HD:(r + 1) * HD] for r in range(ratio)], axis=0)
            scores = lax.dot_general(
                stacked, keys[:, g * HD:(g + 1) * HD], (((1,), (1,)), ((), ())),
                preferred_element_type=f32,
            )
            vg = values[:, g * HD:(g + 1) * HD]
            parts = []
            for r in range(ratio):
                sink = sink_ref[g * ratio + r]
                s = scores[r * WINDOW:(r + 1) * WINDOW] + bias
                top = jnp.maximum(jnp.max(s, axis=1, keepdims=True), sink)
                e = jnp.exp(s - top)
                den = jnp.sum(e, axis=1, keepdims=True) + jnp.exp(sink - top)
                o = jnp.dot(e.astype(bf), vg, preferred_element_type=f32)
                parts.append((o / den).astype(bf))
            att[home, to_rows, span] = jnp.concatenate(parts, axis=1)

    def far_step(i, carry):
        @pl.when(i == half - 1)
        def _():
            for copy in halo:
                copy.wait_recv()
            left = dl[blocks - 1:blocks, :].astype(f32)
            right = dr[0:1, :].astype(f32)
            left = jnp.where(sp == 0, -1.0, left)
            right = jnp.where(sp == sp_count - 1, -1.0, right)
            dx[0] = jnp.broadcast_to(left, (8, WINDOW))
            dx[blocks + 1] = jnp.broadcast_to(right, (8, WINDOW))

        attend_block(jnp.where(tp < 2, half + i, half - 1 - i))
        return carry

    lax.fori_loop(0, half, far_step, 0)
    far_copy = remote(att.at[mate_across], am_far, ms.at[1], mr.at[1], {"tp": mate})
    far_copy.start()
    w_copy.wait_recv()
    far_copy.wait_recv()
    sent = []
    for c in range(chunks):
        cols = slice(c * cw, (c + 1) * cw)
        part = jnp.dot(att[across], w_ref[:, cols], preferred_element_type=f32)
        part += jnp.dot(am_far[...], w_mate[:, cols], preferred_element_type=f32)
        ysend[c] = part.astype(bf)
        copy = remote(ysend.at[c], yrecv.at[c], ys.at[c], yr.at[c], {"tp": across})
        copy.start()
        sent.append(copy)

    def near_step(i, carry):
        attend_block(jnp.where(tp < 2, half - 1 - i, half + i))
        return carry

    lax.fori_loop(0, half, near_step, 0)
    near_copy = remote(att.at[mate], am_near, ms.at[2], mr.at[2], {"tp": mate})
    near_copy.start()
    near_copy.wait_recv()
    for c in range(chunks):
        cols = slice(c * cw, (c + 1) * cw)
        part = jnp.dot(att[tp], w_ref[:, cols], preferred_element_type=f32)
        part += jnp.dot(am_near[...], w_mate[:, cols], preferred_element_type=f32)
        acc[:, cols] = part + res_ref[:, cols].astype(f32)
    for c in range(chunks):
        cols = slice(c * cw, (c + 1) * cw)
        sent[c].wait_recv()
        out_ref[:, cols] = (acc[:, cols] + yrecv[c].astype(f32)).astype(bf)
        if emit is not None:
            emit(c)
    for copy in halo + [w_copy, far_copy, near_copy] + sent:
        copy.wait_send()


def front_scratch(queries, key_rows, residual, out_weight):
    rows, width = residual.shape
    local, heads_width = queries.shape
    kv_width = key_rows.shape[1]
    blocks = local // WINDOW
    bf, f32 = jnp.bfloat16, jnp.float32
    dma = pltpu.SemaphoreType.DMA
    return [
            pltpu.VMEM((blocks + 2, WINDOW, kv_width), bf),
            pltpu.VMEM((blocks + 2, WINDOW, kv_width), bf),
            pltpu.VMEM((blocks, WINDOW), jnp.int32),
            pltpu.VMEM((blocks, WINDOW), jnp.int32),
            pltpu.VMEM((blocks + 2, 8, WINDOW), f32),
            pltpu.VMEM((4, rows, heads_width), bf),
            pltpu.VMEM((rows, heads_width), bf),
            pltpu.VMEM((rows, heads_width), bf),
            pltpu.VMEM(out_weight.shape, bf),
            pltpu.VMEM((rows, width), f32),
            pltpu.VMEM((CHUNKS, rows, width // CHUNKS), bf),
            pltpu.VMEM((CHUNKS, rows, width // CHUNKS), bf),
            dma((6,)), dma((6,)), dma((3,)), dma((3,)), dma((CHUNKS,)), dma((CHUNKS,)),
    ]


def front(queries, key_rows, value_rows, doc_ids, sink_logit, residual, out_weight):
    rows, width = residual.shape
    local, heads_width = queries.shape
    kv_width = key_rows.shape[1]
    blocks = local // WINDOW
    bf, f32 = jnp.bfloat16, jnp.float32
    dma = pltpu.SemaphoreType.DMA
    vm = pl.BlockSpec(memory_space=pltpu.VMEM)
    docs = doc_ids.reshape(blocks, WINDOW)
    return pl.pallas_call(
        functools.partial(front_kernel, CHUNKS, 0, None, None),
        out_shape=jax.ShapeDtypeStruct((rows, width), bf),
        in_specs=[pl.BlockSpec(memory_space=pltpu.SMEM)] + [vm] * 6,
        out_specs=vm,
        scratch_shapes=front_scratch(queries, key_rows, residual, out_weight),
        compiler_params=pltpu.CompilerParams(
            collective_id=4, has_side_effects=True, vmem_limit_bytes=48 * 1024 * 1024
        ),
        name="front",
    )(sink_logit, queries, key_rows, value_rows, docs, residual, out_weight)


def pair_routed(routes, gate_weight):
    count = lax.axis_size("sp")
    experts = count * gate_weight.shape[0]
    return (
        gate_weight.shape[0] == 1
        and routes.shape[1] == 2
        and experts == 2 * GROUPS
    )


def mixture(
    queries, key_rows, value_rows, doc_ids, sink_logit, residual, out_weight,
    norm_gain, routes, route_weights, gate_weight, up_weight, down_weight,
):
    rows, width = residual.shape
    blocks = queries.shape[0] // WINDOW
    heads = queries.shape[1]
    kv_width = key_rows.shape[1]
    docs = doc_ids.reshape(blocks, WINDOW)
    ff = gate_weight.shape[2]
    groups = lax.axis_size("sp") // 2
    cap, hw = rows // groups, width // HALVES
    bf, f32, i32 = jnp.bfloat16, jnp.float32, jnp.int32
    pieces = pltpu.VMEM((HALVES, groups, cap, hw), bf)
    hidden = pltpu.VMEM((groups, cap, ff), bf)
    dma = pltpu.SemaphoreType.DMA
    hbm = pl.BlockSpec(memory_space=pl.ANY)
    edge = pltpu.VMEM((blocks + 2, WINDOW, kv_width), bf)
    per_piece = dma((HALVES, groups))
    moved, spread = pl.pallas_call(
        functools.partial(moe_kernel, groups, HALVES),
        out_shape=(
            jax.ShapeDtypeStruct((rows, width), bf), jax.ShapeDtypeStruct((rows, rows), bf)
        ),
        in_specs=[hbm] * 13,
        out_specs=(hbm, hbm),
        scratch_shapes=[
            pltpu.VMEM((rows, width), bf), pltpu.VMEM((rows, rows), bf),
            pltpu.SMEM(sink_logit.shape, f32), pltpu.VMEM(docs.shape, i32),
            pltpu.VMEM(routes.shape[::-1], i32), pltpu.VMEM(routes.shape[::-1], f32),
            pltpu.VMEM((1, width), f32),
            pltpu.VMEM(queries.shape, bf), pltpu.VMEM((rows, width), bf),
            pltpu.VMEM(out_weight.shape, bf), pltpu.VMEM(out_weight.shape, bf),
            edge, edge,
            pltpu.VMEM((blocks, WINDOW), i32), pltpu.VMEM((blocks, WINDOW), i32),
            pltpu.VMEM((blocks + 2, 8, WINDOW), f32),
            pltpu.VMEM((4, rows, heads), bf),
            pltpu.VMEM((rows, heads), bf), pltpu.VMEM((rows, heads), bf),
            pltpu.VMEM(routes.shape[::-1], i32),
            pltpu.VMEM((rows, 2 * heads), bf),
            pltpu.VMEM((groups, cap, width), f32),
            pieces, pieces, pieces, pieces, pieces, pieces, pieces,
            hidden, hidden, hidden,
            pltpu.VMEM((8, rows), f32), pltpu.VMEM((groups, 8, rows), f32),
            pltpu.VMEM((width, ff), bf), pltpu.VMEM((width, ff), bf),
            pltpu.VMEM((ff, width), bf), pltpu.VMEM((ff, width), bf),
            dma((13,)), dma((6,)), dma((6,)), dma((4,)), dma((4,)),
            per_piece, per_piece, per_piece, per_piece, per_piece, per_piece,
            dma((groups,)), dma((groups,)), per_piece, per_piece,
            dma((groups,)), dma((groups,)), dma((6,)), dma((6,)),
            dma((groups * HALVES + 1,)), pltpu.SemaphoreType.REGULAR,
        ],
        compiler_params=pltpu.CompilerParams(
            collective_id=3, has_side_effects=True, vmem_limit_bytes=56 * 1024 * 1024
        ),
        name="mixture",
    )(
        sink_logit, docs, routes.T, route_weights.T, norm_gain[None, :],
        queries, key_rows.reshape(blocks, WINDOW, kv_width),
        value_rows.reshape(blocks, WINDOW, kv_width), residual, out_weight,
        gate_weight, up_weight, down_weight,
    )
    return pl.pallas_call(
        place_kernel,
        out_shape=jax.ShapeDtypeStruct((rows, width), bf),
        in_specs=[hbm, hbm],
        out_specs=hbm,
        scratch_shapes=[
            pltpu.VMEM((rows, rows), bf), pltpu.VMEM((rows, width), bf),
            pltpu.VMEM((rows, width), bf), dma((3,)), dma((2,)),
        ],
        name="place",
    )(spread, moved)


def fits_front(queries):
    return lax.axis_size("tp") == 4 and queries.shape[0] % (8 * WINDOW) == 0


def stream_of(
    queries, key_rows, value_rows, doc_ids, sink_logit, residual, out_weight
):
    local_rows = queries.shape[0]
    if fits_front(queries):
        return front(queries, key_rows, value_rows, doc_ids, sink_logit, residual, out_weight)
    anchor = lax.axis_index("sp") * local_rows
    extent = local_rows * lax.axis_size("sp")
    doc_float = doc_ids.astype(jnp.bfloat16)
    block_rows = min(512, local_rows)
    padded_keys, padded_values, padded_docs = fetch_margins(key_rows, value_rows, doc_float)
    block_parts = []
    for row_start in range(0, local_rows, block_rows):
        key_end = row_start + block_rows + 2 * WINDOW
        block_parts.append(
            attend(
                queries[row_start : row_start + block_rows],
                padded_keys[row_start:key_end],
                padded_values[row_start:key_end],
                doc_float[row_start : row_start + block_rows],
                padded_docs[row_start:key_end],
                anchor + row_start,
                anchor + row_start - WINDOW,
                sink_logit,
                extent,
            )
        )
    attended = jnp.concatenate(block_parts, axis=0)
    regrouped = lax.all_to_all(attended, "tp", split_axis=0, concat_axis=1, tiled=True)
    shard_rows = out_weight.shape[0]
    initial = jnp.zeros((regrouped.shape[0], out_weight.shape[1]), jnp.float32)
    running = initial
    weight_piece = lax.all_gather(out_weight, "tp", axis=0, tiled=True)
    for shard_index in range(weight_piece.shape[0] // shard_rows):
        columns = lax.dynamic_slice_in_dim(regrouped, shard_index * shard_rows, shard_rows, 1)
        partial_value = jnp.dot(
            columns,
            weight_piece[shard_index * shard_rows : (shard_index + 1) * shard_rows],
            preferred_element_type=jnp.float32,
        )
        running = running + partial_value.astype(jnp.bfloat16).astype(jnp.float32)
    stream = (residual.astype(jnp.float32) + running).astype(jnp.bfloat16)
    return stream


def per_device(
    queries,
    key_rows,
    value_rows,
    doc_ids,
    sink_logit,
    residual,
    out_weight,
    norm_gain,
    gate_weight,
    up_weight,
    down_weight,
    routes,
    route_weights,
):
    front_args = (
        queries, key_rows, value_rows, doc_ids, sink_logit, residual, out_weight
    )
    if pair_routed(routes, gate_weight) and fits_front(queries):
        return mixture(
            *front_args, norm_gain, routes, route_weights, gate_weight, up_weight, down_weight
        )
    stream = stream_of(*front_args)
    stream_f = stream.astype(jnp.float32)
    scale = lax.rsqrt(jnp.mean(stream_f * stream_f, axis=1, keepdims=True) + eps_norm)
    normed = (stream_f * scale * norm_gain[None, :]).astype(jnp.bfloat16)
    home_rows = normed.shape[0]
    width = normed.shape[1]
    route_count = routes.shape[1]
    expert_count = lax.axis_size("sp") * gate_weight.shape[0]
    capacity = route_count * home_rows // expert_count
    flat_routes = routes.reshape(-1)
    one_hot = (flat_routes[:, None] == jnp.arange(expert_count, dtype=jnp.int32)[None, :]).astype(
        jnp.int32
    )
    earlier = jnp.cumsum(one_hot, axis=0) - one_hot
    slot_rank = jnp.sum(earlier * one_hot, axis=1)
    slot_index = flat_routes * capacity + slot_rank
    source_row = (
        jnp.zeros((expert_count * capacity,), jnp.int32)
        .at[slot_index]
        .set(jnp.arange(home_rows * route_count, dtype=jnp.int32) // route_count)
    )
    outgoing = normed[source_row].reshape(expert_count, capacity, width)
    incoming = lax.all_to_all(outgoing, "sp", split_axis=0, concat_axis=0, tiled=True)
    flat_rows = incoming.reshape(-1, width)
    gate_act = jnp.dot(flat_rows, gate_weight[0], preferred_element_type=jnp.float32)
    up_act = jnp.dot(flat_rows, up_weight[0], preferred_element_type=jnp.float32)
    hidden = (jax.nn.silu(gate_act) * up_act).astype(jnp.bfloat16)
    produced = jnp.dot(hidden, down_weight[0], preferred_element_type=jnp.float32).astype(
        jnp.bfloat16
    )
    returned = lax.all_to_all(
        produced.reshape(incoming.shape), "sp", split_axis=0, concat_axis=0, tiled=True
    )
    route_out = returned.reshape(-1, width)[slot_index].reshape(home_rows, route_count, width)
    weighted = jnp.sum(route_weights[:, :, None] * route_out.astype(jnp.float32), axis=1)
    return (stream_f + weighted).astype(jnp.bfloat16)


def solution(mesh):
    return jax.shard_map(
        per_device,
        mesh=mesh,
        in_specs=(
            P("sp", "tp"),
            P("sp", "tp"),
            P("sp", "tp"),
            P("sp"),
            P("tp"),
            P(("sp", "tp"), None),
            P("tp", None),
            P(),
            P("sp", None, None),
            P("sp", None, None),
            P("sp", None, None),
            P(("sp", "tp"), None),
            P(("sp", "tp"), None),
        ),
        out_specs=P(("sp", "tp"), None),
        check_vma=False,
    )
```
